32 devices in a mesh: sp: 4 (over y, x), tp: 8 (over z, core).
Axes of the slice: x: 2, y: 2, z: 4, core: 2. Of those that a mesh axis runs over, the one named last changes fastest.
Arguments:
- pool_input: bfloat16 [16384, 512], P('sp', 'tp'), may hold values from -6 to 6
- gate_pre: bfloat16 [16384, 1024], P(('sp', 'tp')), may hold values from -8 to 8
- resid: bfloat16 [16384, 1024], P(('sp', 'tp')), may hold values from -6 to 6
- docs: int32 [16384], P('sp'), may hold values from 0 to 3, never falling along the last dimension, each value on 1 to 8192 neighbouring positions
- w_up: bfloat16 [512, 1024], replicated, may hold values from -0.25 to 0.25
- w_out: bfloat16 [1024, 1024], replicated, may hold values from -0.1875 to 0.1875
- g_ffn: float32 [1024], replicated, may hold values from 0.1 to 1.9
- w_gate: bfloat16 [4, 1024, 1024], P('sp'), may hold values from -0.5 to 0.5
- w_lift: bfloat16 [4, 1024, 1024], P('sp'), may hold values from -0.5 to 0.5
- w_down: bfloat16 [4, 1024, 1024], P('sp'), may hold values from -0.0390625 to 0.0390625
- routes: int32 [16384, 2], P(('sp', 'tp')), may hold values from 0 to 3, all different within a row; in each aligned block of 512 rows (0 to 511, 512 to 1023, ...) at most 320 rows name the same one
- route_weight: float32 [16384, 2], P(('sp', 'tp')), may hold values from 0.2 to 1
Outputs:
- layer_out: bfloat16 [16384, 1024], P(('sp', 'tp'))
The draws below stay inside these ranges and needn't reach their ends.
Inputs may be any that keep to these rules, and one draw needn't show every extreme that they name: `routes`: each row names 2 different experts; among the 512 rows of one device no expert is named more than 320 times. `docs`: document numbers never fall along the sequence.
All inputs are finite; a program needn't handle non-finite values.
Results may differ from the reference program's by a relative error of at most 0.0075.
Values may be sent and summed in bfloat16 or wider, within the bound.
A program may use at most 128 MiB of HBM per device.

```python
import math
import jax
import jax.numpy as jnp
import numpy as np
from jax import lax

D = 1024
POOL_W = 512
HID = 1024
TOP = 2
RIM = 15
TOK_DEV = 4096
TOKENS = 16384
ROWS = 512
EXPERTS = 4
CAP = 320
N_SP = 4


def levels(stream_key, shape, shards, smallest, top_value):
    gain = 1.0
    for axis_at, parts in shards:
        steps = jax.random.uniform(jax.random.fold_in(jax.random.fold_in(stream_key, 6), axis_at), (parts,), jnp.float32, smallest / len(shards), top_value / len(shards))
        gain = gain * jnp.repeat(jnp.exp(steps), shape[axis_at] // parts).reshape((-1,) + (1,) * (len(shape) - 1 - axis_at))
    return gain


def length_profile(amount, total, limit, slope):
    portions = [(1 << 20) // math.isqrt(grade ** slope) + 1 for grade in range(2, amount + 1)]
    surplus, given = total - limit - (amount - 1), [1] * (amount - 1)
    while surplus > 0:
        candidates = [i for i in range(amount - 1) if given[i] < limit]
        mass, left = sum([portions[i] for i in candidates]), surplus
        for i in candidates:
            extra = min(limit - given[i], max(1, left * portions[i] // mass), surplus)
            given[i] = given[i] + extra
            surplus = surplus - extra
    return np.array([limit] + given)


def uneven_parts(own_key, number_of, total, reach, lean):
    if number_of == 2:
        one = jax.random.randint(own_key, (), max(1, total - reach), min(reach, total - 1) + 1)
        return jnp.stack([one, total - one])
    sizes = jnp.asarray(length_profile(number_of, total, reach, lean), jnp.int32)
    twos = (number_of - 1) // 2
    donor, taker = sizes[1:1 + 2 * twos:2], sizes[2:2 + 2 * twos:2]
    slack = jnp.minimum(donor - 1, reach - taker)
    moved = jax.random.randint(jax.random.fold_in(own_key, 1), (twos,), 0, 1 << 20) % (slack + 1)
    sizes = sizes.at[1:1 + 2 * twos:2].set(donor - moved).at[2:2 + 2 * twos:2].set(taker + moved)
    return sizes[jax.random.permutation(jax.random.fold_in(own_key, 2), number_of)]


def assign_block(stream_key, own, number, rows, count, top, limit, skew):
    order = jax.random.permutation(stream_key, count)
    packed, usual = shares(count, rows * top, limit, skew, True), shares(count, rows * top, limit, skew, False)
    places = jnp.arange(count)

    def named(lengths, turn):
        used = int((lengths > 0).sum())
        fixed = max(1, used // 4)
        passed = fixed + (places - fixed + turn * (used - fixed)) % max(1, count - fixed)
        return jnp.zeros((count,), jnp.int32).at[order[jnp.where(places < fixed, places, passed)]].set(jnp.asarray(lengths, jnp.int32))

    lengths = jnp.where(number % 4 == 0, named(packed, number // 4), named(usual, number - number // 4 - 1))
    mixed = jax.random.permutation(jax.random.fold_in(own, 3), count)
    source_of, sink = mixed[0:count // 2 * 2:2], mixed[1:count // 2 * 2:2]
    margin = jnp.minimum(lengths[source_of] - 1, limit - lengths[sink]) // 2
    margin = jnp.where((source_of == order[0]) | (sink == order[0]) | (lengths[sink] == 0), 0, jnp.maximum(margin, 0))
    passed = jax.random.randint(jax.random.fold_in(own, 4), (count // 2,), 0, 1 << 20) % (margin + 1)
    lengths = lengths.at[source_of].add(-passed).at[sink].add(passed)
    members = jnp.searchsorted(jnp.cumsum(lengths), jnp.arange(rows * top), side="right").astype(jnp.int32)
    grid = members.reshape(top, rows).T
    grid = grid[jax.random.permutation(jax.random.fold_in(own, 1), rows)]
    turn = jax.random.randint(jax.random.fold_in(own, 2), (rows, 1), 0, top)
    return jnp.take_along_axis(grid, (jnp.arange(top)[None, :] + turn) % top, axis=1)


def shares(number_of, total, reach, lean, full):
    loads = [(1 << 20) // math.isqrt(rank ** lean) + 1 for rank in range(1, number_of + 1)]
    largest = reach if full else min(reach, max(-(-total // number_of), total * loads[0] // sum(loads)))
    least = 1 if total - largest >= number_of - 1 else 0
    given, spare = [largest] + [least] * (number_of - 1), total - largest - least * (number_of - 1)
    while spare > 0:
        movable = [i for i in range(1, number_of) if given[i] < largest] or [i for i in range(1, number_of) if given[i] < reach]
        pool, budget = sum([loads[i] for i in movable]), spare
        for i in movable:
            extra = min(reach - given[i], max(1, budget * loads[i] // pool), spare)
            given[i] = given[i] + extra
            spare = spare - extra
    return np.array(given)


def bell_draw(stream_key, dims, deviation, bound, shards=(), held_as=jnp.bfloat16):
    drawn = jax.random.normal(stream_key, dims, jnp.float32) * deviation
    if len(shards) > 0:
        drawn = levels(stream_key, dims, shards, -0.22, 0.18) * drawn
    return jnp.clip(drawn, min=-bound, max=bound).astype(held_as)


def setup_inputs(seed: int = 0) -> dict:
    seeds = jax.random.split(jax.random.key(seed), 13)
    pool_input = bell_draw(seeds[0], (TOKENS, POOL_W), 1.0, 6.0, ((0, 4), (1, 8)))
    gate_pre = bell_draw(seeds[1], (TOKENS, D), 1.5, 8.0, ((0, 32),))
    resid = bell_draw(seeds[2], (TOKENS, D), 1.0, 6.0, ((0, 32),))
    docs = jnp.searchsorted(jnp.cumsum(uneven_parts(seeds[3], N_SP, TOKENS, 2 * TOK_DEV, 2)), jnp.arange(TOKENS), side="right").astype(jnp.int32)
    w_up = bell_draw(seeds[4], (POOL_W, D), POOL_W ** -0.5, 0.25)
    w_out = bell_draw(seeds[5], (D, D), D ** -0.5, 0.1875)
    g_ffn = jnp.clip(1.0 + 0.18 * jax.random.normal(seeds[6], (D,), jnp.float32), 0.1, 1.9)
    w_gate = bell_draw(seeds[7], (EXPERTS, D, HID), (D // 9) ** -0.5, 0.5, ((0, 4),))
    w_lift = bell_draw(seeds[8], (EXPERTS, D, HID), (D // 9) ** -0.5, 0.5, ((0, 4),))
    w_down = bell_draw(seeds[9], (EXPERTS, HID, D), (25 * HID) ** -0.5, 0.0390625, ((0, 4),))
    routes_keys = jax.random.split(jax.random.fold_in(seeds[10], 1), TOKENS // ROWS)
    routes_turns = jax.random.permutation(jax.random.fold_in(seeds[10], 3), TOKENS // ROWS)
    routes = jax.vmap(lambda own, number: assign_block(jax.random.fold_in(seeds[10], 2), own, number, ROWS, EXPERTS, TOP, CAP, 1))(routes_keys, routes_turns).reshape((TOKENS, TOP))
    route_weight = jnp.clip(0.2 + 0.8 * jax.random.uniform(seeds[11], (TOKENS, TOP), jnp.float32) ** levels(seeds[11], (TOKENS, TOP), ((0, 32),), -0.2, 0.2), 0.2, 1.0)
    return dict(pool_input=pool_input, gate_pre=gate_pre, resid=resid, docs=docs, w_up=w_up, w_out=w_out, g_ffn=g_ffn, w_gate=w_gate, w_lift=w_lift, w_down=w_down, routes=routes, route_weight=route_weight)


def pool_mixer(pool_input, docs):
    length = pool_input.shape[0]
    channels = pool_input.shape[1]
    group_size = POOL_W // 4
    channel_ids = lax.iota(jnp.int32, channels)
    window = jnp.power(2, channel_ids // group_size + 1)
    values = pool_input.astype(jnp.float32)
    padded = jnp.concatenate([jnp.zeros((RIM, channels), jnp.float32), values], axis=0)
    doc_padded = jnp.concatenate([jnp.full((RIM,), -1, jnp.int32), docs.astype(jnp.int32)], axis=0)
    running = jnp.zeros((length, channels), jnp.float32)
    counts = jnp.zeros((length, channels), jnp.float32)
    for offset in range(RIM + 1):
        shifted = padded[RIM - offset:RIM - offset + length]
        same_doc = (doc_padded[RIM - offset:RIM - offset + length] == docs).astype(jnp.float32)
        weight_mask = same_doc[:, None] * (offset < window).astype(jnp.float32)[None, :]
        running = running + weight_mask * shifted
        counts = counts + weight_mask
    return (running / counts - values).astype(jnp.bfloat16)

def reference(pool_input, gate_pre, resid, docs, w_up, w_out, g_ffn, w_gate, w_lift, w_down, routes, route_weight):
    pooled = pool_mixer(pool_input, docs)
    lifted = jnp.dot(pooled, w_up, preferred_element_type=jnp.float32)
    gated_rows = (jax.nn.sigmoid(gate_pre.astype(jnp.float32)) * lifted).astype(jnp.bfloat16)
    mixed_rows = (resid.astype(jnp.float32) + jnp.dot(gated_rows, w_out, preferred_element_type=jnp.float32)).astype(jnp.bfloat16)
    mixed_f = mixed_rows.astype(jnp.float32)
    normed = (mixed_f * lax.rsqrt(lax.optimization_barrier(jnp.mean(mixed_f * mixed_f, axis=-1, keepdims=True)) + 1e-06) * g_ffn).astype(jnp.bfloat16)
    gate_f = w_gate.astype(jnp.float32)
    lift_f = w_lift.astype(jnp.float32)
    down_f = w_down.astype(jnp.float32)
    blocks = TOKENS // ROWS
    model_dim = normed.shape[1]

    def one_block(inputs):
        block_rows, block_routes, block_weight, block_mixed = inputs
        flat_ids = block_routes.reshape(-1)
        onehot = (flat_ids[:, None] == lax.iota(jnp.int32, EXPERTS)[None, :]).astype(jnp.int32)
        slot_rank = lax.optimization_barrier(jnp.sum((jnp.cumsum(onehot, axis=0) - onehot) * onehot, axis=1))
        slot_index = flat_ids * CAP + slot_rank
        source = block_rows[lax.iota(jnp.int32, ROWS * TOP) // TOP]
        buffer = jnp.zeros((EXPERTS * CAP, model_dim), jnp.bfloat16).at[slot_index].set(source)
        buffer = buffer.reshape(EXPERTS, CAP, model_dim).astype(jnp.float32)
        gate_act = jnp.minimum(jnp.einsum('ekd,edh->ekh', buffer, gate_f), 7.0)
        lift = jnp.clip(jnp.einsum('ekd,edh->ekh', buffer, lift_f), -7.0, 7.0)
        act = ((lift + 1.0) * gate_act * jax.nn.sigmoid(1.702 * gate_act)).astype(jnp.bfloat16)
        expert_out = jnp.einsum('ekh,ehd->ekd', act.astype(jnp.float32), down_f).astype(jnp.bfloat16)
        returned = expert_out.reshape(EXPERTS * CAP, model_dim)[slot_index].astype(jnp.float32)
        returned = returned * block_weight.reshape(-1)[:, None]
        combined = lax.optimization_barrier(jnp.sum(returned.reshape(ROWS, TOP, model_dim), axis=1))
        return (block_mixed.astype(jnp.float32) + combined).astype(jnp.bfloat16)
    result = lax.map(one_block, (normed.reshape(blocks, ROWS, model_dim), routes.reshape(blocks, ROWS, TOP), route_weight.reshape(blocks, ROWS, TOP), mixed_rows.reshape(blocks, ROWS, model_dim)))
    return result.reshape(TOKENS, model_dim)
```

```python
import functools

import jax
import jax.numpy as jnp
from jax import lax
from jax.experimental import pallas as pl
from jax.experimental.pallas import tpu as pltpu
from jax.sharding import PartitionSpec as P

POOL_W = 512
RIM = 15
TILE = 256
LANES = 128
END_SHARE = 6
MESH = pl.DeviceIdType.MESH


def shifted_2(value, axis, steps):
    count = lax.axis_size(axis)
    leading, last = (max(0, -steps), min(count, count - steps))
    return lax.ppermute(value, axis, [(source, source + steps) for source in range(leading, last)])


def partner(me, step, count):
    other, bit = 0, 1
    while bit < count:
        other = other + ((me // bit + step // bit) % 2) * bit
        bit *= 2
    return other


def tile_of(t):
    return pl.ds(pl.multiple_of(t * TILE, TILE), TILE)


def experts_kernel(
    count,
    mixed_ref,
    gain_ref,
    rank_rows_ref,
    rank_cols_ref,
    weight_ref,
    w_gate_hbm,
    w_lift_hbm,
    w_down_hbm,
    out_ref,
    normed,
    onehot,
    send,
    recv,
    result,
    back,
    total,
    act,
    w_gate,
    w_lift,
    w_down,
    weight_sems,
    go_sems,
    come_sems,
    ret_go_sems,
    ret_come_sems,
):
    rows, model_dim = mixed_ref.shape
    cap = send.shape[1]
    hidden = w_gate.shape[1]
    me = lax.axis_index("sp")
    loads = [
        pltpu.make_async_copy(src.at[0], dst, weight_sems.at[i])
        for i, (src, dst) in enumerate(
            ((w_gate_hbm, w_gate), (w_lift_hbm, w_lift), (w_down_hbm, w_down))
        )
    ]

    barrier = pltpu.get_barrier_semaphore()

    def greet(j, carry):
        pl.semaphore_signal(
            barrier, inc=1, device_id={"sp": partner(me, j, count)}, device_id_type=MESH
        )
        return carry

    lax.fori_loop(1, count, greet, 0)
    for load in loads:
        load.start()

    def norm(t, carry):
        block = pl.ds(pl.multiple_of(t * 64, 64), 64)
        x = mixed_ref[block, :].astype(jnp.float32)
        scale = lax.rsqrt(jnp.mean(x * x, axis=-1, keepdims=True) + 1e-06)
        normed[block, :] = (x * scale * gain_ref[...]).astype(jnp.bfloat16)
        return carry

    lax.fori_loop(0, rows // 64, norm, 0)

    def out_copy(j):
        return pltpu.make_async_remote_copy(
            src_ref=send.at[j],
            dst_ref=recv.at[j],
            send_sem=go_sems.at[j],
            recv_sem=come_sems.at[j],
            device_id={"sp": partner(me, j, count)},
            device_id_type=MESH,
        )

    def back_copy(j):
        return pltpu.make_async_remote_copy(
            src_ref=result.at[j],
            dst_ref=back.at[j],
            send_sem=ret_go_sems.at[j],
            recv_sem=ret_come_sems.at[j],
            device_id={"sp": partner(me, j, count)},
            device_id_type=MESH,
        )

    def pack(j, target):
        slot = lax.broadcasted_iota(jnp.int32, (cap, rows), 0)
        onehot[...] = (slot == rank_rows_ref[j]).astype(jnp.float32).astype(jnp.bfloat16)

        def piece(t, carry):
            cols = tile_of(t)
            target[j, :, cols] = jnp.dot(
                onehot[...], normed[:, cols], preferred_element_type=jnp.float32
            ).astype(jnp.bfloat16)
            return carry

        lax.fori_loop(0, model_dim // TILE, piece, 0)

    def ffn(j, source):
        def up(t, carry):
            cols = tile_of(t)
            x = source[j]
            gate = jnp.minimum(jnp.dot(x, w_gate[:, cols], preferred_element_type=jnp.float32), 7.0)
            lift = jnp.clip(
                jnp.dot(x, w_lift[:, cols], preferred_element_type=jnp.float32), -7.0, 7.0
            )
            act[:, cols] = ((lift + 1.0) * gate * jax.nn.sigmoid(1.702 * gate)).astype(jnp.bfloat16)
            return carry

        lax.fori_loop(0, hidden // TILE, up, 0)

        def down(t, carry):
            cols = tile_of(t)
            result[j, :, cols] = jnp.dot(
                act[...], w_down[:, cols], preferred_element_type=jnp.float32
            ).astype(jnp.bfloat16)
            return carry

        lax.fori_loop(0, model_dim // TILE, down, 0)

    def column(ref, j):
        lane = lax.broadcasted_iota(jnp.int32, ref.shape, 1)
        return jnp.sum(jnp.where(lane == j, ref[...], 0.0), axis=1, keepdims=True)

    def combine(j, source, store):
        rank = column(rank_cols_ref, j).astype(jnp.int32)
        weight = column(weight_ref, j)
        slot = lax.broadcasted_iota(jnp.int32, (rows, cap), 1)
        pick = (slot == rank).astype(jnp.float32).astype(jnp.bfloat16)

        def piece(t, carry):
            cols = tile_of(t)
            found = jnp.dot(pick, source[j, :, cols], preferred_element_type=jnp.float32)
            store(cols, weight * found)
            return carry

        lax.fori_loop(0, model_dim // TILE, piece, 0)

    def store_first(cols, term):
        total[:, cols] = mixed_ref[:, cols].astype(jnp.float32) + term

    def store_more(cols, term):
        total[:, cols] = total[:, cols] + term

    def store_last(cols, term):
        out_ref[:, cols] = (total[:, cols] + term).astype(jnp.bfloat16)

    pl.semaphore_wait(barrier, count - 1)

    def dispatch(j, carry):
        pack(j, send)
        out_copy(j).start()
        return carry

    lax.fori_loop(1, count, dispatch, 0)
    pack(0, send)
    for load in loads:
        load.wait()
    ffn(0, send)
    combine(0, result, store_first)

    def serve(j, carry):
        out_copy(j).wait_recv()
        ffn(j, recv)
        back_copy(j).start()
        return carry

    lax.fori_loop(1, count, serve, 0)

    def gather(j, carry):
        back_copy(j).wait_recv()
        combine(j, back, store_more)
        return carry

    lax.fori_loop(1, count - 1, gather, 0)
    back_copy(count - 1).wait_recv()
    combine(count - 1, back, store_last)

    def finish(j, carry):
        out_copy(j).wait_send()
        back_copy(j).wait_send()
        return carry

    lax.fori_loop(1, count, finish, 0)


def run_experts(mixed, gain, rank, weight, w_gate, w_lift, w_down, cap, count):
    rows, model_dim = mixed.shape
    hidden = w_gate.shape[2]
    vmem = pl.BlockSpec(memory_space=pltpu.VMEM)
    anywhere = pl.BlockSpec(memory_space=pl.ANY)
    slots = pltpu.VMEM((count, cap, model_dim), jnp.bfloat16)
    return pl.pallas_call(
        functools.partial(experts_kernel, count),
        out_shape=jax.ShapeDtypeStruct((rows, model_dim), jnp.bfloat16),
        in_specs=[vmem] * 5 + [anywhere] * 3,
        out_specs=vmem,
        scratch_shapes=[
            pltpu.VMEM((rows, model_dim), jnp.bfloat16),
            pltpu.VMEM((cap, rows), jnp.bfloat16),
            slots,
            slots,
            slots,
            slots,
            pltpu.VMEM((rows, model_dim), jnp.float32),
            pltpu.VMEM((cap, hidden), jnp.bfloat16),
            pltpu.VMEM(w_gate.shape[1:], jnp.bfloat16),
            pltpu.VMEM(w_lift.shape[1:], jnp.bfloat16),
            pltpu.VMEM(w_down.shape[1:], jnp.bfloat16),
            pltpu.SemaphoreType.DMA((3,)),
            pltpu.SemaphoreType.DMA((count,)),
            pltpu.SemaphoreType.DMA((count,)),
            pltpu.SemaphoreType.DMA((count,)),
            pltpu.SemaphoreType.DMA((count,)),
        ],
        compiler_params=pltpu.CompilerParams(
            collective_id=0, has_side_effects=True, vmem_limit_bytes=60 * 2**20
        ),
        cost_estimate=pl.CostEstimate(
            flops=6 * count * cap * model_dim * hidden,
            bytes_accessed=3 * model_dim * hidden * 2,
            transcendentals=count * cap * hidden,
        ),
    )(
        mixed,
        gain[None, :],
        rank.T[:, None, :],
        rank.astype(jnp.float32),
        weight,
        w_gate,
        w_lift,
        w_down,
    )


def fused_kernel(
    count,
    tp_count,
    pool_hbm,
    docs_hbm,
    routes_ref,
    route_weight_ref,
    gain_ref,
    gate_hbm,
    resid_hbm,
    w_up_hbm,
    w_out_hbm,
    w_gate_hbm,
    w_lift_hbm,
    w_down_hbm,
    out_ref,
    pool,
    docs,
    gate_pre,
    resid,
    w_up,
    w_out,
    w_gate,
    w_lift,
    w_down,
    pooled,
    gathered,
    tokens,
    gated,
    mixed,
    normed,
    onehot,
    pick_near,
    pick_local,
    send,
    recv,
    result,
    back,
    own,
    corner,
    act,
    corner_act,
    corner_up,
    corner_down,
    corner_out,
    local_out,
    total,
    load_sems,
    edge_go,
    edge_come,
    pool_go,
    pool_come,
    part_go,
    part_come,
    share_go,
    out_go,
    out_come,
    ret_go,
    ret_come,
    core_go,
    core_come,
):
    channels = pool_hbm.shape[0]
    rows, model_dim = resid.shape
    hidden = w_gate.shape[1]
    half = hidden // 2
    cap = own.shape[0]
    part = cap // 2
    sp, tp = lax.axis_index("sp"), lax.axis_index("tp")
    plane, core = tp // 2, tp % 2
    planes = tp_count // 2
    at_end = (plane == 0) | (plane == planes - 1)
    inside = (plane > 0) & (plane < planes - 1)
    f32, bf16 = jnp.float32, jnp.bfloat16

    loads = [
        pltpu.make_async_copy(src, dst, load_sems.at[i])
        for i, (src, dst) in enumerate(
            (
                (pool_hbm, pool.at[:, LANES:]),
                (docs_hbm, docs.at[:, LANES:]),
                (w_up_hbm, w_up),
                (gate_hbm, gate_pre),
                (w_out_hbm, w_out),
                (resid_hbm, resid),
                (w_gate_hbm.at[0], w_gate),
                (w_lift_hbm.at[0], w_lift),
                (w_down_hbm.at[0], w_down),
            )
        )
    ]
    for load in loads[:2]:
        load.start()
    barrier = pltpu.get_barrier_semaphore()

    def greet_sp(j, carry):
        pl.semaphore_signal(
            barrier, inc=1, device_id={"sp": partner(sp, j, count)}, device_id_type=MESH
        )
        return carry

    def greet_tp(j, carry):
        pl.semaphore_signal(
            barrier, inc=1, device_id={"tp": partner(tp, j, tp_count)}, device_id_type=MESH
        )
        return carry

    lax.fori_loop(1, count, greet_sp, 0)
    lax.fori_loop(1, tp_count, greet_tp, 0)
    for load in loads[2:]:
        load.start()

    def remote(src, dst, go, come, device):
        return pltpu.make_async_remote_copy(
            src_ref=src,
            dst_ref=dst,
            send_sem=go,
            recv_sem=come,
            device_id=device,
            device_id_type=MESH,
        )

    following = {"sp": lax.rem(sp + 1, count)}
    tok_dev = pool_hbm.shape[1]
    edges = [
        remote(
            ref.at[:, pl.ds(tok_dev, LANES)],
            ref.at[:, pl.ds(0, LANES)],
            edge_go.at[i],
            edge_come.at[i],
            following,
        )
        for i, ref in enumerate((pool, docs))
    ]

    parts = [(m, q) for q in range(2) for m in range(2)] + [(2, q) for q in range(2)]
    sources = (w_gate_hbm, w_lift_hbm, w_down_hbm)
    inner = (16 - END_SHARE) // 2

    def span(m, q, zone):
        unit = (model_dim if m < 2 else half) // 16
        if isinstance(zone, int) and zone == 0:
            return q * (END_SHARE * unit // 2), END_SHARE * unit // 2
        start = (END_SHARE + inner * (zone - 1)) * unit + q * (inner * unit // 2)
        return pl.multiple_of(start, 16), inner * unit // 2

    def place(m, start, size):
        if m < 2:
            return corner_up.at[m, pl.ds(start, size), :]
        return corner_down.at[pl.ds(start, size), :]

    def fetch(i, zone):
        m, q = parts[i]
        start, size = span(m, q, zone)
        if m < 2:
            cols = pl.ds(pl.multiple_of(core * half, half), half)
            src = sources[m].at[0, pl.ds(start, size), cols]
        else:
            first = pl.multiple_of(core * half + start, 16)
            src = sources[m].at[0, pl.ds(first, size), :]
        return remote(
            src,
            place(m, start, size),
            part_go.at[i],
            part_come.at[zone, i],
            {"sp": partner(sp, 3, count)},
        )

    def share(i, zone, hop):
        m, q = parts[i]
        start, size = span(m, q, zone)
        return remote(
            place(m, start, size),
            place(m, start, size),
            share_go.at[hop - 1, i],
            part_come.at[zone, i],
            {"tp": partner(tp, 2 * hop, tp_count)},
        )

    def pass_on(i):
        @pl.when(at_end)
        def _():
            fetch(i, 0).wait_recv()
            share(i, 0, 1).start()

        @pl.when(inside)
        def _():
            fetch(i, plane).wait_recv()
            for hop in (3, 2, 1):
                share(i, plane, hop).start()

    def arrived(i):
        @pl.when(at_end)
        def _():
            share(i, 1, 1).wait_recv()
            share(i, 2, 1).wait_recv()

        @pl.when(inside)
        def _():
            share(i, 0, 1).wait_recv()
            share(i, 3 - plane, 1).wait_recv()

    for load in loads[:2]:
        load.wait()
    pl.semaphore_wait(barrier, count - 1 + tp_count - 1)
    for edge in edges:
        edge.start()

    @pl.when(at_end)
    def _():
        for i in range(len(parts)):
            fetch(i, 0).start()

    @pl.when(inside)
    def _():
        for i in range(len(parts)):
            fetch(i, plane).start()

    first, second = routes_ref[0:1, :], routes_ref[1:2, :]
    weight_first, weight_second = route_weight_ref[0:1, :], route_weight_ref[1:2, :]
    named, weights = [], []
    for j in range(count):
        expert = partner(sp, j, count)
        named.append(jnp.where((first == expert) | (second == expert), 1.0, 0.0))
        weights.append(
            jnp.where(first == expert, weight_first, 0.0)
            + jnp.where(second == expert, weight_second, 0.0)
        )
    named = jnp.concatenate(named + named, axis=0)
    weights = jnp.concatenate(weights + weights, axis=0)
    before = lax.broadcasted_iota(jnp.int32, (rows, rows), 0) <= lax.broadcasted_iota(
        jnp.int32, (rows, rows), 1
    )
    place_of = jnp.dot(
        named.astype(bf16), before.astype(f32).astype(bf16), preferred_element_type=f32
    )
    place_of = jnp.where(named > 0.0, place_of - 1.0, -4.0 * cap)
    split = jnp.where(place_of >= part, place_of + part, place_of)
    line = lax.broadcasted_iota(jnp.int32, place_of.shape, 0)
    goal = jnp.where(line == 1, split, place_of)
    goal = jnp.where(line == 2, split + part, goal)
    goal = jnp.where(line == 3, place_of + cap, goal)
    goal_rows = goal.astype(jnp.int32)
    goal_cols = goal.T.astype(jnp.int32)
    weight_cols = weights.T

    slot = lax.broadcasted_iota(jnp.int32, (2 * cap, rows), 0)
    for k, (a, b) in enumerate(((1, 2), (0, 3))):
        hit = (slot == goal_rows[a : a + 1, :]) | (slot == goal_rows[b : b + 1, :])
        onehot[k] = hit.astype(f32).astype(bf16)

    def weighed(slots, j, shift):
        return jnp.where(
            slots == goal_cols[:, j : j + 1] + shift, weight_cols[:, j : j + 1], 0.0
        )

    near_slots = lax.broadcasted_iota(jnp.int32, (rows, 2 * cap), 1)
    pick_near[...] = (weighed(near_slots, 1, 0) + weighed(near_slots, 2, 0)).astype(bf16)
    local_slots = lax.broadcasted_iota(jnp.int32, (rows, 3 * cap), 1)
    pick_local[...] = (
        weighed(local_slots, 0, 0) + weighed(local_slots, 3, 0) + weighed(local_slots, 3, cap)
    ).astype(bf16)

    level = (tp * channels) // (channels * tp_count // 4)
    for edge in edges:
        edge.wait_recv()

    def pool_copy(j):
        return remote(
            pooled.at[j],
            gathered.at[pl.ds(pl.multiple_of(tp * channels, channels), channels), :],
            pool_go.at[j],
            pool_come.at[j],
            {"tp": partner(tp, j, tp_count)},
        )

    def pool_block(j):
        owner = partner(tp, j, tp_count)
        cols = pl.ds(pl.multiple_of(owner * rows, LANES), rows + LANES)
        values = pool[:, cols].astype(f32)
        document = jnp.broadcast_to(docs[:, cols], (8, rows + LANES))
        lane = lax.broadcasted_iota(jnp.int32, document.shape, 1)
        document = jnp.where((lane < LANES) & (owner == 0) & (sp == 0), -1, document)
        running = values
        number = jnp.ones(document.shape, f32)
        for step in range(4):
            shift = 2**step
            same = (document == pltpu.roll(document, shift, 1)) & (level >= step)
            same = same.astype(f32)
            number = number + same * pltpu.roll(number, shift, 1)
            wide = jnp.concatenate([same] * (channels // 8), axis=0)
            running = running + wide * pltpu.roll(running, shift, 1)
        share_of = jnp.concatenate([1.0 / number] * (channels // 8), axis=0)
        return (running * share_of - values)[:, LANES:].astype(bf16)

    def pool_step(i, carry):
        j = tp_count - 1 - i
        pooled[j] = pool_block(j)
        pool_copy(j).start()
        return carry

    lax.fori_loop(0, tp_count - 1, pool_step, 0)
    gathered[pl.ds(pl.multiple_of(tp * channels, channels), channels), :] = pool_block(0)

    for i in range(3):
        pass_on(i)

    for load in loads[2:6]:
        load.wait()

    def pool_wait(j, carry):
        pool_copy(j).wait_recv()
        return carry

    lax.fori_loop(1, tp_count, pool_wait, 0)
    tokens[...] = gathered[...].T

    def lift_up(t, carry):
        cols = tile_of(t)
        lifted = jnp.dot(tokens[...], w_up[:, cols], preferred_element_type=f32)
        gated[:, cols] = (jax.nn.sigmoid(gate_pre[:, cols].astype(f32)) * lifted).astype(bf16)
        return carry

    lax.fori_loop(0, model_dim // TILE, lift_up, 0)

    def mix(t, carry):
        cols = tile_of(t)
        added = jnp.dot(gated[...], w_out[:, cols], preferred_element_type=f32)
        mixed[:, cols] = (resid[:, cols].astype(f32) + added).astype(bf16)
        return carry

    lax.fori_loop(0, model_dim // TILE, mix, 0)

    def norm(t, carry):
        block = pl.ds(pl.multiple_of(t * 64, 64), 64)
        x = mixed[block, :].astype(f32)
        scale = lax.rsqrt(jnp.mean(x * x, axis=-1, keepdims=True) + 1e-06)
        normed[block, :] = (x * scale * gain_ref[...]).astype(bf16)
        return carry

    lax.fori_loop(0, rows // 64, norm, 0)

    def pack_near(t, carry):
        cols = tile_of(t)
        send[:, cols] = jnp.dot(
            onehot[0], normed[:, cols], preferred_element_type=f32
        ).astype(bf16)
        return carry

    lax.fori_loop(0, model_dim // TILE, pack_near, 0)

    def out_copy(h, p):
        block = pl.ds((2 * h + p) * part, part)
        return remote(
            send.at[block],
            recv.at[block],
            out_go.at[2 * h + p],
            out_come.at[2 * h + p],
            {"sp": partner(sp, p + 1, count)},
        )

    def back_copy(h, p):
        block = pl.ds((2 * h + p) * part, part)
        return remote(
            result.at[block],
            back.at[block],
            ret_go.at[2 * h + p],
            ret_come.at[2 * h + p],
            {"sp": partner(sp, p + 1, count)},
        )

    chunks = [(h, p) for h in range(2) for p in range(2)]
    for h, p in chunks:
        out_copy(h, p).start()

    def pack_local(t, carry):
        cols = tile_of(t)
        packed = jnp.dot(onehot[1], normed[:, cols], preferred_element_type=f32).astype(bf16)
        own[:, cols] = packed[:cap]
        corner[0:cap, cols] = packed[cap:]
        return carry

    lax.fori_loop(0, model_dim // TILE, pack_local, 0)
    mate = {"tp": partner(tp, 1, tp_count)}
    corner_copy = remote(
        corner.at[pl.ds(0, cap)], corner.at[pl.ds(cap, cap)], core_go.at[0], core_come.at[0], mate
    )
    corner_copy.start()
    pass_on(3)

    def activate(gate, lift):
        gate = jnp.minimum(gate, 7.0)
        lift = jnp.clip(lift, -7.0, 7.0)
        return ((lift + 1.0) * gate * jax.nn.sigmoid(1.702 * gate)).astype(bf16)

    def ffn(source, target, base):
        def up(t, carry):
            cols = tile_of(t)
            x = source[base : base + cap, :]
            act[:, cols] = activate(
                jnp.dot(x, w_gate[:, cols], preferred_element_type=f32),
                jnp.dot(x, w_lift[:, cols], preferred_element_type=f32),
            )
            return carry

        lax.fori_loop(0, hidden // TILE, up, 0)

        def down(t, carry):
            cols = tile_of(t)
            target[base : base + cap, cols] = jnp.dot(
                act[...], w_down[:, cols], preferred_element_type=f32
            ).astype(bf16)
            return carry

        lax.fori_loop(0, model_dim // TILE, down, 0)

    for load in loads[6:]:
        load.wait()
    ffn(own, local_out, 0)
    pass_on(4)
    pass_on(5)

    for h in range(2):
        for p in range(2):
            out_copy(h, p).wait_recv()
        ffn(recv, result, h * cap)
        for p in range(2):
            back_copy(h, p).start()

    corner_copy.wait_recv()
    for i in range(4):
        arrived(i)

    def corner_lift(t, carry):
        cols = tile_of(t)
        x = corner[...]
        corner_act[:, cols] = activate(
            jnp.dot(x, corner_up[0, :, cols], preferred_element_type=f32),
            jnp.dot(x, corner_up[1, :, cols], preferred_element_type=f32),
        )
        return carry

    lax.fori_loop(0, half // TILE, corner_lift, 0)
    for i in range(4, 6):
        arrived(i)

    def corner_drop(t, carry):
        cols = tile_of(t)
        found = jnp.dot(
            corner_act[...], corner_down[:, cols], preferred_element_type=f32
        ).astype(bf16)
        local_out[cap : 2 * cap, cols] = found[:cap]
        corner_out[:, cols] = found[cap:]
        return carry

    lax.fori_loop(0, model_dim // TILE, corner_drop, 0)
    mate_copy = remote(
        corner_out, local_out.at[pl.ds(2 * cap, cap)], core_go.at[1], core_come.at[1], mate
    )
    mate_copy.start()
    mate_copy.wait_recv()

    def combine_local(t, carry):
        cols = tile_of(t)
        total[:, cols] = mixed[:, cols].astype(f32) + jnp.dot(
            pick_local[...], local_out[:, cols], preferred_element_type=f32
        )
        return carry

    lax.fori_loop(0, model_dim // TILE, combine_local, 0)
    for h, p in chunks:
        back_copy(h, p).wait_recv()

    def combine_near(t, carry):
        cols = tile_of(t)
        found = jnp.dot(pick_near[...], back[:, cols], preferred_element_type=f32)
        out_ref[:, cols] = (total[:, cols] + found).astype(bf16)
        return carry

    lax.fori_loop(0, model_dim // TILE, combine_near, 0)

    for edge in edges:
        edge.wait_send()

    def pool_sent(j, carry):
        pool_copy(j).wait_send()
        return carry

    lax.fori_loop(1, tp_count, pool_sent, 0)
    for h, p in chunks:
        out_copy(h, p).wait_send()
        back_copy(h, p).wait_send()
    corner_copy.wait_send()
    mate_copy.wait_send()
    for i in range(len(parts)):

        @pl.when(at_end)
        def _():
            fetch(i, 0).wait_send()
            share(i, 0, 1).wait_send()

        @pl.when(inside)
        def _():
            fetch(i, plane).wait_send()
            for hop in (1, 2, 3):
                share(i, plane, hop).wait_send()


def run_fused(
    count,
    tp_count,
    pool_input,
    gate_pre,
    resid,
    docs,
    w_up,
    w_out,
    g_ffn,
    w_gate,
    w_lift,
    w_down,
    routes,
    route_weight,
):
    tok_dev, channels = pool_input.shape
    rows, model_dim = resid.shape
    hidden = w_gate.shape[2]
    half = hidden // 2
    pool_w = w_up.shape[0]
    cap = capacity(rows, routes.shape[1], count)
    vmem = pl.BlockSpec(memory_space=pltpu.VMEM)
    anywhere = pl.BlockSpec(memory_space=pl.ANY)
    bf16, f32 = jnp.bfloat16, jnp.float32
    dma = pltpu.SemaphoreType.DMA
    return pl.pallas_call(
        functools.partial(fused_kernel, count, tp_count),
        out_shape=jax.ShapeDtypeStruct((rows, model_dim), bf16),
        in_specs=[anywhere] * 2 + [vmem] * 3 + [anywhere] * 7,
        out_specs=vmem,
        scratch_shapes=[
            pltpu.VMEM((channels, tok_dev + LANES), bf16),
            pltpu.VMEM((1, tok_dev + LANES), jnp.int32),
            pltpu.VMEM((rows, model_dim), bf16),
            pltpu.VMEM((rows, model_dim), bf16),
            pltpu.VMEM(w_up.shape, bf16),
            pltpu.VMEM(w_out.shape, bf16),
            pltpu.VMEM(w_gate.shape[1:], bf16),
            pltpu.VMEM(w_lift.shape[1:], bf16),
            pltpu.VMEM(w_down.shape[1:], bf16),
            pltpu.VMEM((tp_count, channels, rows), bf16),
            pltpu.VMEM((pool_w, rows), bf16),
            pltpu.VMEM((rows, pool_w), bf16),
            pltpu.VMEM((rows, model_dim), bf16),
            pltpu.VMEM((rows, model_dim), bf16),
            pltpu.VMEM((rows, model_dim), bf16),
            pltpu.VMEM((2, 2 * cap, rows), bf16),
            pltpu.VMEM((rows, 2 * cap), bf16),
            pltpu.VMEM((rows, 3 * cap), bf16),
            pltpu.VMEM((2 * cap, model_dim), bf16),
            pltpu.VMEM((2 * cap, model_dim), bf16),
            pltpu.VMEM((2 * cap, model_dim), bf16),
            pltpu.VMEM((2 * cap, model_dim), bf16),
            pltpu.VMEM((cap, model_dim), bf16),
            pltpu.VMEM((2 * cap, model_dim), bf16),
            pltpu.VMEM((cap, hidden), bf16),
            pltpu.VMEM((2 * cap, half), bf16),
            pltpu.VMEM((2, model_dim, half), bf16),
            pltpu.VMEM((half, model_dim), bf16),
            pltpu.VMEM((cap, model_dim), bf16),
            pltpu.VMEM((3 * cap, model_dim), bf16),
            pltpu.VMEM((rows, model_dim), f32),
            dma((9,)),
            dma((2,)),
            dma((2,)),
            dma((tp_count,)),
            dma((tp_count,)),
            dma((6,)),
            dma((3, 6)),
            dma((3, 6)),
            dma((4,)),
            dma((4,)),
            dma((4,)),
            dma((4,)),
            dma((2,)),
            dma((2,)),
        ],
        compiler_params=pltpu.CompilerParams(
            collective_id=1, has_side_effects=True, vmem_limit_bytes=60 * 2**20
        ),
        cost_estimate=pl.CostEstimate(
            flops=6 * count * cap * model_dim * hidden,
            bytes_accessed=3 * model_dim * hidden * 2,
            transcendentals=count * cap * hidden,
        ),
    )(
        pool_input.T,
        docs[None, :],
        routes.T,
        route_weight.T,
        g_ffn[None, :],
        gate_pre,
        resid,
        w_up,
        w_out,
        w_gate,
        w_lift,
        w_down,
    )


def capacity(row_count, top_count, count):
    cap = max(2, 5 * row_count * top_count // (4 * count))
    return (cap + 15) // 16 * 16


def on_device(
    pool_input,
    gate_pre,
    resid,
    docs,
    w_up,
    w_out,
    g_ffn,
    w_gate,
    w_lift,
    w_down,
    routes,
    route_weight,
):
    tok_dev = pool_input.shape[0]
    channels = pool_input.shape[1]
    group_size = POOL_W // 4
    channel_ids = lax.axis_index("tp") * channels + lax.iota(jnp.int32, channels)
    window = jnp.power(2, channel_ids // group_size + 1)
    edge = jnp.concatenate(
        [pool_input[tok_dev - RIM :], docs[tok_dev - RIM :, None].astype(jnp.bfloat16)], axis=1
    )
    before = shifted_2(edge, "sp", 1)
    before_rows = before[:, :channels]
    before_docs = before[:, channels].astype(jnp.int32)
    first_dev = lax.axis_index("sp") == 0
    before_docs = jnp.where(first_dev, -1, before_docs)
    values = pool_input.astype(jnp.float32)
    padded = jnp.concatenate([before_rows.astype(jnp.float32), values], axis=0)
    doc_padded = jnp.concatenate([before_docs.astype(jnp.int32), docs], axis=0)
    earlier = sum(
        (doc_padded[RIM - offset : RIM - offset + tok_dev] == docs).astype(jnp.int32)
        for offset in range(1, RIM + 1)
    )
    reach = jnp.minimum(earlier[:, None] + 1, window[None, :])
    running = values
    for offset in range(1, RIM + 1):
        shifted = padded[RIM - offset : RIM - offset + tok_dev]
        running = running + jnp.where(offset < reach, shifted, 0.0)
    counts = reach.astype(jnp.float32)
    pooled = (running / counts - values).astype(jnp.bfloat16)
    tokens_pooled = lax.all_to_all(pooled, "tp", split_axis=0, concat_axis=1, tiled=True)
    lifted = jnp.dot(tokens_pooled, w_up, preferred_element_type=jnp.float32)
    gated_rows = (jax.nn.sigmoid(gate_pre.astype(jnp.float32)) * lifted).astype(jnp.bfloat16)
    mixed_rows = (
        resid.astype(jnp.float32) + jnp.dot(gated_rows, w_out, preferred_element_type=jnp.float32)
    ).astype(jnp.bfloat16)

    row_count, top_count = routes.shape
    count = lax.axis_size("sp")
    cap = capacity(row_count, top_count, count)
    order = partner(lax.axis_index("sp"), lax.iota(jnp.int32, count), count)
    chosen = routes[:, :, None] == order[None, None, :]
    named = jnp.any(chosen, axis=1)
    rank = jnp.where(named, jnp.cumsum(named.astype(jnp.int32), axis=0) - 1, -1)
    weight = jnp.sum(jnp.where(chosen, route_weight[:, :, None], 0.0), axis=1)
    return run_experts(mixed_rows, g_ffn, rank, weight, w_gate, w_lift, w_down, cap, count)


def solution(mesh):
    in_specs = (
        P("sp", "tp"),
        P(("sp", "tp"), None),
        P(("sp", "tp"), None),
        P("sp"),
        P(),
        P(),
        P(),
        P("sp", None, None),
        P("sp", None, None),
        P("sp", None, None),
        P(("sp", "tp"), None),
        P(("sp", "tp"), None),
    )
    out_specs = P(("sp", "tp"), None)
    count, tp_count = mesh.shape["sp"], mesh.shape["tp"]
    body = on_device
    if count == 4 and tp_count == 8:
        body = functools.partial(run_fused, count, tp_count)
    return jax.shard_map(
        body, mesh=mesh, in_specs=in_specs, out_specs=out_specs, check_vma=False
    )
```

```python
import functools

import jax
import jax.numpy as jnp
from jax import lax
from jax.experimental import pallas as pl
from jax.experimental.pallas import tpu as pltpu
from jax.sharding import PartitionSpec as P

POOL_W = 512
RIM = 15
TILE = 256
LANES = 128
END_SHARE = 6
MESH = pl.DeviceIdType.MESH


def shifted_2(value, axis, steps):
    count = lax.axis_size(axis)
    leading, last = (max(0, -steps), min(count, count - steps))
    return lax.ppermute(value, axis, [(source, source + steps) for source in range(leading, last)])


def partner(me, step, count):
    other, bit = 0, 1
    while bit < count:
        other = other + ((me // bit + step // bit) % 2) * bit
        bit *= 2
    return other


def tile_of(t):
    return pl.ds(pl.multiple_of(t * TILE, TILE), TILE)


def experts_kernel(
    count,
    mixed_ref,
    gain_ref,
    rank_rows_ref,
    rank_cols_ref,
    weight_ref,
    w_gate_hbm,
    w_lift_hbm,
    w_down_hbm,
    out_ref,
    normed,
    onehot,
    send,
    recv,
    result,
    back,
    total,
    act,
    w_gate,
    w_lift,
    w_down,
    weight_sems,
    go_sems,
    come_sems,
    ret_go_sems,
    ret_come_sems,
):
    rows, model_dim = mixed_ref.shape
    cap = send.shape[1]
    hidden = w_gate.shape[1]
    me = lax.axis_index("sp")
    loads = [
        pltpu.make_async_copy(src.at[0], dst, weight_sems.at[i])
        for i, (src, dst) in enumerate(
            ((w_gate_hbm, w_gate), (w_lift_hbm, w_lift), (w_down_hbm, w_down))
        )
    ]

    barrier = pltpu.get_barrier_semaphore()

    def greet(j, carry):
        pl.semaphore_signal(
            barrier, inc=1, device_id={"sp": partner(me, j, count)}, device_id_type=MESH
        )
        return carry

    lax.fori_loop(1, count, greet, 0)
    for load in loads:
        load.start()

    def norm(t, carry):
        block = pl.ds(pl.multiple_of(t * 64, 64), 64)
        x = mixed_ref[block, :].astype(jnp.float32)
        scale = lax.rsqrt(jnp.mean(x * x, axis=-1, keepdims=True) + 1e-06)
        normed[block, :] = (x * scale * gain_ref[...]).astype(jnp.bfloat16)
        return carry

    lax.fori_loop(0, rows // 64, norm, 0)

    def out_copy(j):
        return pltpu.make_async_remote_copy(
            src_ref=send.at[j],
            dst_ref=recv.at[j],
            send_sem=go_sems.at[j],
            recv_sem=come_sems.at[j],
            device_id={"sp": partner(me, j, count)},
            device_id_type=MESH,
        )

    def back_copy(j):
        return pltpu.make_async_remote_copy(
            src_ref=result.at[j],
            dst_ref=back.at[j],
            send_sem=ret_go_sems.at[j],
            recv_sem=ret_come_sems.at[j],
            device_id={"sp": partner(me, j, count)},
            device_id_type=MESH,
        )

    def pack(j, target):
        slot = lax.broadcasted_iota(jnp.int32, (cap, rows), 0)
        onehot[...] = (slot == rank_rows_ref[j]).astype(jnp.float32).astype(jnp.bfloat16)

        def piece(t, carry):
            cols = tile_of(t)
            target[j, :, cols] = jnp.dot(
                onehot[...], normed[:, cols], preferred_element_type=jnp.float32
            ).astype(jnp.bfloat16)
            return carry

        lax.fori_loop(0, model_dim // TILE, piece, 0)

    def ffn(j, source):
        def up(t, carry):
            cols = tile_of(t)
            x = source[j]
            gate = jnp.minimum(jnp.dot(x, w_gate[:, cols], preferred_element_type=jnp.float32), 7.0)
            lift = jnp.clip(
                jnp.dot(x, w_lift[:, cols], preferred_element_type=jnp.float32), -7.0, 7.0
            )
            act[:, cols] = ((lift + 1.0) * gate * jax.nn.sigmoid(1.702 * gate)).astype(jnp.bfloat16)
            return carry

        lax.fori_loop(0, hidden // TILE, up, 0)

        def down(t, carry):
            cols = tile_of(t)
            result[j, :, cols] = jnp.dot(
                act[...], w_down[:, cols], preferred_element_type=jnp.float32
            ).astype(jnp.bfloat16)
            return carry

        lax.fori_loop(0, model_dim // TILE, down, 0)

    def column(ref, j):
        lane = lax.broadcasted_iota(jnp.int32, ref.shape, 1)
        return jnp.sum(jnp.where(lane == j, ref[...], 0.0), axis=1, keepdims=True)

    def combine(j, source, store):
        rank = column(rank_cols_ref, j).astype(jnp.int32)
        weight = column(weight_ref, j)
        slot = lax.broadcasted_iota(jnp.int32, (rows, cap), 1)
        pick = (slot == rank).astype(jnp.float32).astype(jnp.bfloat16)

        def piece(t, carry):
            cols = tile_of(t)
            found = jnp.dot(pick, source[j, :, cols], preferred_element_type=jnp.float32)
            store(cols, weight * found)
            return carry

        lax.fori_loop(0, model_dim // TILE, piece, 0)

    def store_first(cols, term):
        total[:, cols] = mixed_ref[:, cols].astype(jnp.float32) + term

    def store_more(cols, term):
        total[:, cols] = total[:, cols] + term

    def store_last(cols, term):
        out_ref[:, cols] = (total[:, cols] + term).astype(jnp.bfloat16)

    pl.semaphore_wait(barrier, count - 1)

    def dispatch(j, carry):
        pack(j, send)
        out_copy(j).start()
        return carry

    lax.fori_loop(1, count, dispatch, 0)
    pack(0, send)
    for load in loads:
        load.wait()
    ffn(0, send)
    combine(0, result, store_first)

    def serve(j, carry):
        out_copy(j).wait_recv()
        ffn(j, recv)
        back_copy(j).start()
        return carry

    lax.fori_loop(1, count, serve, 0)

    def gather(j, carry):
        back_copy(j).wait_recv()
        combine(j, back, store_more)
        return carry

    lax.fori_loop(1, count - 1, gather, 0)
    back_copy(count - 1).wait_recv()
    combine(count - 1, back, store_last)

    def finish(j, carry):
        out_copy(j).wait_send()
        back_copy(j).wait_send()
        return carry

    lax.fori_loop(1, count, finish, 0)


def run_experts(mixed, gain, rank, weight, w_gate, w_lift, w_down, cap, count):
    rows, model_dim = mixed.shape
    hidden = w_gate.shape[2]
    vmem = pl.BlockSpec(memory_space=pltpu.VMEM)
    anywhere = pl.BlockSpec(memory_space=pl.ANY)
    slots = pltpu.VMEM((count, cap, model_dim), jnp.bfloat16)
    return pl.pallas_call(
        functools.partial(experts_kernel, count),
        out_shape=jax.ShapeDtypeStruct((rows, model_dim), jnp.bfloat16),
        in_specs=[vmem] * 5 + [anywhere] * 3,
        out_specs=vmem,
        scratch_shapes=[
            pltpu.VMEM((rows, model_dim), jnp.bfloat16),
            pltpu.VMEM((cap, rows), jnp.bfloat16),
            slots,
            slots,
            slots,
            slots,
            pltpu.VMEM((rows, model_dim), jnp.float32),
            pltpu.VMEM((cap, hidden), jnp.bfloat16),
            pltpu.VMEM(w_gate.shape[1:], jnp.bfloat16),
            pltpu.VMEM(w_lift.shape[1:], jnp.bfloat16),
            pltpu.VMEM(w_down.shape[1:], jnp.bfloat16),
            pltpu.SemaphoreType.DMA((3,)),
            pltpu.SemaphoreType.DMA((count,)),
            pltpu.SemaphoreType.DMA((count,)),
            pltpu.SemaphoreType.DMA((count,)),
            pltpu.SemaphoreType.DMA((count,)),
        ],
        compiler_params=pltpu.CompilerParams(
            collective_id=0, has_side_effects=True, vmem_limit_bytes=60 * 2**20
        ),
        cost_estimate=pl.CostEstimate(
            flops=6 * count * cap * model_dim * hidden,
            bytes_accessed=3 * model_dim * hidden * 2,
            transcendentals=count * cap * hidden,
        ),
    )(
        mixed,
        gain[None, :],
        rank.T[:, None, :],
        rank.astype(jnp.float32),
        weight,
        w_gate,
        w_lift,
        w_down,
    )


def fused_kernel(
    count,
    tp_count,
    pool_hbm,
    docs_hbm,
    routes_hbm,
    route_weight_hbm,
    gain_hbm,
    gate_hbm,
    resid_hbm,
    w_up_hbm,
    w_out_hbm,
    w_gate_hbm,
    w_lift_hbm,
    w_down_hbm,
    out_ref,
    pool,
    docs,
    routes_ref,
    route_weight_ref,
    gain,
    gate_pre,
    resid,
    w_up,
    w_out,
    w_gate,
    w_lift,
    w_down,
    pooled,
    gathered,
    tokens,
    gated,
    mixed,
    normed,
    onehot,
    pick_own,
    pick_rest,
    send,
    recv,
    result,
    back,
    own,
    corner,
    act,
    corner_act,
    corner_up,
    corner_down,
    corner_out,
    local_out,
    total,
    load_sems,
    edge_go,
    edge_come,
    pool_go,
    pool_come,
    part_go,
    part_come,
    share_go,
    out_go,
    out_come,
    ret_go,
    ret_come,
    core_go,
    core_come,
):
    channels = pool_hbm.shape[0]
    rows, model_dim = resid.shape
    hidden = w_gate.shape[1]
    half = hidden // 2
    cap = own.shape[0]
    part = cap // 2
    sp, tp = lax.axis_index("sp"), lax.axis_index("tp")
    plane, core = tp // 2, tp % 2
    planes = tp_count // 2
    at_end = (plane == 0) | (plane == planes - 1)
    inside = (plane > 0) & (plane < planes - 1)
    f32, bf16 = jnp.float32, jnp.bfloat16

    loads = [
        pltpu.make_async_copy(src, dst, load_sems.at[i])
        for i, (src, dst) in enumerate(
            (
                (pool_hbm, pool.at[:, LANES:]),
                (docs_hbm, docs.at[:, LANES:]),
                (routes_hbm, routes_ref),
                (route_weight_hbm, route_weight_ref),
                (w_up_hbm, w_up),
                (gate_hbm, gate_pre),
                (w_out_hbm, w_out),
                (resid_hbm, resid),
                (gain_hbm, gain),
                (w_gate_hbm.at[0], w_gate),
                (w_lift_hbm.at[0], w_lift),
                (w_down_hbm.at[0], w_down),
            )
        )
    ]
    for load in loads[:2]:
        load.start()
    barrier = pltpu.get_barrier_semaphore()

    def greet_sp(j, carry):
        pl.semaphore_signal(
            barrier, inc=1, device_id={"sp": partner(sp, j, count)}, device_id_type=MESH
        )
        return carry

    def greet_tp(j, carry):
        pl.semaphore_signal(
            barrier, inc=1, device_id={"tp": partner(tp, j, tp_count)}, device_id_type=MESH
        )
        return carry

    lax.fori_loop(1, count, greet_sp, 0)
    lax.fori_loop(1, tp_count, greet_tp, 0)
    for load in loads[2:]:
        load.start()

    def remote(src, dst, go, come, device):
        return pltpu.make_async_remote_copy(
            src_ref=src,
            dst_ref=dst,
            send_sem=go,
            recv_sem=come,
            device_id=device,
            device_id_type=MESH,
        )

    following = {"sp": lax.rem(sp + 1, count)}
    tok_dev = pool_hbm.shape[1]
    edges = [
        remote(
            ref.at[:, pl.ds(tok_dev, LANES)],
            ref.at[:, pl.ds(0, LANES)],
            edge_go.at[i],
            edge_come.at[i],
            following,
        )
        for i, ref in enumerate((pool, docs))
    ]

    parts = [(m, q) for q in range(4) for m in range(2)] + [(2, q) for q in range(2)]
    sources = (w_gate_hbm, w_lift_hbm, w_down_hbm)
    inner = (16 - END_SHARE) // 2

    def span(m, q, zone):
        unit, cuts = (model_dim // 16, 4) if m < 2 else (half // 16, 2)
        if isinstance(zone, int) and zone == 0:
            return q * (END_SHARE * unit // cuts), END_SHARE * unit // cuts
        start = (END_SHARE + inner * (zone - 1)) * unit + q * (inner * unit // cuts)
        return pl.multiple_of(start, 16), inner * unit // cuts

    def place(m, start, size):
        if m < 2:
            return corner_up.at[m, pl.ds(start, size), :]
        return corner_down.at[pl.ds(start, size), :]

    def fetch(i, zone):
        m, q = parts[i]
        start, size = span(m, q, zone)
        if m < 2:
            cols = pl.ds(pl.multiple_of(core * half, half), half)
            src = sources[m].at[0, pl.ds(start, size), cols]
        else:
            first = pl.multiple_of(core * half + start, 16)
            src = sources[m].at[0, pl.ds(first, size), :]
        return remote(
            src,
            place(m, start, size),
            part_go.at[i],
            part_come.at[zone, i],
            {"sp": partner(sp, 3, count)},
        )

    def share(i, zone, hop):
        m, q = parts[i]
        start, size = span(m, q, zone)
        return remote(
            place(m, start, size),
            place(m, start, size),
            share_go.at[hop - 1, i],
            part_come.at[zone, i],
            {"tp": partner(tp, 2 * hop, tp_count)},
        )

    def pass_on(i):
        @pl.when(at_end)
        def _():
            fetch(i, 0).wait_recv()
            share(i, 0, 1).start()

        @pl.when(inside)
        def _():
            fetch(i, plane).wait_recv()
            for hop in (3, 2, 1):
                share(i, plane, hop).start()

    def arrived(i):
        @pl.when(at_end)
        def _():
            share(i, 1, 1).wait_recv()
            share(i, 2, 1).wait_recv()

        @pl.when(inside)
        def _():
            share(i, 0, 1).wait_recv()
            share(i, 3 - plane, 1).wait_recv()

    for load in loads[:2]:
        load.wait()
    pl.semaphore_wait(barrier, count - 1 + tp_count - 1)
    for edge in edges:
        edge.start()

    @pl.when(at_end)
    def _():
        for i in range(len(parts)):
            fetch(i, 0).start()

    @pl.when(inside)
    def _():
        for i in range(len(parts)):
            fetch(i, plane).start()

    level = (tp * channels) // (channels * tp_count // 4)

    def pool_copy(j):
        return remote(
            pooled.at[j],
            gathered.at[pl.ds(pl.multiple_of(tp * channels, channels), channels), :],
            pool_go.at[j],
            pool_come.at[j],
            {"tp": partner(tp, j, tp_count)},
        )

    def pool_block(j):
        owner = partner(tp, j, tp_count)
        cols = pl.ds(pl.multiple_of(owner * rows, LANES), rows + LANES)
        values = pool[:, cols].astype(f32)
        document = jnp.broadcast_to(docs[:, cols], (8, rows + LANES))
        lane = lax.broadcasted_iota(jnp.int32, document.shape, 1)
        document = jnp.where((lane < LANES) & (owner == 0) & (sp == 0), -1, document)
        running = values
        number = jnp.ones(document.shape, f32)
        for step in range(4):
            shift = 2**step
            same = (document == pltpu.roll(document, shift, 1)) & (level >= step)
            same = same.astype(f32)
            number = number + same * pltpu.roll(number, shift, 1)
            wide = jnp.concatenate([same] * (channels // 8), axis=0)
            running = running + wide * pltpu.roll(running, shift, 1)
        share_of = jnp.concatenate([1.0 / number] * (channels // 8), axis=0)
        return (running * share_of - values)[:, LANES:].astype(bf16)

    def pool_send(j):
        pooled[j] = pool_block(j)
        pool_copy(j).start()

    def pool_step(i, carry):
        j = tp_count - 1 - i

        @pl.when(j != tp)
        def _():
            pool_send(j)

        return carry

    lax.fori_loop(0, tp_count - 1, pool_step, 0)
    for edge in edges:
        edge.wait_recv()

    @pl.when(tp != 0)
    def _():
        pool_send(tp)

    gathered[pl.ds(pl.multiple_of(tp * channels, channels), channels), :] = pool_block(0)
    pass_on(0)

    for load in loads[2:4]:
        load.wait()

    first, second = routes_ref[0:1, :], routes_ref[1:2, :]
    weight_first, weight_second = route_weight_ref[0:1, :], route_weight_ref[1:2, :]
    named, weights = [], []
    for j in range(count):
        expert = partner(sp, j, count)
        named.append(jnp.where((first == expert) | (second == expert), 1.0, 0.0))
        weights.append(
            jnp.where(first == expert, weight_first, 0.0)
            + jnp.where(second == expert, weight_second, 0.0)
        )
    named = jnp.concatenate(named + named, axis=0)
    weights = jnp.concatenate(weights + weights, axis=0)
    before = lax.broadcasted_iota(jnp.int32, (rows, rows), 0) <= lax.broadcasted_iota(
        jnp.int32, (rows, rows), 1
    )
    place_of = jnp.dot(
        named.astype(bf16), before.astype(f32).astype(bf16), preferred_element_type=f32
    )
    place_of = jnp.where(named > 0.0, place_of - 1.0, -4.0 * cap)
    split = jnp.where(place_of >= part, place_of + part, place_of)
    line = lax.broadcasted_iota(jnp.int32, place_of.shape, 0)
    goal = jnp.where(line == 1, split, place_of)
    goal = jnp.where(line == 2, split + part, goal)
    goal = jnp.where(line == 3, place_of + cap, goal)
    goal_rows = goal.astype(jnp.int32)
    goal_cols = goal.T.astype(jnp.int32)
    weight_cols = weights.T

    slot = lax.broadcasted_iota(jnp.int32, (2 * cap, rows), 0)
    for k, (a, b) in enumerate(((1, 2), (0, 3))):
        hit = (slot == goal_rows[a : a + 1, :]) | (slot == goal_rows[b : b + 1, :])
        onehot[k] = hit.astype(f32).astype(bf16)

    def weighed(slots, j, shift):
        return jnp.where(
            slots == goal_cols[:, j : j + 1] + shift, weight_cols[:, j : j + 1], 0.0
        )

    slots = lax.broadcasted_iota(jnp.int32, (rows, cap), 1)
    pick_own[...] = weighed(slots, 0, 0).astype(bf16)
    slots = lax.broadcasted_iota(jnp.int32, (rows, 4 * cap), 1)
    found = weighed(slots, 1, 0) + weighed(slots, 2, 0)
    found = found + weighed(slots, 3, cap) + weighed(slots, 3, 2 * cap)
    pick_rest[...] = found.astype(bf16)

    for i in range(1, 4):
        pass_on(i)

    for load in loads[4:9]:
        load.wait()

    def pool_wait(j, carry):
        pool_copy(j).wait_recv()
        return carry

    lax.fori_loop(1, tp_count, pool_wait, 0)
    tokens[...] = gathered[...].T

    def lift_up(t, carry):
        cols = tile_of(t)
        lifted = jnp.dot(tokens[...], w_up[:, cols], preferred_element_type=f32)
        gated[:, cols] = (jax.nn.sigmoid(gate_pre[:, cols].astype(f32)) * lifted).astype(bf16)
        return carry

    lax.fori_loop(0, model_dim // TILE, lift_up, 0)

    def mix(t, carry):
        cols = tile_of(t)
        added = jnp.dot(gated[...], w_out[:, cols], preferred_element_type=f32)
        mixed[:, cols] = (resid[:, cols].astype(f32) + added).astype(bf16)
        return carry

    lax.fori_loop(0, model_dim // TILE, mix, 0)

    def norm(t, carry):
        block = pl.ds(pl.multiple_of(t * 64, 64), 64)
        x = mixed[block, :].astype(f32)
        scale = lax.rsqrt(jnp.mean(x * x, axis=-1, keepdims=True) + 1e-06)
        normed[block, :] = (x * scale * gain[...]).astype(bf16)
        return carry

    for i in range(4, 6):
        pass_on(i)
    lax.fori_loop(0, rows // 64, norm, 0)

    def pack_near(t, carry):
        cols = tile_of(t)
        send[:, cols] = jnp.dot(
            onehot[0], normed[:, cols], preferred_element_type=f32
        ).astype(bf16)
        return carry

    lax.fori_loop(0, model_dim // TILE, pack_near, 0)

    def out_copy(h, p):
        block = pl.ds((2 * h + p) * part, part)
        return remote(
            send.at[block],
            recv.at[block],
            out_go.at[2 * h + p],
            out_come.at[2 * h + p],
            {"sp": partner(sp, p + 1, count)},
        )

    def back_copy(h, p):
        block = pl.ds((2 * h + p) * part, part)
        return remote(
            result.at[block],
            back.at[block],
            ret_go.at[2 * h + p],
            ret_come.at[2 * h + p],
            {"sp": partner(sp, p + 1, count)},
        )

    chunks = [(h, p) for h in range(2) for p in range(2)]
    for h, p in chunks:
        out_copy(h, p).start()

    pass_on(6)

    def pack_local(t, carry):
        cols = tile_of(t)
        packed = jnp.dot(onehot[1], normed[:, cols], preferred_element_type=f32).astype(bf16)
        own[:, cols] = packed[:cap]
        corner[0:cap, cols] = packed[cap:]
        return carry

    lax.fori_loop(0, model_dim // TILE, pack_local, 0)
    mate = {"tp": partner(tp, 1, tp_count)}
    corner_copy = remote(
        corner.at[pl.ds(0, cap)], corner.at[pl.ds(cap, cap)], core_go.at[0], core_come.at[0], mate
    )
    corner_copy.start()
    pass_on(7)

    def activate(gate, lift):
        gate = jnp.minimum(gate, 7.0)
        lift = jnp.clip(lift, -7.0, 7.0)
        return ((lift + 1.0) * gate * jax.nn.sigmoid(1.702 * gate)).astype(bf16)

    def ffn(source, target, base):
        def up(t, carry):
            cols = tile_of(t)
            x = source[base : base + cap, :]
            act[:, cols] = activate(
                jnp.dot(x, w_gate[:, cols], preferred_element_type=f32),
                jnp.dot(x, w_lift[:, cols], preferred_element_type=f32),
            )
            return carry

        lax.fori_loop(0, hidden // TILE, up, 0)

        def down(t, carry):
            cols = tile_of(t)
            target[base : base + cap, cols] = jnp.dot(
                act[...], w_down[:, cols], preferred_element_type=f32
            ).astype(bf16)
            return carry

        lax.fori_loop(0, model_dim // TILE, down, 0)

    for load in loads[9:]:
        load.wait()
    ffn(own, local_out, 0)
    pass_on(8)

    def combine_own(t, carry):
        cols = tile_of(t)
        total[:, cols] = mixed[:, cols].astype(f32) + jnp.dot(
            pick_own[...], local_out[:, cols], preferred_element_type=f32
        )
        return carry

    lax.fori_loop(0, model_dim // TILE, combine_own, 0)
    pass_on(9)

    for h in range(2):
        for p in range(2):
            out_copy(h, p).wait_recv()
        ffn(recv, result, h * cap)
        for p in range(2):
            back_copy(h, p).start()

    corner_copy.wait_recv()
    for i in range(8):
        arrived(i)

    def corner_lift(t, carry):
        cols = tile_of(t)
        x = corner[...]
        corner_act[:, cols] = activate(
            jnp.dot(x, corner_up[0, :, cols], preferred_element_type=f32),
            jnp.dot(x, corner_up[1, :, cols], preferred_element_type=f32),
        )
        return carry

    lax.fori_loop(0, half // TILE, corner_lift, 0)
    for i in range(8, 10):
        arrived(i)

    def corner_drop(block, target, base):
        def drop(t, carry):
            cols = tile_of(t)
            target[base : base + cap, cols] = jnp.dot(
                corner_act[block * cap : (block + 1) * cap, :],
                corner_down[:, cols],
                preferred_element_type=f32,
            ).astype(bf16)
            return carry

        lax.fori_loop(0, model_dim // TILE, drop, 0)

    corner_drop(1, corner_out, 0)
    mate_copy = remote(
        corner_out, back.at[pl.ds(3 * cap, cap)], core_go.at[1], core_come.at[1], mate
    )
    mate_copy.start()
    corner_drop(0, back, 2 * cap)
    for h, p in chunks:
        back_copy(h, p).wait_recv()
    mate_copy.wait_recv()

    def combine_rest(t, carry):
        cols = tile_of(t)
        found = jnp.dot(pick_rest[...], back[:, cols], preferred_element_type=f32)
        out_ref[:, cols] = (total[:, cols] + found).astype(bf16)
        return carry

    lax.fori_loop(0, model_dim // TILE, combine_rest, 0)

    for edge in edges:
        edge.wait_send()

    def pool_sent(j, carry):
        pool_copy(j).wait_send()
        return carry

    lax.fori_loop(1, tp_count, pool_sent, 0)
    for h, p in chunks:
        out_copy(h, p).wait_send()
        back_copy(h, p).wait_send()
    corner_copy.wait_send()
    mate_copy.wait_send()
    for i in range(len(parts)):

        @pl.when(at_end)
        def _():
            fetch(i, 0).wait_send()
            share(i, 0, 1).wait_send()

        @pl.when(inside)
        def _():
            fetch(i, plane).wait_send()
            for hop in (1, 2, 3):
                share(i, plane, hop).wait_send()


def run_fused(
    count,
    tp_count,
    pool_input,
    gate_pre,
    resid,
    docs,
    w_up,
    w_out,
    g_ffn,
    w_gate,
    w_lift,
    w_down,
    routes,
    route_weight,
):
    tok_dev, channels = pool_input.shape
    rows, model_dim = resid.shape
    hidden = w_gate.shape[2]
    half = hidden // 2
    pool_w = w_up.shape[0]
    top = routes.shape[1]
    cap = capacity(rows, top, count)
    vmem = pl.BlockSpec(memory_space=pltpu.VMEM)
    bf16, f32 = jnp.bfloat16, jnp.float32
    hbm = functools.partial(pltpu.with_memory_space_constraint, memory_space=pltpu.HBM)
    dma = pltpu.SemaphoreType.DMA
    return pl.pallas_call(
        functools.partial(fused_kernel, count, tp_count),
        out_shape=jax.ShapeDtypeStruct((rows, model_dim), bf16),
        in_specs=[pl.BlockSpec(memory_space=pltpu.HBM)] * 12,
        out_specs=vmem,
        scratch_shapes=[
            pltpu.VMEM((channels, tok_dev + LANES), bf16),
            pltpu.VMEM((1, tok_dev + LANES), jnp.int32),
            pltpu.VMEM((top, rows), jnp.int32),
            pltpu.VMEM((top, rows), f32),
            pltpu.VMEM((1, model_dim), f32),
            pltpu.VMEM((rows, model_dim), bf16),
            pltpu.VMEM((rows, model_dim), bf16),
            pltpu.VMEM(w_up.shape, bf16),
            pltpu.VMEM(w_out.shape, bf16),
            pltpu.VMEM(w_gate.shape[1:], bf16),
            pltpu.VMEM(w_lift.shape[1:], bf16),
            pltpu.VMEM(w_down.shape[1:], bf16),
            pltpu.VMEM((tp_count, channels, rows), bf16),
            pltpu.VMEM((pool_w, rows), bf16),
            pltpu.VMEM((rows, pool_w), bf16),
            pltpu.VMEM((rows, model_dim), bf16),
            pltpu.VMEM((rows, model_dim), bf16),
            pltpu.VMEM((rows, model_dim), bf16),
            pltpu.VMEM((2, 2 * cap, rows), bf16),
            pltpu.VMEM((rows, cap), bf16),
            pltpu.VMEM((rows, 4 * cap), bf16),
            pltpu.VMEM((2 * cap, model_dim), bf16),
            pltpu.VMEM((2 * cap, model_dim), bf16),
            pltpu.VMEM((2 * cap, model_dim), bf16),
            pltpu.VMEM((4 * cap, model_dim), bf16),
            pltpu.VMEM((cap, model_dim), bf16),
            pltpu.VMEM((2 * cap, model_dim), bf16),
            pltpu.VMEM((cap, hidden), bf16),
            pltpu.VMEM((2 * cap, half), bf16),
            pltpu.VMEM((2, model_dim, half), bf16),
            pltpu.VMEM((half, model_dim), bf16),
            pltpu.VMEM((cap, model_dim), bf16),
            pltpu.VMEM((cap, model_dim), bf16),
            pltpu.VMEM((rows, model_dim), f32),
            dma((12,)),
            dma((2,)),
            dma((2,)),
            dma((tp_count,)),
            dma((tp_count,)),
            dma((10,)),
            dma((3, 10)),
            dma((3, 10)),
            dma((4,)),
            dma((4,)),
            dma((4,)),
            dma((4,)),
            dma((2,)),
            dma((2,)),
        ],
        compiler_params=pltpu.CompilerParams(
            collective_id=1, has_side_effects=True, vmem_limit_bytes=52 * 2**20
        ),
        cost_estimate=pl.CostEstimate(
            flops=6 * count * cap * model_dim * hidden,
            bytes_accessed=3 * model_dim * hidden * 2,
            transcendentals=count * cap * hidden,
        ),
    )(
        hbm(pool_input.T),
        hbm(docs[None, :]),
        hbm(routes.T),
        hbm(route_weight.T),
        hbm(g_ffn[None, :]),
        gate_pre,
        resid,
        w_up,
        w_out,
        w_gate,
        w_lift,
        w_down,
    )


def capacity(row_count, top_count, count):
    cap = max(2, 5 * row_count * top_count // (4 * count))
    return (cap + 15) // 16 * 16


def on_device(
    pool_input,
    gate_pre,
    resid,
    docs,
    w_up,
    w_out,
    g_ffn,
    w_gate,
    w_lift,
    w_down,
    routes,
    route_weight,
):
    tok_dev = pool_input.shape[0]
    channels = pool_input.shape[1]
    group_size = POOL_W // 4
    channel_ids = lax.axis_index("tp") * channels + lax.iota(jnp.int32, channels)
    window = jnp.power(2, channel_ids // group_size + 1)
    edge = jnp.concatenate(
        [pool_input[tok_dev - RIM :], docs[tok_dev - RIM :, None].astype(jnp.bfloat16)], axis=1
    )
    before = shifted_2(edge, "sp", 1)
    before_rows = before[:, :channels]
    before_docs = before[:, channels].astype(jnp.int32)
    first_dev = lax.axis_index("sp") == 0
    before_docs = jnp.where(first_dev, -1, before_docs)
    values = pool_input.astype(jnp.float32)
    padded = jnp.concatenate([before_rows.astype(jnp.float32), values], axis=0)
    doc_padded = jnp.concatenate([before_docs.astype(jnp.int32), docs], axis=0)
    earlier = sum(
        (doc_padded[RIM - offset : RIM - offset + tok_dev] == docs).astype(jnp.int32)
        for offset in range(1, RIM + 1)
    )
    reach = jnp.minimum(earlier[:, None] + 1, window[None, :])
    running = values
    for offset in range(1, RIM + 1):
        shifted = padded[RIM - offset : RIM - offset + tok_dev]
        running = running + jnp.where(offset < reach, shifted, 0.0)
    counts = reach.astype(jnp.float32)
    pooled = (running / counts - values).astype(jnp.bfloat16)
    tokens_pooled = lax.all_to_all(pooled, "tp", split_axis=0, concat_axis=1, tiled=True)
    lifted = jnp.dot(tokens_pooled, w_up, preferred_element_type=jnp.float32)
    gated_rows = (jax.nn.sigmoid(gate_pre.astype(jnp.float32)) * lifted).astype(jnp.bfloat16)
    mixed_rows = (
        resid.astype(jnp.float32) + jnp.dot(gated_rows, w_out, preferred_element_type=jnp.float32)
    ).astype(jnp.bfloat16)

    row_count, top_count = routes.shape
    count = lax.axis_size("sp")
    cap = capacity(row_count, top_count, count)
    order = partner(lax.axis_index("sp"), lax.iota(jnp.int32, count), count)
    chosen = routes[:, :, None] == order[None, None, :]
    named = jnp.any(chosen, axis=1)
    rank = jnp.where(named, jnp.cumsum(named.astype(jnp.int32), axis=0) - 1, -1)
    weight = jnp.sum(jnp.where(chosen, route_weight[:, :, None], 0.0), axis=1)
    return run_experts(mixed_rows, g_ffn, rank, weight, w_gate, w_lift, w_down, cap, count)


def solution(mesh):
    in_specs = (
        P("sp", "tp"),
        P(("sp", "tp"), None),
        P(("sp", "tp"), None),
        P("sp"),
        P(),
        P(),
        P(),
        P("sp", None, None),
        P("sp", None, None),
        P("sp", None, None),
        P(("sp", "tp"), None),
        P(("sp", "tp"), None),
    )
    out_specs = P(("sp", "tp"), None)
    count, tp_count = mesh.shape["sp"], mesh.shape["tp"]
    body = on_device
    if count == 4 and tp_count == 8:
        body = functools.partial(run_fused, count, tp_count)
    return jax.shard_map(
        body, mesh=mesh, in_specs=in_specs, out_specs=out_specs, check_vma=False
    )
```

```python
import functools

import jax
import jax.numpy as jnp
from jax import lax
from jax.experimental import pallas as pl
from jax.experimental.pallas import tpu as pltpu
from jax.sharding import PartitionSpec as P

POOL_W = 512
RIM = 15
TILE = 256
LANES = 128
UNIT = 16
END_SHARE = (11, 11, 12)
MESH = pl.DeviceIdType.MESH


def shifted_2(value, axis, steps):
    count = lax.axis_size(axis)
    leading, last = (max(0, -steps), min(count, count - steps))
    return lax.ppermute(value, axis, [(source, source + steps) for source in range(leading, last)])


def partner(me, step, count):
    other, bit = 0, 1
    while bit < count:
        other = other + ((me // bit + step // bit) % 2) * bit
        bit *= 2
    return other


def tile_of(t):
    return pl.ds(pl.multiple_of(t * TILE, TILE), TILE)


def experts_kernel(
    count,
    mixed_ref,
    gain_ref,
    rank_rows_ref,
    rank_cols_ref,
    weight_ref,
    w_gate_hbm,
    w_lift_hbm,
    w_down_hbm,
    out_ref,
    normed,
    onehot,
    send,
    recv,
    result,
    back,
    total,
    act,
    w_gate,
    w_lift,
    w_down,
    weight_sems,
    go_sems,
    come_sems,
    ret_go_sems,
    ret_come_sems,
):
    rows, model_dim = mixed_ref.shape
    cap = send.shape[1]
    hidden = w_gate.shape[1]
    me = lax.axis_index("sp")
    loads = [
        pltpu.make_async_copy(src.at[0], dst, weight_sems.at[i])
        for i, (src, dst) in enumerate(
            ((w_gate_hbm, w_gate), (w_lift_hbm, w_lift), (w_down_hbm, w_down))
        )
    ]

    barrier = pltpu.get_barrier_semaphore()

    def greet(j, carry):
        pl.semaphore_signal(
            barrier, inc=1, device_id={"sp": partner(me, j, count)}, device_id_type=MESH
        )
        return carry

    lax.fori_loop(1, count, greet, 0)
    for load in loads:
        load.start()

    def norm(t, carry):
        block = pl.ds(pl.multiple_of(t * 64, 64), 64)
        x = mixed_ref[block, :].astype(jnp.float32)
        scale = lax.rsqrt(jnp.mean(x * x, axis=-1, keepdims=True) + 1e-06)
        normed[block, :] = (x * scale * gain_ref[...]).astype(jnp.bfloat16)
        return carry

    lax.fori_loop(0, rows // 64, norm, 0)

    def out_copy(j):
        return pltpu.make_async_remote_copy(
            src_ref=send.at[j],
            dst_ref=recv.at[j],
            send_sem=go_sems.at[j],
            recv_sem=come_sems.at[j],
            device_id={"sp": partner(me, j, count)},
            device_id_type=MESH,
        )

    def back_copy(j):
        return pltpu.make_async_remote_copy(
            src_ref=result.at[j],
            dst_ref=back.at[j],
            send_sem=ret_go_sems.at[j],
            recv_sem=ret_come_sems.at[j],
            device_id={"sp": partner(me, j, count)},
            device_id_type=MESH,
        )

    def pack(j, target):
        slot = lax.broadcasted_iota(jnp.int32, (cap, rows), 0)
        onehot[...] = (slot == rank_rows_ref[j]).astype(jnp.float32).astype(jnp.bfloat16)

        def piece(t, carry):
            cols = tile_of(t)
            target[j, :, cols] = jnp.dot(
                onehot[...], normed[:, cols], preferred_element_type=jnp.float32
            ).astype(jnp.bfloat16)
            return carry

        lax.fori_loop(0, model_dim // TILE, piece, 0)

    def ffn(j, source):
        def up(t, carry):
            cols = tile_of(t)
            x = source[j]
            gate = jnp.minimum(jnp.dot(x, w_gate[:, cols], preferred_element_type=jnp.float32), 7.0)
            lift = jnp.clip(
                jnp.dot(x, w_lift[:, cols], preferred_element_type=jnp.float32), -7.0, 7.0
            )
            act[:, cols] = ((lift + 1.0) * gate * jax.nn.sigmoid(1.702 * gate)).astype(jnp.bfloat16)
            return carry

        lax.fori_loop(0, hidden // TILE, up, 0)

        def down(t, carry):
            cols = tile_of(t)
            result[j, :, cols] = jnp.dot(
                act[...], w_down[:, cols], preferred_element_type=jnp.float32
            ).astype(jnp.bfloat16)
            return carry

        lax.fori_loop(0, model_dim // TILE, down, 0)

    def column(ref, j):
        lane = lax.broadcasted_iota(jnp.int32, ref.shape, 1)
        return jnp.sum(jnp.where(lane == j, ref[...], 0.0), axis=1, keepdims=True)

    def combine(j, source, store):
        rank = column(rank_cols_ref, j).astype(jnp.int32)
        weight = column(weight_ref, j)
        slot = lax.broadcasted_iota(jnp.int32, (rows, cap), 1)
        pick = (slot == rank).astype(jnp.float32).astype(jnp.bfloat16)

        def piece(t, carry):
            cols = tile_of(t)
            found = jnp.dot(pick, source[j, :, cols], preferred_element_type=jnp.float32)
            store(cols, weight * found)
            return carry

        lax.fori_loop(0, model_dim // TILE, piece, 0)

    def store_first(cols, term):
        total[:, cols] = mixed_ref[:, cols].astype(jnp.float32) + term

    def store_more(cols, term):
        total[:, cols] = total[:, cols] + term

    def store_last(cols, term):
        out_ref[:, cols] = (total[:, cols] + term).astype(jnp.bfloat16)

    pl.semaphore_wait(barrier, count - 1)

    def dispatch(j, carry):
        pack(j, send)
        out_copy(j).start()
        return carry

    lax.fori_loop(1, count, dispatch, 0)
    pack(0, send)
    for load in loads:
        load.wait()
    ffn(0, send)
    combine(0, result, store_first)

    def serve(j, carry):
        out_copy(j).wait_recv()
        ffn(j, recv)
        back_copy(j).start()
        return carry

    lax.fori_loop(1, count, serve, 0)

    def gather(j, carry):
        back_copy(j).wait_recv()
        combine(j, back, store_more)
        return carry

    lax.fori_loop(1, count - 1, gather, 0)
    back_copy(count - 1).wait_recv()
    combine(count - 1, back, store_last)

    def finish(j, carry):
        out_copy(j).wait_send()
        back_copy(j).wait_send()
        return carry

    lax.fori_loop(1, count, finish, 0)


def run_experts(mixed, gain, rank, weight, w_gate, w_lift, w_down, cap, count):
    rows, model_dim = mixed.shape
    hidden = w_gate.shape[2]
    vmem = pl.BlockSpec(memory_space=pltpu.VMEM)
    anywhere = pl.BlockSpec(memory_space=pl.ANY)
    slots = pltpu.VMEM((count, cap, model_dim), jnp.bfloat16)
    return pl.pallas_call(
        functools.partial(experts_kernel, count),
        out_shape=jax.ShapeDtypeStruct((rows, model_dim), jnp.bfloat16),
        in_specs=[vmem] * 5 + [anywhere] * 3,
        out_specs=vmem,
        scratch_shapes=[
            pltpu.VMEM((rows, model_dim), jnp.bfloat16),
            pltpu.VMEM((cap, rows), jnp.bfloat16),
            slots,
            slots,
            slots,
            slots,
            pltpu.VMEM((rows, model_dim), jnp.float32),
            pltpu.VMEM((cap, hidden), jnp.bfloat16),
            pltpu.VMEM(w_gate.shape[1:], jnp.bfloat16),
            pltpu.VMEM(w_lift.shape[1:], jnp.bfloat16),
            pltpu.VMEM(w_down.shape[1:], jnp.bfloat16),
            pltpu.SemaphoreType.DMA((3,)),
            pltpu.SemaphoreType.DMA((count,)),
            pltpu.SemaphoreType.DMA((count,)),
            pltpu.SemaphoreType.DMA((count,)),
            pltpu.SemaphoreType.DMA((count,)),
        ],
        compiler_params=pltpu.CompilerParams(
            collective_id=0, has_side_effects=True, vmem_limit_bytes=60 * 2**20
        ),
        cost_estimate=pl.CostEstimate(
            flops=6 * count * cap * model_dim * hidden,
            bytes_accessed=3 * model_dim * hidden * 2,
            transcendentals=count * cap * hidden,
        ),
    )(
        mixed,
        gain[None, :],
        rank.T[:, None, :],
        rank.astype(jnp.float32),
        weight,
        w_gate,
        w_lift,
        w_down,
    )


def fused_kernel(
    count,
    tp_count,
    pool_hbm,
    docs_hbm,
    routes_hbm,
    route_weight_hbm,
    gain_hbm,
    gate_hbm,
    resid_hbm,
    w_up_hbm,
    w_out_hbm,
    w_gate_hbm,
    w_lift_hbm,
    w_down_hbm,
    out_ref,
    pool,
    docs,
    routes_ref,
    route_weight_ref,
    gain,
    gate_pre,
    resid,
    w_up,
    w_out,
    w_gate,
    w_lift,
    w_down,
    pooled,
    gathered,
    tokens,
    gated,
    mixed,
    normed,
    onehot,
    pick_own,
    pick_rest,
    send,
    recv,
    result,
    back,
    own,
    corner,
    act,
    corner_act,
    corner_up,
    corner_down,
    corner_out,
    local_out,
    total,
    load_sems,
    edge_go,
    edge_come,
    pool_go,
    pool_come,
    part_go,
    part_come,
    share_go,
    out_go,
    out_come,
    ret_go,
    ret_come,
    late_go,
    late_come,
    mate_go,
    mate_come,
    core_go,
    core_come,
):
    channels = pool_hbm.shape[0]
    rows, model_dim = resid.shape
    hidden = w_gate.shape[1]
    half = hidden // 2
    cap = own.shape[0]
    part = cap // 2
    sp, tp = lax.axis_index("sp"), lax.axis_index("tp")
    plane, core = tp // 2, tp % 2
    planes = tp_count // 2
    at_end = (plane == 0) | (plane == planes - 1)
    inside = (plane > 0) & (plane < planes - 1)
    f32, bf16 = jnp.float32, jnp.bfloat16

    loads = [
        pltpu.make_async_copy(src, dst, load_sems.at[i])
        for i, (src, dst) in enumerate(
            (
                (pool_hbm, pool.at[:, LANES:]),
                (docs_hbm, docs.at[:, LANES:]),
                (w_gate_hbm.at[0], w_gate),
                (w_lift_hbm.at[0], w_lift),
                (w_down_hbm.at[0], w_down),
                (routes_hbm, routes_ref),
                (route_weight_hbm, route_weight_ref),
                (w_up_hbm, w_up),
                (gate_hbm, gate_pre),
                (w_out_hbm, w_out),
                (resid_hbm, resid),
                (gain_hbm, gain),
            )
        )
    ]
    for load in loads:
        load.start()
    barrier = pltpu.get_barrier_semaphore()

    def greet_sp(j, carry):
        pl.semaphore_signal(
            barrier, inc=1, device_id={"sp": partner(sp, j, count)}, device_id_type=MESH
        )
        return carry

    def greet_tp(j, carry):
        pl.semaphore_signal(
            barrier, inc=1, device_id={"tp": partner(tp, j, tp_count)}, device_id_type=MESH
        )
        return carry

    lax.fori_loop(1, count, greet_sp, 0)
    lax.fori_loop(1, tp_count, greet_tp, 0)
    def remote(src, dst, go, come, device):
        return pltpu.make_async_remote_copy(
            src_ref=src,
            dst_ref=dst,
            send_sem=go,
            recv_sem=come,
            device_id=device,
            device_id_type=MESH,
        )

    following = {"sp": lax.rem(sp + 1, count)}
    tok_dev = pool_hbm.shape[1]
    edges = [
        remote(
            ref.at[:, pl.ds(tok_dev, LANES)],
            ref.at[:, pl.ds(0, LANES)],
            edge_go.at[i],
            edge_come.at[i],
            following,
        )
        for i, ref in enumerate((pool, docs))
    ]

    pieces = [(m, q) for q in range(4) for m in range(2)] + [(2, q) for q in range(4)]
    sources = (w_gate, w_lift, w_down)
    far = partner(sp, 3, count)

    def span(m, q, zone):
        units = (model_dim if m < 2 else half) // UNIT
        ends = units * END_SHARE[m] // 32
        inner = (units - ends) // 2
        is_end = isinstance(zone, int) and zone == 0
        size = ends if is_end else inner
        low, high = (q * size // 4, (q + 1) * size // 4) if m < 2 else (0, size)
        if is_end:
            return low * UNIT, (high - low) * UNIT
        start = (ends + inner * (zone - 1) + low) * UNIT
        return pl.multiple_of(start, UNIT), (high - low) * UNIT

    def place(m, q, start, size):
        if m < 2:
            return corner_up.at[m, pl.ds(start, size), :]
        return corner_down.at[pl.ds(start, size), pl.ds(q * TILE, TILE)]

    def fetch(i, zone):
        m, q = pieces[i]
        start, size = span(m, q, zone)
        if m < 2:
            cols = pl.ds(pl.multiple_of(core * half, half), half)
            src = sources[m].at[pl.ds(start, size), cols]
        else:
            first = pl.multiple_of(core * half + start, UNIT)
            src = sources[m].at[pl.ds(first, size), pl.ds(q * TILE, TILE)]
        return remote(
            src,
            place(m, q, start, size),
            part_go.at[i],
            part_come.at[zone, i],
            {"sp": far},
        )

    def share(i, zone, way):
        m, q = pieces[i]
        start, size = span(m, q, zone)
        return remote(
            place(m, q, start, size),
            place(m, q, start, size),
            share_go.at[way, i],
            part_come.at[zone, i],
            {"tp": partner(tp, 6 if way == 1 else 2, tp_count)},
        )

    def pass_on(i):
        @pl.when(at_end)
        def _():
            fetch(i, 0).wait_recv()
            share(i, 0, 0).start()

        @pl.when(inside)
        def _():
            fetch(i, plane).wait_recv()
            share(i, plane, 1).start()
            share(i, plane, 0).start()

    def relay(i):
        @pl.when(inside)
        def _():
            share(i, 3 - plane, 1).wait_recv()
            share(i, 3 - plane, 2).start()

    def arrived(i):
        @pl.when(at_end)
        def _():
            share(i, 1, 0).wait_recv()
            share(i, 2, 0).wait_recv()

        @pl.when(inside)
        def _():
            share(i, 0, 0).wait_recv()

    def fetch_all(some):
        @pl.when(at_end)
        def _():
            for i in some:
                fetch(i, 0).start()

        @pl.when(inside)
        def _():
            for i in some:
                fetch(i, plane).start()

    for load in loads[:2]:
        load.wait()
    pl.semaphore_wait(barrier, count - 1 + tp_count - 1)
    for edge in edges:
        edge.start()

    for load in loads[2:4]:
        load.wait()
    fetch_all(range(8))

    level = (tp * channels) // (channels * tp_count // 4)

    def pool_copy(j):
        return remote(
            pooled.at[j],
            gathered.at[pl.ds(pl.multiple_of(tp * channels, channels), channels), :],
            pool_go.at[j],
            pool_come.at[j],
            {"tp": partner(tp, j, tp_count)},
        )

    def pool_block(j):
        owner = partner(tp, j, tp_count)
        cols = pl.ds(pl.multiple_of(owner * rows, LANES), rows + LANES)
        values = pool[:, cols].astype(f32)
        document = jnp.broadcast_to(docs[:, cols], (8, rows + LANES))
        lane = lax.broadcasted_iota(jnp.int32, document.shape, 1)
        document = jnp.where((lane < LANES) & (owner == 0) & (sp == 0), -1, document)
        running = values
        number = jnp.ones(document.shape, f32)
        for step in range(4):
            shift = 2**step
            same = (document == pltpu.roll(document, shift, 1)) & (level >= step)
            same = same.astype(f32)
            number = number + same * pltpu.roll(number, shift, 1)
            wide = jnp.concatenate([same] * (channels // 8), axis=0)
            running = running + wide * pltpu.roll(running, shift, 1)
        share_of = jnp.concatenate([1.0 / number] * (channels // 8), axis=0)
        return (running * share_of - values)[:, LANES:].astype(bf16)

    def pool_send(j):
        pooled[j] = pool_block(j)
        pool_copy(j).start()

    def pool_step(i, carry):
        j = tp_count - 1 - i

        @pl.when(j != tp)
        def _():
            pool_send(j)

        return carry

    lax.fori_loop(0, tp_count - 1, pool_step, 0)
    loads[4].wait()
    fetch_all(range(8, 12))
    for edge in edges:
        edge.wait_recv()

    @pl.when(tp != 0)
    def _():
        pool_send(tp)

    gathered[pl.ds(pl.multiple_of(tp * channels, channels), channels), :] = pool_block(0)
    pass_on(0)

    for load in loads[5:7]:
        load.wait()

    first, second = routes_ref[0:1, :], routes_ref[1:2, :]
    weight_first, weight_second = route_weight_ref[0:1, :], route_weight_ref[1:2, :]
    named, weights = [], []
    for j in range(count):
        expert = partner(sp, j, count)
        named.append(jnp.where((first == expert) | (second == expert), 1.0, 0.0))
        weights.append(
            jnp.where(first == expert, weight_first, 0.0)
            + jnp.where(second == expert, weight_second, 0.0)
        )
    named = jnp.concatenate(named + named, axis=0)
    weights = jnp.concatenate(weights + weights, axis=0)
    before = lax.broadcasted_iota(jnp.int32, (rows, rows), 0) <= lax.broadcasted_iota(
        jnp.int32, (rows, rows), 1
    )
    place_of = jnp.dot(
        named.astype(bf16), before.astype(f32).astype(bf16), preferred_element_type=f32
    )
    place_of = jnp.where(named > 0.0, place_of - 1.0, -4.0 * cap)
    split = jnp.where(place_of >= part, place_of + part, place_of)
    line = lax.broadcasted_iota(jnp.int32, place_of.shape, 0)
    goal = jnp.where(line == 1, split, place_of)
    goal = jnp.where(line == 2, split + part, goal)
    goal = jnp.where(line == 3, place_of + cap, goal)
    goal_rows = goal.astype(jnp.int32)
    goal_cols = goal.T.astype(jnp.int32)
    weight_cols = weights.T

    slot = lax.broadcasted_iota(jnp.int32, (2 * cap, rows), 0)
    for k, (a, b) in enumerate(((1, 2), (0, 3))):
        hit = (slot == goal_rows[a : a + 1, :]) | (slot == goal_rows[b : b + 1, :])
        onehot[k] = hit.astype(f32).astype(bf16)

    def weighed(slots, j, shift):
        return jnp.where(
            slots == goal_cols[:, j : j + 1] + shift, weight_cols[:, j : j + 1], 0.0
        )

    slots = lax.broadcasted_iota(jnp.int32, (rows, cap), 1)
    pick_own[...] = weighed(slots, 0, 0).astype(bf16)
    slots = lax.broadcasted_iota(jnp.int32, (rows, 4 * cap), 1)
    found = weighed(slots, 1, 0) + weighed(slots, 2, 0)
    found = found + weighed(slots, 3, cap) + weighed(slots, 3, 2 * cap)
    pick_rest[...] = found.astype(bf16)

    for i in range(1, 4):
        pass_on(i)

    for load in loads[7:]:
        load.wait()

    def pool_wait(j, carry):
        pool_copy(j).wait_recv()
        return carry

    lax.fori_loop(1, tp_count, pool_wait, 0)
    tokens[...] = gathered[...].T

    def lift_up(t, carry):
        cols = tile_of(t)
        lifted = jnp.dot(tokens[...], w_up[:, cols], preferred_element_type=f32)
        gated[:, cols] = (jax.nn.sigmoid(gate_pre[:, cols].astype(f32)) * lifted).astype(bf16)
        return carry

    lax.fori_loop(0, model_dim // TILE, lift_up, 0)

    def mix(t, carry):
        cols = tile_of(t)
        added = jnp.dot(gated[...], w_out[:, cols], preferred_element_type=f32)
        mixed[:, cols] = (resid[:, cols].astype(f32) + added).astype(bf16)
        return carry

    lax.fori_loop(0, model_dim // TILE, mix, 0)

    def norm(t, carry):
        block = pl.ds(pl.multiple_of(t * 64, 64), 64)
        x = mixed[block, :].astype(f32)
        scale = lax.rsqrt(jnp.mean(x * x, axis=-1, keepdims=True) + 1e-06)
        normed[block, :] = (x * scale * gain[...]).astype(bf16)
        return carry

    for i in range(4, 6):
        pass_on(i)
    lax.fori_loop(0, rows // 64, norm, 0)

    def pack_near(t, carry):
        cols = tile_of(t)
        send[:, cols] = jnp.dot(
            onehot[0], normed[:, cols], preferred_element_type=f32
        ).astype(bf16)
        return carry

    lax.fori_loop(0, model_dim // TILE, pack_near, 0)

    def out_copy(h, p):
        block = pl.ds((2 * h + p) * part, part)
        return remote(
            send.at[block],
            recv.at[block],
            out_go.at[2 * h + p],
            out_come.at[2 * h + p],
            {"sp": partner(sp, p + 1, count)},
        )

    def back_copy(p):
        block = pl.ds(p * part, part)
        return remote(
            result.at[block],
            back.at[block],
            ret_go.at[p],
            ret_come.at[p],
            {"sp": partner(sp, p + 1, count)},
        )

    def late_copy(p, t):
        block = pl.ds((2 + p) * part, part)
        return remote(
            result.at[block, tile_of(t)],
            back.at[block, tile_of(t)],
            late_go.at[p, t],
            late_come.at[p, t],
            {"sp": partner(sp, p + 1, count)},
        )

    chunks = [(h, p) for h in range(2) for p in range(2)]
    for h, p in chunks:
        out_copy(h, p).start()

    pass_on(6)

    def pack_local(t, carry):
        cols = tile_of(t)
        packed = jnp.dot(onehot[1], normed[:, cols], preferred_element_type=f32).astype(bf16)
        own[:, cols] = packed[:cap]
        corner[0:cap, cols] = packed[cap:]
        return carry

    lax.fori_loop(0, model_dim // TILE, pack_local, 0)
    mate = {"tp": partner(tp, 1, tp_count)}
    corner_copy = remote(
        corner.at[pl.ds(0, cap)], corner.at[pl.ds(cap, cap)], core_go.at[0], core_come.at[0], mate
    )
    corner_copy.start()
    pass_on(7)

    def activate(gate, lift):
        gate = jnp.minimum(gate, 7.0)
        lift = jnp.clip(lift, -7.0, 7.0)
        return ((lift + 1.0) * gate * jax.nn.sigmoid(1.702 * gate)).astype(bf16)

    def ffn(source, target, base, then=lambda t: None):
        def up(t, carry):
            cols = tile_of(t)
            x = source[base : base + cap, :]
            act[:, cols] = activate(
                jnp.dot(x, w_gate[:, cols], preferred_element_type=f32),
                jnp.dot(x, w_lift[:, cols], preferred_element_type=f32),
            )
            return carry

        lax.fori_loop(0, hidden // TILE, up, 0)

        def down(t, carry):
            cols = tile_of(t)
            target[base : base + cap, cols] = jnp.dot(
                act[...], w_down[:, cols], preferred_element_type=f32
            ).astype(bf16)
            then(t)
            return carry

        lax.fori_loop(0, model_dim // TILE, down, 0)

    ffn(own, local_out, 0)
    pass_on(8)
    pass_on(9)

    def combine_own(t, carry):
        cols = tile_of(t)
        total[:, cols] = mixed[:, cols].astype(f32) + jnp.dot(
            pick_own[...], local_out[:, cols], preferred_element_type=f32
        )
        return carry

    lax.fori_loop(0, model_dim // TILE, combine_own, 0)
    pass_on(10)
    pass_on(11)
    for i in range(8):
        relay(i)

    for p in range(2):
        out_copy(0, p).wait_recv()
    ffn(recv, result, 0)
    for p in range(2):
        back_copy(p).start()
    for i in range(8, 12):
        relay(i)
    for p in range(2):
        out_copy(1, p).wait_recv()

    def send_back(t):
        for p in range(2):
            late_copy(p, t).start()

    ffn(recv, result, cap, send_back)

    corner_copy.wait_recv()
    for i in range(8):
        arrived(i)

    def corner_lift(t, carry):
        cols = tile_of(t)
        x = corner[...]
        corner_act[:, cols] = activate(
            jnp.dot(x, corner_up[0, :, cols], preferred_element_type=f32),
            jnp.dot(x, corner_up[1, :, cols], preferred_element_type=f32),
        )
        return carry

    lax.fori_loop(0, half // TILE, corner_lift, 0)
    def mate_copy(t):
        return remote(
            corner_out.at[:, tile_of(t)],
            back.at[pl.ds(3 * cap, cap), tile_of(t)],
            mate_go.at[t],
            mate_come.at[t],
            mate,
        )

    def corner_drop(t):
        cols = tile_of(t)
        for block, target, base in ((1, corner_out, 0), (0, back, 2 * cap)):
            target[base : base + cap, cols] = jnp.dot(
                corner_act[block * cap : (block + 1) * cap, :],
                corner_down[:, cols],
                preferred_element_type=f32,
            ).astype(bf16)
            if block == 1:
                mate_copy(t).start()

    def combine_rest(t):
        cols = tile_of(t)
        for p in range(2):
            late_copy(p, t).wait_recv()
        mate_copy(t).wait_recv()
        found = jnp.dot(pick_rest[...], back[:, cols], preferred_element_type=f32)
        out_ref[:, cols] = (total[:, cols] + found).astype(bf16)

    tiles = model_dim // TILE
    for p in range(2):
        back_copy(p).wait_recv()
    for t in range(tiles):
        arrived(8 + t)
        corner_drop(t)
        if t > 0:
            combine_rest(t - 1)
    combine_rest(tiles - 1)

    for edge in edges:
        edge.wait_send()

    def pool_sent(j, carry):
        pool_copy(j).wait_send()
        return carry

    lax.fori_loop(1, tp_count, pool_sent, 0)
    for h, p in chunks:
        out_copy(h, p).wait_send()
    corner_copy.wait_send()
    for p in range(2):
        back_copy(p).wait_send()

    def late_sent(t, carry):
        mate_copy(t).wait_send()
        for p in range(2):
            late_copy(p, t).wait_send()
        return carry

    lax.fori_loop(0, tiles, late_sent, 0)

    @pl.when(at_end)
    def _():
        for i in range(len(pieces)):
            fetch(i, 0).wait_send()
            share(i, 0, 0).wait_send()

    @pl.when(inside)
    def _():
        for i in range(len(pieces)):
            fetch(i, plane).wait_send()
            for way in range(2):
                share(i, plane, way).wait_send()
            share(i, 3 - plane, 2).wait_send()


def run_fused(
    count,
    tp_count,
    pool_input,
    gate_pre,
    resid,
    docs,
    w_up,
    w_out,
    g_ffn,
    w_gate,
    w_lift,
    w_down,
    routes,
    route_weight,
):
    tok_dev, channels = pool_input.shape
    rows, model_dim = resid.shape
    hidden = w_gate.shape[2]
    half = hidden // 2
    pool_w = w_up.shape[0]
    top = routes.shape[1]
    cap = capacity(rows, top, count)
    vmem = pl.BlockSpec(memory_space=pltpu.VMEM)
    bf16, f32 = jnp.bfloat16, jnp.float32
    hbm = functools.partial(pltpu.with_memory_space_constraint, memory_space=pltpu.HBM)
    dma = pltpu.SemaphoreType.DMA
    return pl.pallas_call(
        functools.partial(fused_kernel, count, tp_count),
        out_shape=jax.ShapeDtypeStruct((rows, model_dim), bf16),
        in_specs=[pl.BlockSpec(memory_space=pltpu.HBM)] * 12,
        out_specs=vmem,
        scratch_shapes=[
            pltpu.VMEM((channels, tok_dev + LANES), bf16),
            pltpu.VMEM((1, tok_dev + LANES), jnp.int32),
            pltpu.VMEM((top, rows), jnp.int32),
            pltpu.VMEM((top, rows), f32),
            pltpu.VMEM((1, model_dim), f32),
            pltpu.VMEM((rows, model_dim), bf16),
            pltpu.VMEM((rows, model_dim), bf16),
            pltpu.VMEM(w_up.shape, bf16),
            pltpu.VMEM(w_out.shape, bf16),
            pltpu.VMEM(w_gate.shape[1:], bf16),
            pltpu.VMEM(w_lift.shape[1:], bf16),
            pltpu.VMEM(w_down.shape[1:], bf16),
            pltpu.VMEM((tp_count, channels, rows), bf16),
            pltpu.VMEM((pool_w, rows), bf16),
            pltpu.VMEM((rows, pool_w), bf16),
            pltpu.VMEM((rows, model_dim), bf16),
            pltpu.VMEM((rows, model_dim), bf16),
            pltpu.VMEM((rows, model_dim), bf16),
            pltpu.VMEM((2, 2 * cap, rows), bf16),
            pltpu.VMEM((rows, cap), bf16),
            pltpu.VMEM((rows, 4 * cap), bf16),
            pltpu.VMEM((2 * cap, model_dim), bf16),
            pltpu.VMEM((2 * cap, model_dim), bf16),
            pltpu.VMEM((2 * cap, model_dim), bf16),
            pltpu.VMEM((4 * cap, model_dim), bf16),
            pltpu.VMEM((cap, model_dim), bf16),
            pltpu.VMEM((2 * cap, model_dim), bf16),
            pltpu.VMEM((cap, hidden), bf16),
            pltpu.VMEM((2 * cap, half), bf16),
            pltpu.VMEM((2, model_dim, half), bf16),
            pltpu.VMEM((half, model_dim), bf16),
            pltpu.VMEM((cap, model_dim), bf16),
            pltpu.VMEM((cap, model_dim), bf16),
            pltpu.VMEM((rows, model_dim), f32),
            dma((12,)),
            dma((2,)),
            dma((2,)),
            dma((tp_count,)),
            dma((tp_count,)),
            dma((12,)),
            dma((3, 12)),
            dma((3, 12)),
            dma((4,)),
            dma((4,)),
            dma((2,)),
            dma((2,)),
            dma((2, 4)),
            dma((2, 4)),
            dma((4,)),
            dma((4,)),
            dma((1,)),
            dma((1,)),
        ],
        compiler_params=pltpu.CompilerParams(
            collective_id=1, has_side_effects=True, vmem_limit_bytes=52 * 2**20
        ),
        cost_estimate=pl.CostEstimate(
            flops=6 * count * cap * model_dim * hidden,
            bytes_accessed=3 * model_dim * hidden * 2,
            transcendentals=count * cap * hidden,
        ),
    )(
        hbm(pool_input.T),
        hbm(docs[None, :]),
        hbm(routes.T),
        hbm(route_weight.T),
        hbm(g_ffn[None, :]),
        gate_pre,
        resid,
        w_up,
        w_out,
        w_gate,
        w_lift,
        w_down,
    )


def capacity(row_count, top_count, count):
    cap = max(2, 5 * row_count * top_count // (4 * count))
    return (cap + 15) // 16 * 16


def on_device(
    pool_input,
    gate_pre,
    resid,
    docs,
    w_up,
    w_out,
    g_ffn,
    w_gate,
    w_lift,
    w_down,
    routes,
    route_weight,
):
    tok_dev = pool_input.shape[0]
    channels = pool_input.shape[1]
    group_size = POOL_W // 4
    channel_ids = lax.axis_index("tp") * channels + lax.iota(jnp.int32, channels)
    window = jnp.power(2, channel_ids // group_size + 1)
    edge = jnp.concatenate(
        [pool_input[tok_dev - RIM :], docs[tok_dev - RIM :, None].astype(jnp.bfloat16)], axis=1
    )
    before = shifted_2(edge, "sp", 1)
    before_rows = before[:, :channels]
    before_docs = before[:, channels].astype(jnp.int32)
    first_dev = lax.axis_index("sp") == 0
    before_docs = jnp.where(first_dev, -1, before_docs)
    values = pool_input.astype(jnp.float32)
    padded = jnp.concatenate([before_rows.astype(jnp.float32), values], axis=0)
    doc_padded = jnp.concatenate([before_docs.astype(jnp.int32), docs], axis=0)
    earlier = sum(
        (doc_padded[RIM - offset : RIM - offset + tok_dev] == docs).astype(jnp.int32)
        for offset in range(1, RIM + 1)
    )
    reach = jnp.minimum(earlier[:, None] + 1, window[None, :])
    running = values
    for offset in range(1, RIM + 1):
        shifted = padded[RIM - offset : RIM - offset + tok_dev]
        running = running + jnp.where(offset < reach, shifted, 0.0)
    counts = reach.astype(jnp.float32)
    pooled = (running / counts - values).astype(jnp.bfloat16)
    tokens_pooled = lax.all_to_all(pooled, "tp", split_axis=0, concat_axis=1, tiled=True)
    lifted = jnp.dot(tokens_pooled, w_up, preferred_element_type=jnp.float32)
    gated_rows = (jax.nn.sigmoid(gate_pre.astype(jnp.float32)) * lifted).astype(jnp.bfloat16)
    mixed_rows = (
        resid.astype(jnp.float32) + jnp.dot(gated_rows, w_out, preferred_element_type=jnp.float32)
    ).astype(jnp.bfloat16)

    row_count, top_count = routes.shape
    count = lax.axis_size("sp")
    cap = capacity(row_count, top_count, count)
    order = partner(lax.axis_index("sp"), lax.iota(jnp.int32, count), count)
    chosen = routes[:, :, None] == order[None, None, :]
    named = jnp.any(chosen, axis=1)
    rank = jnp.where(named, jnp.cumsum(named.astype(jnp.int32), axis=0) - 1, -1)
    weight = jnp.sum(jnp.where(chosen, route_weight[:, :, None], 0.0), axis=1)
    return run_experts(mixed_rows, g_ffn, rank, weight, w_gate, w_lift, w_down, cap, count)


def solution(mesh):
    in_specs = (
        P("sp", "tp"),
        P(("sp", "tp"), None),
        P(("sp", "tp"), None),
        P("sp"),
        P(),
        P(),
        P(),
        P("sp", None, None),
        P("sp", None, None),
        P("sp", None, None),
        P(("sp", "tp"), None),
        P(("sp", "tp"), None),
    )
    out_specs = P(("sp", "tp"), None)
    count, tp_count = mesh.shape["sp"], mesh.shape["tp"]
    body = on_device
    if count == 4 and tp_count == 8:
        body = functools.partial(run_fused, count, tp_count)
    return jax.shard_map(
        body, mesh=mesh, in_specs=in_specs, out_specs=out_specs, check_vma=False
    )
```

```python
import functools

import jax
import jax.numpy as jnp
from jax import lax
from jax.experimental import pallas as pl
from jax.experimental.pallas import tpu as pltpu
from jax.sharding import PartitionSpec as P

POOL_W = 512
RIM = 15
TILE = 256
LANES = 128
UNIT = 16
END_SHARE = (11, 11, 12)
MESH = pl.DeviceIdType.MESH


def shifted_2(value, axis, steps):
    count = lax.axis_size(axis)
    leading, last = (max(0, -steps), min(count, count - steps))
    return lax.ppermute(value, axis, [(source, source + steps) for source in range(leading, last)])


def partner(me, step, count):
    other, bit = 0, 1
    while bit < count:
        other = other + ((me // bit + step // bit) % 2) * bit
        bit *= 2
    return other


def tile_of(t):
    return pl.ds(pl.multiple_of(t * TILE, TILE), TILE)


def experts_kernel(
    count,
    mixed_ref,
    gain_ref,
    rank_rows_ref,
    rank_cols_ref,
    weight_ref,
    w_gate_hbm,
    w_lift_hbm,
    w_down_hbm,
    out_ref,
    normed,
    onehot,
    send,
    recv,
    result,
    back,
    total,
    act,
    w_gate,
    w_lift,
    w_down,
    weight_sems,
    go_sems,
    come_sems,
    ret_go_sems,
    ret_come_sems,
):
    rows, model_dim = mixed_ref.shape
    cap = send.shape[1]
    hidden = w_gate.shape[1]
    me = lax.axis_index("sp")
    loads = [
        pltpu.make_async_copy(src.at[0], dst, weight_sems.at[i])
        for i, (src, dst) in enumerate(
            ((w_gate_hbm, w_gate), (w_lift_hbm, w_lift), (w_down_hbm, w_down))
        )
    ]

    barrier = pltpu.get_barrier_semaphore()

    def greet(j, carry):
        pl.semaphore_signal(
            barrier, inc=1, device_id={"sp": partner(me, j, count)}, device_id_type=MESH
        )
        return carry

    lax.fori_loop(1, count, greet, 0)
    for load in loads:
        load.start()

    def norm(t, carry):
        block = pl.ds(pl.multiple_of(t * 64, 64), 64)
        x = mixed_ref[block, :].astype(jnp.float32)
        scale = lax.rsqrt(jnp.mean(x * x, axis=-1, keepdims=True) + 1e-06)
        normed[block, :] = (x * scale * gain_ref[...]).astype(jnp.bfloat16)
        return carry

    lax.fori_loop(0, rows // 64, norm, 0)

    def out_copy(j):
        return pltpu.make_async_remote_copy(
            src_ref=send.at[j],
            dst_ref=recv.at[j],
            send_sem=go_sems.at[j],
            recv_sem=come_sems.at[j],
            device_id={"sp": partner(me, j, count)},
            device_id_type=MESH,
        )

    def back_copy(j):
        return pltpu.make_async_remote_copy(
            src_ref=result.at[j],
            dst_ref=back.at[j],
            send_sem=ret_go_sems.at[j],
            recv_sem=ret_come_sems.at[j],
            device_id={"sp": partner(me, j, count)},
            device_id_type=MESH,
        )

    def pack(j, target):
        slot = lax.broadcasted_iota(jnp.int32, (cap, rows), 0)
        onehot[...] = (slot == rank_rows_ref[j]).astype(jnp.float32).astype(jnp.bfloat16)

        def piece(t, carry):
            cols = tile_of(t)
            target[j, :, cols] = jnp.dot(
                onehot[...], normed[:, cols], preferred_element_type=jnp.float32
            ).astype(jnp.bfloat16)
            return carry

        lax.fori_loop(0, model_dim // TILE, piece, 0)

    def ffn(j, source):
        def up(t, carry):
            cols = tile_of(t)
            x = source[j]
            gate = jnp.minimum(jnp.dot(x, w_gate[:, cols], preferred_element_type=jnp.float32), 7.0)
            lift = jnp.clip(
                jnp.dot(x, w_lift[:, cols], preferred_element_type=jnp.float32), -7.0, 7.0
            )
            act[:, cols] = ((lift + 1.0) * gate * jax.nn.sigmoid(1.702 * gate)).astype(jnp.bfloat16)
            return carry

        lax.fori_loop(0, hidden // TILE, up, 0)

        def down(t, carry):
            cols = tile_of(t)
            result[j, :, cols] = jnp.dot(
                act[...], w_down[:, cols], preferred_element_type=jnp.float32
            ).astype(jnp.bfloat16)
            return carry

        lax.fori_loop(0, model_dim // TILE, down, 0)

    def column(ref, j):
        lane = lax.broadcasted_iota(jnp.int32, ref.shape, 1)
        return jnp.sum(jnp.where(lane == j, ref[...], 0.0), axis=1, keepdims=True)

    def combine(j, source, store):
        rank = column(rank_cols_ref, j).astype(jnp.int32)
        weight = column(weight_ref, j)
        slot = lax.broadcasted_iota(jnp.int32, (rows, cap), 1)
        pick = (slot == rank).astype(jnp.float32).astype(jnp.bfloat16)

        def piece(t, carry):
            cols = tile_of(t)
            found = jnp.dot(pick, source[j, :, cols], preferred_element_type=jnp.float32)
            store(cols, weight * found)
            return carry

        lax.fori_loop(0, model_dim // TILE, piece, 0)

    def store_first(cols, term):
        total[:, cols] = mixed_ref[:, cols].astype(jnp.float32) + term

    def store_more(cols, term):
        total[:, cols] = total[:, cols] + term

    def store_last(cols, term):
        out_ref[:, cols] = (total[:, cols] + term).astype(jnp.bfloat16)

    pl.semaphore_wait(barrier, count - 1)

    def dispatch(j, carry):
        pack(j, send)
        out_copy(j).start()
        return carry

    lax.fori_loop(1, count, dispatch, 0)
    pack(0, send)
    for load in loads:
        load.wait()
    ffn(0, send)
    combine(0, result, store_first)

    def serve(j, carry):
        out_copy(j).wait_recv()
        ffn(j, recv)
        back_copy(j).start()
        return carry

    lax.fori_loop(1, count, serve, 0)

    def gather(j, carry):
        back_copy(j).wait_recv()
        combine(j, back, store_more)
        return carry

    lax.fori_loop(1, count - 1, gather, 0)
    back_copy(count - 1).wait_recv()
    combine(count - 1, back, store_last)

    def finish(j, carry):
        out_copy(j).wait_send()
        back_copy(j).wait_send()
        return carry

    lax.fori_loop(1, count, finish, 0)


def run_experts(mixed, gain, rank, weight, w_gate, w_lift, w_down, cap, count):
    rows, model_dim = mixed.shape
    hidden = w_gate.shape[2]
    vmem = pl.BlockSpec(memory_space=pltpu.VMEM)
    anywhere = pl.BlockSpec(memory_space=pl.ANY)
    slots = pltpu.VMEM((count, cap, model_dim), jnp.bfloat16)
    return pl.pallas_call(
        functools.partial(experts_kernel, count),
        out_shape=jax.ShapeDtypeStruct((rows, model_dim), jnp.bfloat16),
        in_specs=[vmem] * 5 + [anywhere] * 3,
        out_specs=vmem,
        scratch_shapes=[
            pltpu.VMEM((rows, model_dim), jnp.bfloat16),
            pltpu.VMEM((cap, rows), jnp.bfloat16),
            slots,
            slots,
            slots,
            slots,
            pltpu.VMEM((rows, model_dim), jnp.float32),
            pltpu.VMEM((cap, hidden), jnp.bfloat16),
            pltpu.VMEM(w_gate.shape[1:], jnp.bfloat16),
            pltpu.VMEM(w_lift.shape[1:], jnp.bfloat16),
            pltpu.VMEM(w_down.shape[1:], jnp.bfloat16),
            pltpu.SemaphoreType.DMA((3,)),
            pltpu.SemaphoreType.DMA((count,)),
            pltpu.SemaphoreType.DMA((count,)),
            pltpu.SemaphoreType.DMA((count,)),
            pltpu.SemaphoreType.DMA((count,)),
        ],
        compiler_params=pltpu.CompilerParams(
            collective_id=0, has_side_effects=True, vmem_limit_bytes=60 * 2**20
        ),
        cost_estimate=pl.CostEstimate(
            flops=6 * count * cap * model_dim * hidden,
            bytes_accessed=3 * model_dim * hidden * 2,
            transcendentals=count * cap * hidden,
        ),
    )(
        mixed,
        gain[None, :],
        rank.T[:, None, :],
        rank.astype(jnp.float32),
        weight,
        w_gate,
        w_lift,
        w_down,
    )


def fused_kernel(
    count,
    tp_count,
    pool_hbm,
    docs_hbm,
    routes_hbm,
    route_weight_hbm,
    gain_hbm,
    gate_hbm,
    resid_hbm,
    w_up_hbm,
    w_out_hbm,
    w_gate_hbm,
    w_lift_hbm,
    w_down_hbm,
    out_ref,
    pool,
    docs,
    routes_ref,
    route_weight_ref,
    gain,
    gate_pre,
    resid,
    w_up,
    w_out,
    w_gate,
    w_lift,
    w_down,
    pooled,
    gathered,
    tokens,
    gated,
    mixed,
    normed,
    onehot,
    pick_own,
    pick_near,
    pick_rest,
    send,
    recv,
    result,
    back,
    own,
    corner,
    act,
    corner_act,
    corner_up,
    corner_down,
    corner_out,
    local_out,
    total,
    load_sems,
    edge_go,
    edge_come,
    pool_go,
    pool_come,
    part_go,
    direct_come,
    share_go,
    near_come,
    middle_come,
    out_go,
    out_come,
    ret_go,
    ret_come,
    late_go,
    late_come,
    mate_go,
    mate_come,
    core_go,
    core_come,
):
    channels = pool_hbm.shape[0]
    rows, model_dim = resid.shape
    hidden = w_gate.shape[1]
    half = hidden // 2
    cap = own.shape[0]
    part = cap // 2
    sp, tp = lax.axis_index("sp"), lax.axis_index("tp")
    plane, core = tp // 2, tp % 2
    planes = tp_count // 2
    at_end = (plane == 0) | (plane == planes - 1)
    inside = (plane > 0) & (plane < planes - 1)
    f32, bf16 = jnp.float32, jnp.bfloat16

    loads = [
        pltpu.make_async_copy(src, dst, load_sems.at[i])
        for i, (src, dst) in enumerate(
            (
                (pool_hbm, pool.at[:, LANES:]),
                (docs_hbm, docs.at[:, LANES:]),
                (w_gate_hbm.at[0], w_gate),
                (w_lift_hbm.at[0], w_lift),
                (w_down_hbm.at[0], w_down),
                (routes_hbm, routes_ref),
                (route_weight_hbm, route_weight_ref),
                (w_up_hbm, w_up),
                (gate_hbm, gate_pre),
                (w_out_hbm, w_out),
                (resid_hbm, resid),
                (gain_hbm, gain),
            )
        )
    ]
    for load in loads:
        load.start()
    barrier = pltpu.get_barrier_semaphore()

    def greet_sp(j, carry):
        pl.semaphore_signal(
            barrier, inc=1, device_id={"sp": partner(sp, j, count)}, device_id_type=MESH
        )
        return carry

    def greet_tp(j, carry):
        pl.semaphore_signal(
            barrier, inc=1, device_id={"tp": partner(tp, j, tp_count)}, device_id_type=MESH
        )
        return carry

    lax.fori_loop(1, count, greet_sp, 0)
    lax.fori_loop(1, tp_count, greet_tp, 0)
    def remote(src, dst, go, come, device):
        return pltpu.make_async_remote_copy(
            src_ref=src,
            dst_ref=dst,
            send_sem=go,
            recv_sem=come,
            device_id=device,
            device_id_type=MESH,
        )

    mate = {"tp": partner(tp, 1, tp_count)}
    following = {"sp": lax.rem(sp + 1, count)}
    tok_dev = pool_hbm.shape[1]
    edges = [
        remote(
            ref.at[:, pl.ds(tok_dev, LANES)],
            ref.at[:, pl.ds(0, LANES)],
            edge_go.at[i],
            edge_come.at[i],
            following,
        )
        for i, ref in enumerate((pool, docs))
    ]

    pieces = [(m, q) for q in range(4) for m in range(2)] + [(2, q) for q in range(4)]
    sources = (w_gate, w_lift, w_down)
    far = partner(sp, 3, count)

    def span(m, q, zone):
        units = (model_dim if m < 2 else half) // UNIT
        ends = units * END_SHARE[m] // 32
        inner = (units - ends) // 2
        is_end = isinstance(zone, int) and zone == 0
        size = ends if is_end else inner
        low, high = (q * size // 4, (q + 1) * size // 4) if m < 2 else (0, size)
        if is_end:
            return low * UNIT, (high - low) * UNIT
        start = (ends + inner * (zone - 1) + low) * UNIT
        return pl.multiple_of(start, UNIT), (high - low) * UNIT

    def place(m, q, start, size):
        if m < 2:
            return corner_up.at[m, pl.ds(start, size), :]
        return corner_down.at[pl.ds(start, size), pl.ds(q * TILE, TILE)]

    def fetch(i, zone):
        m, q = pieces[i]
        start, size = span(m, q, zone)
        if m < 2:
            cols = pl.ds(pl.multiple_of(core * half, half), half)
            src = sources[m].at[pl.ds(start, size), cols]
        else:
            first = pl.multiple_of(core * half + start, UNIT)
            src = sources[m].at[pl.ds(first, size), pl.ds(q * TILE, TILE)]
        return remote(
            src,
            place(m, q, start, size),
            part_go.at[m // 2],
            direct_come.at[i],
            {"sp": far},
        )

    def share(i, zone, way):
        m, q = pieces[i]
        start, size = span(m, q, zone)
        return remote(
            place(m, q, start, size),
            place(m, q, start, size),
            share_go.at[way, m // 2],
            middle_come.at[i] if way == 1 else near_come.at[way // 2, max(i - 7, 0)],
            {"tp": partner(tp, 6 if way == 1 else 2, tp_count)},
        )

    def pass_on(i):
        @pl.when(at_end)
        def _():
            fetch(i, 0).wait_recv()
            share(i, 0, 0).start()

        @pl.when(inside)
        def _():
            fetch(i, plane).wait_recv()
            share(i, plane, 1).start()
            share(i, plane, 0).start()

    def relay(i):
        @pl.when(inside)
        def _():
            share(i, 3 - plane, 1).wait_recv()
            share(i, 3 - plane, 2).start()

    def whole(zone, down):
        start, size = span(2 if down else 0, 0, zone)
        if down:
            return corner_down.at[pl.ds(start, size), :]
        size = sum(span(0, q, zone)[1] for q in range(4))
        return corner_up.at[:, pl.ds(start, size), :]

    def up_arrived():
        @pl.when(at_end)
        def _():
            for way, zone in ((0, 1), (2, 2)):
                ref = whole(zone, False)
                remote(ref, ref, share_go.at[0, 0], near_come.at[way // 2, 0], mate).wait_recv()

        @pl.when(inside)
        def _():
            ref = whole(0, False)
            remote(ref, ref, share_go.at[0, 0], near_come.at[0, 0], mate).wait_recv()

    def arrived(i):
        @pl.when(at_end)
        def _():
            share(i, 1, 0).wait_recv()
            share(i, 2, 2).wait_recv()

        @pl.when(inside)
        def _():
            share(i, 0, 0).wait_recv()

    def fetch_all(some):
        @pl.when(at_end)
        def _():
            for i in some:
                fetch(i, 0).start()

        @pl.when(inside)
        def _():
            for i in some:
                fetch(i, plane).start()

    for load in loads[:2]:
        load.wait()
    pl.semaphore_wait(barrier, count - 1 + tp_count - 1)
    for edge in edges:
        edge.start()

    for load in loads[2:4]:
        load.wait()
    fetch_all(range(8))

    level = (tp * channels) // (channels * tp_count // 4)

    def pool_copy(j):
        return remote(
            pooled.at[j],
            gathered.at[pl.ds(pl.multiple_of(tp * channels, channels), channels), :],
            pool_go.at[0],
            pool_come.at[0],
            {"tp": partner(tp, j, tp_count)},
        )

    def pool_block(j):
        owner = partner(tp, j, tp_count)
        cols = pl.ds(pl.multiple_of(owner * rows, LANES), rows + LANES)
        values = pool[:, cols].astype(f32)
        document = jnp.broadcast_to(docs[:, cols], (8, rows + LANES))
        lane = lax.broadcasted_iota(jnp.int32, document.shape, 1)
        document = jnp.where((lane < LANES) & (owner == 0) & (sp == 0), -1, document)
        running = values
        number = jnp.ones(document.shape, f32)
        for step in range(4):
            shift = 2**step
            same = (document == pltpu.roll(document, shift, 1)) & (level >= step)
            same = same.astype(f32)
            number = number + same * pltpu.roll(number, shift, 1)
            wide = jnp.concatenate([same] * (channels // 8), axis=0)
            running = running + wide * pltpu.roll(running, shift, 1)
        share_of = jnp.concatenate([1.0 / number] * (channels // 8), axis=0)
        return (running * share_of - values)[:, LANES:].astype(bf16)

    def pool_send(j):
        pooled[j] = pool_block(j)
        pool_copy(j).start()

    def pool_step(i, carry):
        j = tp_count - 1 - i

        @pl.when(j != tp)
        def _():
            pool_send(j)

        return carry

    lax.fori_loop(0, tp_count - 1, pool_step, 0)
    loads[4].wait()
    fetch_all(range(8, 12))
    for edge in edges:
        edge.wait_recv()

    @pl.when(tp != 0)
    def _():
        pool_send(tp)

    gathered[pl.ds(pl.multiple_of(tp * channels, channels), channels), :] = pool_block(0)
    pass_on(0)

    for load in loads[5:7]:
        load.wait()

    first, second = routes_ref[0:1, :], routes_ref[1:2, :]
    weight_first, weight_second = route_weight_ref[0:1, :], route_weight_ref[1:2, :]
    named, weights = [], []
    for j in range(count):
        expert = partner(sp, j, count)
        named.append(jnp.where((first == expert) | (second == expert), 1.0, 0.0))
        weights.append(
            jnp.where(first == expert, weight_first, 0.0)
            + jnp.where(second == expert, weight_second, 0.0)
        )
    named = jnp.concatenate(named + named, axis=0)
    weights = jnp.concatenate(weights + weights, axis=0)
    before = lax.broadcasted_iota(jnp.int32, (rows, rows), 0) <= lax.broadcasted_iota(
        jnp.int32, (rows, rows), 1
    )
    place_of = jnp.dot(
        named.astype(bf16), before.astype(f32).astype(bf16), preferred_element_type=f32
    )
    place_of = jnp.where(named > 0.0, place_of - 1.0, -4.0 * cap)
    split = jnp.where(place_of >= part, place_of + part, place_of)
    line = lax.broadcasted_iota(jnp.int32, place_of.shape, 0)
    goal = jnp.where(line == 1, split, place_of)
    goal = jnp.where(line == 2, split + part, goal)
    goal = jnp.where(line == 3, place_of + cap, goal)
    goal_rows = goal.astype(jnp.int32)
    goal_cols = goal.T.astype(jnp.int32)
    weight_cols = weights.T

    slot = lax.broadcasted_iota(jnp.int32, (2 * cap, rows), 0)
    for k, (a, b) in enumerate(((1, 2), (0, 3))):
        hit = (slot == goal_rows[a : a + 1, :]) | (slot == goal_rows[b : b + 1, :])
        onehot[k] = hit.astype(f32).astype(bf16)

    def weighed(slots, j, shift):
        return jnp.where(
            slots == goal_cols[:, j : j + 1] + shift, weight_cols[:, j : j + 1], 0.0
        )

    slots = lax.broadcasted_iota(jnp.int32, (rows, cap), 1)
    pick_own[...] = weighed(slots, 0, 0).astype(bf16)
    pick_near[...] = (weighed(slots, 1, 0) + weighed(slots, 2, 0)).astype(bf16)
    slots = lax.broadcasted_iota(jnp.int32, (rows, 3 * cap), 1)
    found = weighed(slots, 3, -cap) + weighed(slots, 3, 0)
    late = jnp.where(slots >= 2 * cap, slots - cap, -1)
    found = found + weighed(late, 1, 0) + weighed(late, 2, 0)
    pick_rest[...] = found.astype(bf16)

    for i in range(1, 4):
        pass_on(i)

    for load in loads[7:]:
        load.wait()

    others = gathered.at[pl.ds(0, (tp_count - 1) * channels), :]
    remote(others, others, pool_go.at[0], pool_come.at[0], mate).wait_recv()
    tokens[...] = gathered[...].T

    def lift_up(t, carry):
        cols = tile_of(t)
        lifted = jnp.dot(tokens[...], w_up[:, cols], preferred_element_type=f32)
        gated[:, cols] = (jax.nn.sigmoid(gate_pre[:, cols].astype(f32)) * lifted).astype(bf16)
        return carry

    lax.fori_loop(0, model_dim // TILE, lift_up, 0)

    def mix(t, carry):
        cols = tile_of(t)
        added = jnp.dot(gated[...], w_out[:, cols], preferred_element_type=f32)
        mixed[:, cols] = (resid[:, cols].astype(f32) + added).astype(bf16)
        return carry

    lax.fori_loop(0, model_dim // TILE, mix, 0)

    def norm(t, carry):
        block = pl.ds(pl.multiple_of(t * 64, 64), 64)
        x = mixed[block, :].astype(f32)
        scale = lax.rsqrt(jnp.mean(x * x, axis=-1, keepdims=True) + 1e-06)
        normed[block, :] = (x * scale * gain[...]).astype(bf16)
        return carry

    for i in range(4, 6):
        pass_on(i)
    lax.fori_loop(0, rows // 64, norm, 0)

    def pack_near(t, carry):
        cols = tile_of(t)
        send[:, cols] = jnp.dot(
            onehot[0], normed[:, cols], preferred_element_type=f32
        ).astype(bf16)
        return carry

    lax.fori_loop(0, model_dim // TILE, pack_near, 0)

    def out_copy(h, p):
        block = pl.ds((2 * h + p) * part, part)
        return remote(
            send.at[block],
            recv.at[block],
            out_go.at[0],
            out_come.at[h],
            {"sp": partner(sp, p + 1, count)},
        )

    def back_copy(p):
        block = pl.ds(p * part, part)
        return remote(
            result.at[block],
            back.at[block],
            ret_go.at[0],
            ret_come.at[0],
            {"sp": partner(sp, p + 1, count)},
        )

    def late_copy(p, t):
        return remote(
            result.at[pl.ds((2 + p) * part, part), tile_of(t)],
            back.at[pl.ds(3 * cap + p * part, part), tile_of(t)],
            late_go.at[0],
            late_come.at[t],
            {"sp": partner(sp, p + 1, count)},
        )

    chunks = [(h, p) for h in range(2) for p in range(2)]
    for h, p in chunks:
        out_copy(h, p).start()

    pass_on(6)

    def pack_local(t, carry):
        cols = tile_of(t)
        packed = jnp.dot(onehot[1], normed[:, cols], preferred_element_type=f32).astype(bf16)
        own[:, cols] = packed[:cap]
        corner[0:cap, cols] = packed[cap:]
        return carry

    lax.fori_loop(0, model_dim // TILE, pack_local, 0)
    corner_copy = remote(
        corner.at[pl.ds(0, cap)], corner.at[pl.ds(cap, cap)], core_go.at[0], core_come.at[0], mate
    )
    corner_copy.start()
    pass_on(7)

    def activate(gate, lift):
        gate = jnp.minimum(gate, 7.0)
        lift = jnp.clip(lift, -7.0, 7.0)
        return ((lift + 1.0) * gate * jax.nn.sigmoid(1.702 * gate)).astype(bf16)

    def ffn(source, target, base, then=lambda t: None):
        def up(t, carry):
            cols = tile_of(t)
            x = source[base : base + cap, :]
            act[:, cols] = activate(
                jnp.dot(x, w_gate[:, cols], preferred_element_type=f32),
                jnp.dot(x, w_lift[:, cols], preferred_element_type=f32),
            )
            return carry

        lax.fori_loop(0, hidden // TILE, up, 0)

        def down(t, carry):
            cols = tile_of(t)
            target[base : base + cap, cols] = jnp.dot(
                act[...], w_down[:, cols], preferred_element_type=f32
            ).astype(bf16)
            then(t)
            return carry

        lax.fori_loop(0, model_dim // TILE, down, 0)

    ffn(own, local_out, 0)
    pass_on(8)
    pass_on(9)

    def combine_own(t, carry):
        cols = tile_of(t)
        total[:, cols] = mixed[:, cols].astype(f32) + jnp.dot(
            pick_own[...], local_out[:, cols], preferred_element_type=f32
        )
        return carry

    lax.fori_loop(0, model_dim // TILE, combine_own, 0)
    pass_on(10)
    pass_on(11)
    for i in range(8):
        relay(i)

    def near_arrived(h):
        block = pl.ds(h * cap, cap)
        remote(send.at[block], recv.at[block], out_go.at[0], out_come.at[h], mate).wait_recv()

    near_arrived(0)
    ffn(recv, result, 0)
    for p in range(2):
        back_copy(p).start()
    for i in range(8, 12):
        relay(i)
    near_arrived(1)

    def send_back(t):
        for p in range(2):
            late_copy(p, t).start()

    ffn(recv, result, cap, send_back)

    corner_copy.wait_recv()
    up_arrived()

    def corner_lift(t, carry):
        cols = tile_of(t)
        x = corner[...]
        corner_act[:, cols] = activate(
            jnp.dot(x, corner_up[0, :, cols], preferred_element_type=f32),
            jnp.dot(x, corner_up[1, :, cols], preferred_element_type=f32),
        )
        return carry

    lax.fori_loop(0, half // TILE, corner_lift, 0)
    def mate_copy(t):
        return remote(
            corner_out.at[:, tile_of(t)],
            back.at[pl.ds(2 * cap, cap), tile_of(t)],
            mate_go.at[0],
            mate_come.at[t],
            mate,
        )

    def corner_drop(t):
        cols = tile_of(t)
        for block, target, base in ((1, corner_out, 0), (0, back, cap)):
            target[base : base + cap, cols] = jnp.dot(
                corner_act[block * cap : (block + 1) * cap, :],
                corner_down[:, cols],
                preferred_element_type=f32,
            ).astype(bf16)
            if block == 1:
                mate_copy(t).start()

    def combine_near(t, carry):
        cols = tile_of(t)
        found = jnp.dot(pick_near[...], back[0:cap, cols], preferred_element_type=f32)
        total[:, cols] = total[:, cols] + found
        return carry

    def combine_rest(t):
        cols = tile_of(t)
        mate_copy(t).wait_recv()
        block = back.at[pl.ds(3 * cap, cap), cols]
        remote(block, block, late_go.at[0], late_come.at[t], mate).wait_recv()
        found = jnp.dot(pick_rest[...], back[cap:, cols], preferred_element_type=f32)
        out_ref[:, cols] = (total[:, cols] + found).astype(bf16)

    tiles = model_dim // TILE
    block = pl.ds(0, cap)
    remote(result.at[block], back.at[block], ret_go.at[0], ret_come.at[0], mate).wait_recv()
    lax.fori_loop(0, tiles, combine_near, 0)
    for t in range(tiles):
        arrived(8 + t)
        corner_drop(t)
        if t > 0:
            combine_rest(t - 1)
    combine_rest(tiles - 1)

    for edge in edges:
        edge.wait_send()

    others = pooled.at[pl.ds(1, tp_count - 1)]
    remote(others, others, pool_go.at[0], pool_come.at[0], mate).wait_send()
    remote(send, recv, out_go.at[0], out_come.at[0], mate).wait_send()
    corner_copy.wait_send()
    block = pl.ds(0, cap)
    remote(result.at[block], back.at[block], ret_go.at[0], ret_come.at[0], mate).wait_send()
    block = pl.ds(cap, cap)
    remote(result.at[block], back.at[block], late_go.at[0], late_come.at[0], mate).wait_send()
    remote(corner_out, corner_out, mate_go.at[0], mate_come.at[0], mate).wait_send()

    def gone(ref, sem):
        remote(ref, ref, sem, direct_come.at[0], mate).wait_send()

    @pl.when(at_end)
    def _():
        for k in range(2):
            gone(whole(0, k), part_go.at[k])
            gone(whole(0, k), share_go.at[0, k])

    @pl.when(inside)
    def _():
        for k in range(2):
            gone(whole(plane, k), part_go.at[k])
            gone(whole(plane, k), share_go.at[0, k])
            gone(whole(plane, k), share_go.at[1, k])
            gone(whole(3 - plane, k), share_go.at[2, k])


def run_fused(
    count,
    tp_count,
    pool_input,
    gate_pre,
    resid,
    docs,
    w_up,
    w_out,
    g_ffn,
    w_gate,
    w_lift,
    w_down,
    routes,
    route_weight,
):
    tok_dev, channels = pool_input.shape
    rows, model_dim = resid.shape
    hidden = w_gate.shape[2]
    half = hidden // 2
    pool_w = w_up.shape[0]
    top = routes.shape[1]
    cap = capacity(rows, top, count)
    vmem = pl.BlockSpec(memory_space=pltpu.VMEM)
    bf16, f32 = jnp.bfloat16, jnp.float32
    hbm = functools.partial(pltpu.with_memory_space_constraint, memory_space=pltpu.HBM)
    dma = pltpu.SemaphoreType.DMA
    return pl.pallas_call(
        functools.partial(fused_kernel, count, tp_count),
        out_shape=jax.ShapeDtypeStruct((rows, model_dim), bf16),
        in_specs=[pl.BlockSpec(memory_space=pltpu.HBM)] * 12,
        out_specs=vmem,
        scratch_shapes=[
            pltpu.VMEM((channels, tok_dev + LANES), bf16),
            pltpu.VMEM((1, tok_dev + LANES), jnp.int32),
            pltpu.VMEM((top, rows), jnp.int32),
            pltpu.VMEM((top, rows), f32),
            pltpu.VMEM((1, model_dim), f32),
            pltpu.VMEM((rows, model_dim), bf16),
            pltpu.VMEM((rows, model_dim), bf16),
            pltpu.VMEM(w_up.shape, bf16),
            pltpu.VMEM(w_out.shape, bf16),
            pltpu.VMEM(w_gate.shape[1:], bf16),
            pltpu.VMEM(w_lift.shape[1:], bf16),
            pltpu.VMEM(w_down.shape[1:], bf16),
            pltpu.VMEM((tp_count, channels, rows), bf16),
            pltpu.VMEM((pool_w, rows), bf16),
            pltpu.VMEM((rows, pool_w), bf16),
            pltpu.VMEM((rows, model_dim), bf16),
            pltpu.VMEM((rows, model_dim), bf16),
            pltpu.VMEM((rows, model_dim), bf16),
            pltpu.VMEM((2, 2 * cap, rows), bf16),
            pltpu.VMEM((rows, cap), bf16),
            pltpu.VMEM((rows, cap), bf16),
            pltpu.VMEM((rows, 3 * cap), bf16),
            pltpu.VMEM((2 * cap, model_dim), bf16),
            pltpu.VMEM((2 * cap, model_dim), bf16),
            pltpu.VMEM((2 * cap, model_dim), bf16),
            pltpu.VMEM((4 * cap, model_dim), bf16),
            pltpu.VMEM((cap, model_dim), bf16),
            pltpu.VMEM((2 * cap, model_dim), bf16),
            pltpu.VMEM((cap, hidden), bf16),
            pltpu.VMEM((2 * cap, half), bf16),
            pltpu.VMEM((2, model_dim, half), bf16),
            pltpu.VMEM((half, model_dim), bf16),
            pltpu.VMEM((cap, model_dim), bf16),
            pltpu.VMEM((cap, model_dim), bf16),
            pltpu.VMEM((rows, model_dim), f32),
            dma((12,)),
            dma((2,)),
            dma((2,)),
            dma((1,)),
            dma((1,)),
            dma((2,)),
            dma((12,)),
            dma((3, 2)),
            dma((2, 5)),
            dma((12,)),
            dma((1,)),
            dma((2,)),
            dma((1,)),
            dma((1,)),
            dma((1,)),
            dma((4,)),
            dma((1,)),
            dma((4,)),
            dma((1,)),
            dma((1,)),
        ],
        compiler_params=pltpu.CompilerParams(
            collective_id=1, has_side_effects=True, vmem_limit_bytes=52 * 2**20
        ),
        cost_estimate=pl.CostEstimate(
            flops=6 * count * cap * model_dim * hidden,
            bytes_accessed=3 * model_dim * hidden * 2,
            transcendentals=count * cap * hidden,
        ),
    )(
        hbm(pool_input.T),
        hbm(docs[None, :]),
        hbm(routes.T),
        hbm(route_weight.T),
        hbm(g_ffn[None, :]),
        gate_pre,
        resid,
        w_up,
        w_out,
        w_gate,
        w_lift,
        w_down,
    )


def capacity(row_count, top_count, count):
    cap = max(2, 5 * row_count * top_count // (4 * count))
    return (cap + 15) // 16 * 16


def on_device(
    pool_input,
    gate_pre,
    resid,
    docs,
    w_up,
    w_out,
    g_ffn,
    w_gate,
    w_lift,
    w_down,
    routes,
    route_weight,
):
    tok_dev = pool_input.shape[0]
    channels = pool_input.shape[1]
    group_size = POOL_W // 4
    channel_ids = lax.axis_index("tp") * channels + lax.iota(jnp.int32, channels)
    window = jnp.power(2, channel_ids // group_size + 1)
    edge = jnp.concatenate(
        [pool_input[tok_dev - RIM :], docs[tok_dev - RIM :, None].astype(jnp.bfloat16)], axis=1
    )
    before = shifted_2(edge, "sp", 1)
    before_rows = before[:, :channels]
    before_docs = before[:, channels].astype(jnp.int32)
    first_dev = lax.axis_index("sp") == 0
    before_docs = jnp.where(first_dev, -1, before_docs)
    values = pool_input.astype(jnp.float32)
    padded = jnp.concatenate([before_rows.astype(jnp.float32), values], axis=0)
    doc_padded = jnp.concatenate([before_docs.astype(jnp.int32), docs], axis=0)
    earlier = sum(
        (doc_padded[RIM - offset : RIM - offset + tok_dev] == docs).astype(jnp.int32)
        for offset in range(1, RIM + 1)
    )
    reach = jnp.minimum(earlier[:, None] + 1, window[None, :])
    running = values
    for offset in range(1, RIM + 1):
        shifted = padded[RIM - offset : RIM - offset + tok_dev]
        running = running + jnp.where(offset < reach, shifted, 0.0)
    counts = reach.astype(jnp.float32)
    pooled = (running / counts - values).astype(jnp.bfloat16)
    tokens_pooled = lax.all_to_all(pooled, "tp", split_axis=0, concat_axis=1, tiled=True)
    lifted = jnp.dot(tokens_pooled, w_up, preferred_element_type=jnp.float32)
    gated_rows = (jax.nn.sigmoid(gate_pre.astype(jnp.float32)) * lifted).astype(jnp.bfloat16)
    mixed_rows = (
        resid.astype(jnp.float32) + jnp.dot(gated_rows, w_out, preferred_element_type=jnp.float32)
    ).astype(jnp.bfloat16)

    row_count, top_count = routes.shape
    count = lax.axis_size("sp")
    cap = capacity(row_count, top_count, count)
    order = partner(lax.axis_index("sp"), lax.iota(jnp.int32, count), count)
    chosen = routes[:, :, None] == order[None, None, :]
    named = jnp.any(chosen, axis=1)
    rank = jnp.where(named, jnp.cumsum(named.astype(jnp.int32), axis=0) - 1, -1)
    weight = jnp.sum(jnp.where(chosen, route_weight[:, :, None], 0.0), axis=1)
    return run_experts(mixed_rows, g_ffn, rank, weight, w_gate, w_lift, w_down, cap, count)


def solution(mesh):
    in_specs = (
        P("sp", "tp"),
        P(("sp", "tp"), None),
        P(("sp", "tp"), None),
        P("sp"),
        P(),
        P(),
        P(),
        P("sp", None, None),
        P("sp", None, None),
        P("sp", None, None),
        P(("sp", "tp"), None),
        P(("sp", "tp"), None),
    )
    out_specs = P(("sp", "tp"), None)
    count, tp_count = mesh.shape["sp"], mesh.shape["tp"]
    body = on_device
    if count == 4 and tp_count == 8:
        body = functools.partial(run_fused, count, tp_count)
    return jax.shard_map(
        body, mesh=mesh, in_specs=in_specs, out_specs=out_specs, check_vma=False
    )
```

```python
import functools

import jax
import jax.numpy as jnp
from jax import lax
from jax.experimental import pallas as pl
from jax.experimental.pallas import tpu as pltpu
from jax.sharding import PartitionSpec as P

POOL_W = 512
RIM = 15
TILE = 256
LANES = 128
UNIT = 16
END_SHARE = (11, 11, 12)
MESH = pl.DeviceIdType.MESH


def shifted_2(value, axis, steps):
    count = lax.axis_size(axis)
    leading, last = (max(0, -steps), min(count, count - steps))
    return lax.ppermute(value, axis, [(source, source + steps) for source in range(leading, last)])


def partner(me, step, count):
    other, bit = 0, 1
    while bit < count:
        other = other + ((me // bit + step // bit) % 2) * bit
        bit *= 2
    return other


def tile_of(t):
    return pl.ds(pl.multiple_of(t * TILE, TILE), TILE)


def experts_kernel(
    count,
    mixed_ref,
    gain_ref,
    rank_rows_ref,
    rank_cols_ref,
    weight_ref,
    w_gate_hbm,
    w_lift_hbm,
    w_down_hbm,
    out_ref,
    normed,
    onehot,
    send,
    recv,
    result,
    back,
    total,
    act,
    w_gate,
    w_lift,
    w_down,
    weight_sems,
    go_sems,
    come_sems,
    ret_go_sems,
    ret_come_sems,
):
    rows, model_dim = mixed_ref.shape
    cap = send.shape[1]
    hidden = w_gate.shape[1]
    me = lax.axis_index("sp")
    loads = [
        pltpu.make_async_copy(src.at[0], dst, weight_sems.at[i])
        for i, (src, dst) in enumerate(
            ((w_gate_hbm, w_gate), (w_lift_hbm, w_lift), (w_down_hbm, w_down))
        )
    ]

    barrier = pltpu.get_barrier_semaphore()

    def greet(j, carry):
        pl.semaphore_signal(
            barrier, inc=1, device_id={"sp": partner(me, j, count)}, device_id_type=MESH
        )
        return carry

    lax.fori_loop(1, count, greet, 0)
    for load in loads:
        load.start()

    def norm(t, carry):
        block = pl.ds(pl.multiple_of(t * 64, 64), 64)
        x = mixed_ref[block, :].astype(jnp.float32)
        scale = lax.rsqrt(jnp.mean(x * x, axis=-1, keepdims=True) + 1e-06)
        normed[block, :] = (x * scale * gain_ref[...]).astype(jnp.bfloat16)
        return carry

    lax.fori_loop(0, rows // 64, norm, 0)

    def out_copy(j):
        return pltpu.make_async_remote_copy(
            src_ref=send.at[j],
            dst_ref=recv.at[j],
            send_sem=go_sems.at[j],
            recv_sem=come_sems.at[j],
            device_id={"sp": partner(me, j, count)},
            device_id_type=MESH,
        )

    def back_copy(j):
        return pltpu.make_async_remote_copy(
            src_ref=result.at[j],
            dst_ref=back.at[j],
            send_sem=ret_go_sems.at[j],
            recv_sem=ret_come_sems.at[j],
            device_id={"sp": partner(me, j, count)},
            device_id_type=MESH,
        )

    def pack(j, target):
        slot = lax.broadcasted_iota(jnp.int32, (cap, rows), 0)
        onehot[...] = (slot == rank_rows_ref[j]).astype(jnp.float32).astype(jnp.bfloat16)

        def piece(t, carry):
            cols = tile_of(t)
            target[j, :, cols] = jnp.dot(
                onehot[...], normed[:, cols], preferred_element_type=jnp.float32
            ).astype(jnp.bfloat16)
            return carry

        lax.fori_loop(0, model_dim // TILE, piece, 0)

    def ffn(j, source):
        def up(t, carry):
            cols = tile_of(t)
            x = source[j]
            gate = jnp.minimum(jnp.dot(x, w_gate[:, cols], preferred_element_type=jnp.float32), 7.0)
            lift = jnp.clip(
                jnp.dot(x, w_lift[:, cols], preferred_element_type=jnp.float32), -7.0, 7.0
            )
            act[:, cols] = ((lift + 1.0) * gate * jax.nn.sigmoid(1.702 * gate)).astype(jnp.bfloat16)
            return carry

        lax.fori_loop(0, hidden // TILE, up, 0)

        def down(t, carry):
            cols = tile_of(t)
            result[j, :, cols] = jnp.dot(
                act[...], w_down[:, cols], preferred_element_type=jnp.float32
            ).astype(jnp.bfloat16)
            return carry

        lax.fori_loop(0, model_dim // TILE, down, 0)

    def column(ref, j):
        lane = lax.broadcasted_iota(jnp.int32, ref.shape, 1)
        return jnp.sum(jnp.where(lane == j, ref[...], 0.0), axis=1, keepdims=True)

    def combine(j, source, store):
        rank = column(rank_cols_ref, j).astype(jnp.int32)
        weight = column(weight_ref, j)
        slot = lax.broadcasted_iota(jnp.int32, (rows, cap), 1)
        pick = (slot == rank).astype(jnp.float32).astype(jnp.bfloat16)

        def piece(t, carry):
            cols = tile_of(t)
            found = jnp.dot(pick, source[j, :, cols], preferred_element_type=jnp.float32)
            store(cols, weight * found)
            return carry

        lax.fori_loop(0, model_dim // TILE, piece, 0)

    def store_first(cols, term):
        total[:, cols] = mixed_ref[:, cols].astype(jnp.float32) + term

    def store_more(cols, term):
        total[:, cols] = total[:, cols] + term

    def store_last(cols, term):
        out_ref[:, cols] = (total[:, cols] + term).astype(jnp.bfloat16)

    pl.semaphore_wait(barrier, count - 1)

    def dispatch(j, carry):
        pack(j, send)
        out_copy(j).start()
        return carry

    lax.fori_loop(1, count, dispatch, 0)
    pack(0, send)
    for load in loads:
        load.wait()
    ffn(0, send)
    combine(0, result, store_first)

    def serve(j, carry):
        out_copy(j).wait_recv()
        ffn(j, recv)
        back_copy(j).start()
        return carry

    lax.fori_loop(1, count, serve, 0)

    def gather(j, carry):
        back_copy(j).wait_recv()
        combine(j, back, store_more)
        return carry

    lax.fori_loop(1, count - 1, gather, 0)
    back_copy(count - 1).wait_recv()
    combine(count - 1, back, store_last)

    def finish(j, carry):
        out_copy(j).wait_send()
        back_copy(j).wait_send()
        return carry

    lax.fori_loop(1, count, finish, 0)


def run_experts(mixed, gain, rank, weight, w_gate, w_lift, w_down, cap, count):
    rows, model_dim = mixed.shape
    hidden = w_gate.shape[2]
    vmem = pl.BlockSpec(memory_space=pltpu.VMEM)
    anywhere = pl.BlockSpec(memory_space=pl.ANY)
    slots = pltpu.VMEM((count, cap, model_dim), jnp.bfloat16)
    return pl.pallas_call(
        functools.partial(experts_kernel, count),
        out_shape=jax.ShapeDtypeStruct((rows, model_dim), jnp.bfloat16),
        in_specs=[vmem] * 5 + [anywhere] * 3,
        out_specs=vmem,
        scratch_shapes=[
            pltpu.VMEM((rows, model_dim), jnp.bfloat16),
            pltpu.VMEM((cap, rows), jnp.bfloat16),
            slots,
            slots,
            slots,
            slots,
            pltpu.VMEM((rows, model_dim), jnp.float32),
            pltpu.VMEM((cap, hidden), jnp.bfloat16),
            pltpu.VMEM(w_gate.shape[1:], jnp.bfloat16),
            pltpu.VMEM(w_lift.shape[1:], jnp.bfloat16),
            pltpu.VMEM(w_down.shape[1:], jnp.bfloat16),
            pltpu.SemaphoreType.DMA((3,)),
            pltpu.SemaphoreType.DMA((count,)),
            pltpu.SemaphoreType.DMA((count,)),
            pltpu.SemaphoreType.DMA((count,)),
            pltpu.SemaphoreType.DMA((count,)),
        ],
        compiler_params=pltpu.CompilerParams(
            collective_id=0, has_side_effects=True, vmem_limit_bytes=60 * 2**20
        ),
        cost_estimate=pl.CostEstimate(
            flops=6 * count * cap * model_dim * hidden,
            bytes_accessed=3 * model_dim * hidden * 2,
            transcendentals=count * cap * hidden,
        ),
    )(
        mixed,
        gain[None, :],
        rank.T[:, None, :],
        rank.astype(jnp.float32),
        weight,
        w_gate,
        w_lift,
        w_down,
    )


def halves_dot(rows, weights):
    half = rows.shape[0] // 2
    parts = [
        jnp.dot(part, weights, preferred_element_type=jnp.float32)
        for part in (rows[:half], rows[half:])
    ]
    return jnp.concatenate(parts, axis=0)


def fused_kernel(
    count,
    tp_count,
    pool_hbm,
    docs_hbm,
    routes_hbm,
    route_weight_hbm,
    gain_hbm,
    gate_hbm,
    resid_hbm,
    w_up_hbm,
    w_out_hbm,
    w_gate_hbm,
    w_lift_hbm,
    w_down_hbm,
    out_ref,
    pool,
    docs,
    routes_ref,
    route_weight_ref,
    gain,
    gate_pre,
    resid,
    w_up,
    w_out,
    w_gate,
    w_lift,
    w_down,
    pooled,
    gathered,
    tokens,
    gated,
    mixed,
    normed,
    onehot,
    pick_own,
    pick_near,
    pick_rest,
    send,
    recv,
    result,
    back,
    own,
    corner,
    act,
    corner_act,
    corner_up,
    corner_down,
    corner_out,
    local_out,
    total,
    load_sems,
    edge_go,
    edge_come,
    pool_go,
    pool_come,
    part_go,
    direct_come,
    share_go,
    near_come,
    middle_come,
    out_go,
    out_come,
    ret_go,
    ret_come,
    late_go,
    late_come,
    mate_go,
    mate_come,
    core_go,
    core_come,
):
    channels = pool_hbm.shape[0]
    rows, model_dim = resid.shape
    hidden = w_gate.shape[1]
    half = hidden // 2
    cap = own.shape[0]
    part = cap // 2
    sp, tp = lax.axis_index("sp"), lax.axis_index("tp")
    plane, core = tp // 2, tp % 2
    planes = tp_count // 2
    at_end = (plane == 0) | (plane == planes - 1)
    inside = (plane > 0) & (plane < planes - 1)
    f32, bf16 = jnp.float32, jnp.bfloat16

    loads = [
        pltpu.make_async_copy(src, dst, load_sems.at[i])
        for i, (src, dst) in enumerate(
            (
                (pool_hbm, pool.at[:, LANES:]),
                (docs_hbm, docs.at[:, LANES:]),
                (w_gate_hbm.at[0], w_gate),
                (w_lift_hbm.at[0], w_lift),
                (w_down_hbm.at[0], w_down),
                (routes_hbm, routes_ref),
                (route_weight_hbm, route_weight_ref),
                (w_up_hbm, w_up),
                (gate_hbm, gate_pre),
                (w_out_hbm, w_out),
                (resid_hbm, resid),
                (gain_hbm, gain),
            )
        )
    ]
    for load in loads[:5]:
        load.start()
    barrier = pltpu.get_barrier_semaphore()

    def greet_sp(j, carry):
        pl.semaphore_signal(
            barrier, inc=1, device_id={"sp": partner(sp, j, count)}, device_id_type=MESH
        )
        return carry

    def greet_tp(j, carry):
        pl.semaphore_signal(
            barrier, inc=1, device_id={"tp": partner(tp, j, tp_count)}, device_id_type=MESH
        )
        return carry

    lax.fori_loop(1, count, greet_sp, 0)
    lax.fori_loop(1, tp_count, greet_tp, 0)
    def remote(src, dst, go, come, device):
        return pltpu.make_async_remote_copy(
            src_ref=src,
            dst_ref=dst,
            send_sem=go,
            recv_sem=come,
            device_id=device,
            device_id_type=MESH,
        )

    mate = {"tp": partner(tp, 1, tp_count)}
    following = {"sp": lax.rem(sp + 1, count)}
    tok_dev = pool_hbm.shape[1]
    edges = [
        remote(
            ref.at[:, pl.ds(tok_dev, LANES)],
            ref.at[:, pl.ds(0, LANES)],
            edge_go.at[i],
            edge_come.at[i],
            following,
        )
        for i, ref in enumerate((pool, docs))
    ]

    pieces = [(m, q) for q in range(4) for m in range(2)] + [(2, q) for q in range(4)]
    sources = (w_gate, w_lift, w_down)
    far = partner(sp, 3, count)

    def span(m, q, zone):
        units = (model_dim if m < 2 else half) // UNIT
        ends = units * END_SHARE[m] // 32
        inner = (units - ends) // 2
        is_end = isinstance(zone, int) and zone == 0
        size = ends if is_end else inner
        low, high = (q % 2 * size // 2, (q % 2 + 1) * size // 2) if m < 2 else (0, size)
        if is_end:
            return low * UNIT, (high - low) * UNIT
        start = (ends + inner * (zone - 1) + low) * UNIT
        return pl.multiple_of(start, UNIT), (high - low) * UNIT

    def place(m, q, start, size):
        if m < 2:
            return corner_up.at[m, pl.ds(start, size), tile_of(q // 2)]
        return corner_down.at[pl.ds(start, size), pl.ds(q * TILE, TILE)]

    def fetch(i, zone):
        m, q = pieces[i]
        start, size = span(m, q, zone)
        if m < 2:
            cols = pl.ds(pl.multiple_of(core * half + q // 2 * TILE, TILE), TILE)
            src = sources[m].at[pl.ds(start, size), cols]
        else:
            first = pl.multiple_of(core * half + start, UNIT)
            src = sources[m].at[pl.ds(first, size), pl.ds(q * TILE, TILE)]
        return remote(
            src,
            place(m, q, start, size),
            part_go.at[m // 2],
            direct_come.at[i],
            {"sp": far},
        )

    def share(i, zone, way):
        m, q = pieces[i]
        start, size = span(m, q, zone)
        return remote(
            place(m, q, start, size),
            place(m, q, start, size),
            share_go.at[way, m // 2],
            middle_come.at[i] if way == 1 else near_come.at[way // 2, i // 4 if i < 8 else i - 6],
            {"tp": partner(tp, 6 if way == 1 else 2, tp_count)},
        )

    def pass_on(i):
        @pl.when(at_end)
        def _():
            fetch(i, 0).wait_recv()
            share(i, 0, 0).start()

        @pl.when(inside)
        def _():
            fetch(i, plane).wait_recv()
            share(i, plane, 1).start()
            share(i, plane, 0).start()

    def relay(i):
        @pl.when(inside)
        def _():
            share(i, 3 - plane, 1).wait_recv()
            share(i, 3 - plane, 2).start()

    def whole(zone, down):
        start, size = span(2 if down else 0, 0, zone)
        if down:
            return corner_down.at[pl.ds(start, size), :]
        size = sum(span(0, q, zone)[1] for q in range(2))
        return corner_up.at[:, pl.ds(start, size), :]

    def up_arrived(u):
        def wait_for(zone, kind):
            ref = whole(zone, False).at[:, :, tile_of(u)]
            remote(ref, ref, share_go.at[0, 0], near_come.at[kind, u], mate).wait_recv()

        @pl.when(at_end)
        def _():
            wait_for(1, 0)
            wait_for(2, 1)

        @pl.when(inside)
        def _():
            wait_for(0, 0)

    def arrived(i):
        @pl.when(at_end)
        def _():
            share(i, 1, 0).wait_recv()
            share(i, 2, 2).wait_recv()

        @pl.when(inside)
        def _():
            share(i, 0, 0).wait_recv()

    def fetch_all(some):
        @pl.when(at_end)
        def _():
            for i in some:
                fetch(i, 0).start()

        @pl.when(inside)
        def _():
            for i in some:
                fetch(i, plane).start()

    for load in loads[:2]:
        load.wait()
    pl.semaphore_wait(barrier, count - 1 + tp_count - 1)
    for edge in edges:
        edge.start()

    for load in loads[2:4]:
        load.wait()
    fetch_all(range(8))
    for load in loads[5:]:
        load.start()

    level = (tp * channels) // (channels * tp_count // 4)

    def pool_copy(j):
        return remote(
            pooled.at[j],
            gathered.at[pl.ds(pl.multiple_of(tp * channels, channels), channels), :],
            pool_go.at[0],
            pool_come.at[0],
            {"tp": partner(tp, j, tp_count)},
        )

    def pool_block(j):
        owner = partner(tp, j, tp_count)
        cols = pl.ds(pl.multiple_of(owner * rows, LANES), rows + LANES)
        values = pool[:, cols].astype(f32)
        document = jnp.broadcast_to(docs[:, cols], (8, rows + LANES))
        lane = lax.broadcasted_iota(jnp.int32, document.shape, 1)
        document = jnp.where((lane < LANES) & (owner == 0) & (sp == 0), -1, document)
        running = values
        number = jnp.ones(document.shape, f32)
        for step in range(4):
            shift = 2**step
            same = (document == pltpu.roll(document, shift, 1)) & (level >= step)
            same = same.astype(f32)
            number = number + same * pltpu.roll(number, shift, 1)
            wide = jnp.concatenate([same] * (channels // 8), axis=0)
            running = running + wide * pltpu.roll(running, shift, 1)
        share_of = jnp.concatenate([1.0 / number] * (channels // 8), axis=0)
        return (running * share_of - values)[:, LANES:].astype(bf16)

    def pool_send(j):
        pooled[j] = pool_block(j)
        pool_copy(j).start()

    def pool_step(i, carry):
        j = tp_count - 1 - i

        @pl.when(j != tp)
        def _():
            pool_send(j)

        return carry

    lax.fori_loop(0, tp_count - 1, pool_step, 0)
    loads[4].wait()
    fetch_all(range(8, 12))
    for edge in edges:
        edge.wait_recv()

    @pl.when(tp != 0)
    def _():
        pool_send(tp)

    gathered[pl.ds(pl.multiple_of(tp * channels, channels), channels), :] = pool_block(0)
    pass_on(0)

    for load in loads[5:7]:
        load.wait()

    first, second = routes_ref[0:1, :], routes_ref[1:2, :]
    weight_first, weight_second = route_weight_ref[0:1, :], route_weight_ref[1:2, :]
    named, weights = [], []
    for j in range(count):
        expert = partner(sp, j, count)
        named.append(jnp.where((first == expert) | (second == expert), 1.0, 0.0))
        weights.append(
            jnp.where(first == expert, weight_first, 0.0)
            + jnp.where(second == expert, weight_second, 0.0)
        )
    named = jnp.concatenate(named + named, axis=0)
    weights = jnp.concatenate(weights + weights, axis=0)
    before = lax.broadcasted_iota(jnp.int32, (rows, rows), 0) <= lax.broadcasted_iota(
        jnp.int32, (rows, rows), 1
    )
    place_of = jnp.dot(
        named.astype(bf16), before.astype(f32).astype(bf16), preferred_element_type=f32
    )
    place_of = jnp.where(named > 0.0, place_of - 1.0, -4.0 * cap)
    split = jnp.where(place_of >= part, place_of + part, place_of)
    line = lax.broadcasted_iota(jnp.int32, place_of.shape, 0)
    goal = jnp.where(line == 1, split, place_of)
    goal = jnp.where(line == 2, split + part, goal)
    goal = jnp.where(line == 3, place_of + cap, goal)
    goal_rows = goal.astype(jnp.int32)
    goal_cols = goal.T.astype(jnp.int32)
    weight_cols = weights.T

    slot = lax.broadcasted_iota(jnp.int32, (2 * cap, rows), 0)
    for k, (a, b) in enumerate(((1, 2), (0, 3))):
        hit = (slot == goal_rows[a : a + 1, :]) | (slot == goal_rows[b : b + 1, :])
        onehot[k] = hit.astype(f32).astype(bf16)

    def weighed(slots, j, shift):
        return jnp.where(
            slots == goal_cols[:, j : j + 1] + shift, weight_cols[:, j : j + 1], 0.0
        )

    slots = lax.broadcasted_iota(jnp.int32, (rows, cap), 1)
    pick_own[...] = weighed(slots, 0, 0).astype(bf16)
    pick_near[...] = (weighed(slots, 1, 0) + weighed(slots, 2, 0)).astype(bf16)
    slots = lax.broadcasted_iota(jnp.int32, (rows, 3 * cap), 1)
    found = weighed(slots, 3, -cap) + weighed(slots, 3, 0)
    late = jnp.where(slots >= 2 * cap, slots - cap, -1)
    found = found + weighed(late, 1, 0) + weighed(late, 2, 0)
    pick_rest[...] = found.astype(bf16)

    for i in range(1, 4):
        pass_on(i)

    for load in loads[7:]:
        load.wait()

    others = gathered.at[pl.ds(0, (tp_count - 1) * channels), :]
    remote(others, others, pool_go.at[0], pool_come.at[0], mate).wait_recv()
    tokens[...] = gathered[...].T

    def lift_up(t, carry):
        cols = tile_of(t)
        lifted = halves_dot(tokens[...], w_up[:, cols])
        gated[:, cols] = (jax.nn.sigmoid(gate_pre[:, cols].astype(f32)) * lifted).astype(bf16)
        return carry

    lax.fori_loop(0, model_dim // TILE, lift_up, 0)

    def mix(t, carry):
        cols = tile_of(t)
        added = halves_dot(gated[...], w_out[:, cols])
        mixed[:, cols] = (resid[:, cols].astype(f32) + added).astype(bf16)
        return carry

    lax.fori_loop(0, model_dim // TILE, mix, 0)

    def norm(t, carry):
        block = pl.ds(pl.multiple_of(t * 64, 64), 64)
        x = mixed[block, :].astype(f32)
        scale = lax.rsqrt(jnp.mean(x * x, axis=-1, keepdims=True) + 1e-06)
        normed[block, :] = (x * scale * gain[...]).astype(bf16)
        return carry

    for i in range(4, 6):
        pass_on(i)
    lax.fori_loop(0, rows // 64, norm, 0)

    def pack_near(t, carry):
        cols = tile_of(t)
        send[:, cols] = halves_dot(onehot[0], normed[:, cols]).astype(bf16)
        return carry

    lax.fori_loop(0, model_dim // TILE, pack_near, 0)

    def out_copy(h, p):
        block = pl.ds((2 * h + p) * part, part)
        return remote(
            send.at[block],
            recv.at[block],
            out_go.at[0],
            out_come.at[h],
            {"sp": partner(sp, p + 1, count)},
        )

    def back_copy(p):
        block = pl.ds(p * part, part)
        return remote(
            result.at[block],
            back.at[block],
            ret_go.at[0],
            ret_come.at[0],
            {"sp": partner(sp, p + 1, count)},
        )

    def late_copy(p, t):
        return remote(
            result.at[pl.ds((2 + p) * part, part), tile_of(t)],
            back.at[pl.ds(3 * cap + p * part, part), tile_of(t)],
            late_go.at[0],
            late_come.at[t],
            {"sp": partner(sp, p + 1, count)},
        )

    chunks = [(h, p) for h in range(2) for p in range(2)]
    for h, p in chunks:
        out_copy(h, p).start()

    pass_on(6)

    def pack_local(t, carry):
        cols = tile_of(t)
        packed = halves_dot(onehot[1], normed[:, cols]).astype(bf16)
        own[:, cols] = packed[:cap]
        corner[0:cap, cols] = packed[cap:]
        return carry

    lax.fori_loop(0, model_dim // TILE, pack_local, 0)
    corner_copy = remote(
        corner.at[pl.ds(0, cap)], corner.at[pl.ds(cap, cap)], core_go.at[0], core_come.at[0], mate
    )
    corner_copy.start()
    pass_on(7)

    def activate(gate, lift):
        gate = jnp.minimum(gate, 7.0)
        lift = jnp.clip(lift, -7.0, 7.0)
        return ((lift + 1.0) * gate * jax.nn.sigmoid(1.702 * gate)).astype(bf16)

    def ffn(source, target, base, then=lambda t: None):
        def up(t, carry):
            cols = tile_of(t)
            x = source[base : base + cap, :]
            act[:, cols] = activate(
                jnp.dot(x, w_gate[:, cols], preferred_element_type=f32),
                jnp.dot(x, w_lift[:, cols], preferred_element_type=f32),
            )
            return carry

        lax.fori_loop(0, hidden // TILE, up, 0)

        def down(t, carry):
            cols = tile_of(t)
            target[base : base + cap, cols] = halves_dot(act[...], w_down[:, cols]).astype(bf16)
            then(t)
            return carry

        lax.fori_loop(0, model_dim // TILE, down, 0)

    ffn(own, local_out, 0)
    pass_on(8)
    pass_on(9)

    def combine_own(t, carry):
        cols = tile_of(t)
        found = halves_dot(pick_own[...], local_out[:, cols])
        total[:, cols] = mixed[:, cols].astype(f32) + found
        return carry

    lax.fori_loop(0, model_dim // TILE, combine_own, 0)
    pass_on(10)
    pass_on(11)
    for i in range(8):
        relay(i)

    def near_arrived(h):
        block = pl.ds(h * cap, cap)
        remote(send.at[block], recv.at[block], out_go.at[0], out_come.at[h], mate).wait_recv()

    near_arrived(0)
    ffn(recv, result, 0)
    for p in range(2):
        back_copy(p).start()
    for i in range(8, 12):
        relay(i)
    near_arrived(1)

    def send_back(t):
        for p in range(2):
            late_copy(p, t).start()

    ffn(recv, result, cap, send_back)

    corner_copy.wait_recv()

    def corner_lift(t):
        cols = tile_of(t)
        x = corner[...]
        corner_act[:, cols] = activate(
            jnp.dot(x, corner_up[0, :, cols], preferred_element_type=f32),
            jnp.dot(x, corner_up[1, :, cols], preferred_element_type=f32),
        )

    def combine_near(t, carry):
        cols = tile_of(t)
        found = halves_dot(pick_near[...], back[0:cap, cols])
        total[:, cols] = total[:, cols] + found
        return carry

    tiles = model_dim // TILE
    up_arrived(0)
    corner_lift(0)
    block = pl.ds(0, cap)
    remote(result.at[block], back.at[block], ret_go.at[0], ret_come.at[0], mate).wait_recv()
    lax.fori_loop(0, tiles, combine_near, 0)
    for u in range(1, half // TILE):
        up_arrived(u)
        corner_lift(u)

    def mate_copy(t):
        return remote(
            corner_out.at[:, tile_of(t)],
            back.at[pl.ds(2 * cap, cap), tile_of(t)],
            mate_go.at[0],
            mate_come.at[t],
            mate,
        )

    def corner_drop(t):
        cols = tile_of(t)
        found = halves_dot(corner_act[...], corner_down[:, cols]).astype(bf16)
        corner_out[:, cols] = found[cap:]
        mate_copy(t).start()
        back[cap : 2 * cap, cols] = found[:cap]

    def combine_rest(t):
        cols = tile_of(t)
        mate_copy(t).wait_recv()
        block = back.at[pl.ds(3 * cap, cap), cols]
        remote(block, block, late_go.at[0], late_come.at[t], mate).wait_recv()
        found = halves_dot(pick_rest[...], back[cap:, cols])
        out_ref[:, cols] = (total[:, cols] + found).astype(bf16)

    for t in range(tiles):
        arrived(8 + t)
        corner_drop(t)
        if t > 0:
            combine_rest(t - 1)
    combine_rest(tiles - 1)

    for edge in edges:
        edge.wait_send()

    others = pooled.at[pl.ds(1, tp_count - 1)]
    remote(others, others, pool_go.at[0], pool_come.at[0], mate).wait_send()
    remote(send, recv, out_go.at[0], out_come.at[0], mate).wait_send()
    corner_copy.wait_send()
    block = pl.ds(0, cap)
    remote(result.at[block], back.at[block], ret_go.at[0], ret_come.at[0], mate).wait_send()
    block = pl.ds(cap, cap)
    remote(result.at[block], back.at[block], late_go.at[0], late_come.at[0], mate).wait_send()
    remote(corner_out, corner_out, mate_go.at[0], mate_come.at[0], mate).wait_send()

    def gone(ref, sem):
        remote(ref, ref, sem, direct_come.at[0], mate).wait_send()

    @pl.when(at_end)
    def _():
        for k in range(2):
            gone(whole(0, k), part_go.at[k])
            gone(whole(0, k), share_go.at[0, k])

    @pl.when(inside)
    def _():
        for k in range(2):
            gone(whole(plane, k), part_go.at[k])
            gone(whole(plane, k), share_go.at[0, k])
            gone(whole(plane, k), share_go.at[1, k])
            gone(whole(3 - plane, k), share_go.at[2, k])


def run_fused(
    count,
    tp_count,
    pool_input,
    gate_pre,
    resid,
    docs,
    w_up,
    w_out,
    g_ffn,
    w_gate,
    w_lift,
    w_down,
    routes,
    route_weight,
):
    tok_dev, channels = pool_input.shape
    rows, model_dim = resid.shape
    hidden = w_gate.shape[2]
    half = hidden // 2
    pool_w = w_up.shape[0]
    top = routes.shape[1]
    cap = capacity(rows, top, count)
    vmem = pl.BlockSpec(memory_space=pltpu.VMEM)
    bf16, f32 = jnp.bfloat16, jnp.float32
    hbm = functools.partial(pltpu.with_memory_space_constraint, memory_space=pltpu.HBM)
    dma = pltpu.SemaphoreType.DMA
    return pl.pallas_call(
        functools.partial(fused_kernel, count, tp_count),
        out_shape=jax.ShapeDtypeStruct((rows, model_dim), bf16),
        in_specs=[pl.BlockSpec(memory_space=pltpu.HBM)] * 12,
        out_specs=vmem,
        scratch_shapes=[
            pltpu.VMEM((channels, tok_dev + LANES), bf16),
            pltpu.VMEM((1, tok_dev + LANES), jnp.int32),
            pltpu.VMEM((top, rows), jnp.int32),
            pltpu.VMEM((top, rows), f32),
            pltpu.VMEM((1, model_dim), f32),
            pltpu.VMEM((rows, model_dim), bf16),
            pltpu.VMEM((rows, model_dim), bf16),
            pltpu.VMEM(w_up.shape, bf16),
            pltpu.VMEM(w_out.shape, bf16),
            pltpu.VMEM(w_gate.shape[1:], bf16),
            pltpu.VMEM(w_lift.shape[1:], bf16),
            pltpu.VMEM(w_down.shape[1:], bf16),
            pltpu.VMEM((tp_count, channels, rows), bf16),
            pltpu.VMEM((pool_w, rows), bf16),
            pltpu.VMEM((rows, pool_w), bf16),
            pltpu.VMEM((rows, model_dim), bf16),
            pltpu.VMEM((rows, model_dim), bf16),
            pltpu.VMEM((rows, model_dim), bf16),
            pltpu.VMEM((2, 2 * cap, rows), bf16),
            pltpu.VMEM((rows, cap), bf16),
            pltpu.VMEM((rows, cap), bf16),
            pltpu.VMEM((rows, 3 * cap), bf16),
            pltpu.VMEM((2 * cap, model_dim), bf16),
            pltpu.VMEM((2 * cap, model_dim), bf16),
            pltpu.VMEM((2 * cap, model_dim), bf16),
            pltpu.VMEM((4 * cap, model_dim), bf16),
            pltpu.VMEM((cap, model_dim), bf16),
            pltpu.VMEM((2 * cap, model_dim), bf16),
            pltpu.VMEM((cap, hidden), bf16),
            pltpu.VMEM((2 * cap, half), bf16),
            pltpu.VMEM((2, model_dim, half), bf16),
            pltpu.VMEM((half, model_dim), bf16),
            pltpu.VMEM((cap, model_dim), bf16),
            pltpu.VMEM((cap, model_dim), bf16),
            pltpu.VMEM((rows, model_dim), f32),
            dma((12,)),
            dma((2,)),
            dma((2,)),
            dma((1,)),
            dma((1,)),
            dma((2,)),
            dma((12,)),
            dma((3, 2)),
            dma((2, 6)),
            dma((12,)),
            dma((1,)),
            dma((2,)),
            dma((1,)),
            dma((1,)),
            dma((1,)),
            dma((4,)),
            dma((1,)),
            dma((4,)),
            dma((1,)),
            dma((1,)),
        ],
        compiler_params=pltpu.CompilerParams(
            collective_id=1, has_side_effects=True, vmem_limit_bytes=52 * 2**20
        ),
        cost_estimate=pl.CostEstimate(
            flops=6 * count * cap * model_dim * hidden,
            bytes_accessed=3 * model_dim * hidden * 2,
            transcendentals=count * cap * hidden,
        ),
    )(
        hbm(pool_input.T),
        hbm(docs[None, :]),
        hbm(routes.T),
        hbm(route_weight.T),
        hbm(g_ffn[None, :]),
        gate_pre,
        resid,
        w_up,
        w_out,
        w_gate,
        w_lift,
        w_down,
    )


def capacity(row_count, top_count, count):
    cap = max(2, 5 * row_count * top_count // (4 * count))
    return (cap + 15) // 16 * 16


def on_device(
    pool_input,
    gate_pre,
    resid,
    docs,
    w_up,
    w_out,
    g_ffn,
    w_gate,
    w_lift,
    w_down,
    routes,
    route_weight,
):
    tok_dev = pool_input.shape[0]
    channels = pool_input.shape[1]
    group_size = POOL_W // 4
    channel_ids = lax.axis_index("tp") * channels + lax.iota(jnp.int32, channels)
    window = jnp.power(2, channel_ids // group_size + 1)
    edge = jnp.concatenate(
        [pool_input[tok_dev - RIM :], docs[tok_dev - RIM :, None].astype(jnp.bfloat16)], axis=1
    )
    before = shifted_2(edge, "sp", 1)
    before_rows = before[:, :channels]
    before_docs = before[:, channels].astype(jnp.int32)
    first_dev = lax.axis_index("sp") == 0
    before_docs = jnp.where(first_dev, -1, before_docs)
    values = pool_input.astype(jnp.float32)
    padded = jnp.concatenate([before_rows.astype(jnp.float32), values], axis=0)
    doc_padded = jnp.concatenate([before_docs.astype(jnp.int32), docs], axis=0)
    earlier = sum(
        (doc_padded[RIM - offset : RIM - offset + tok_dev] == docs).astype(jnp.int32)
        for offset in range(1, RIM + 1)
    )
    reach = jnp.minimum(earlier[:, None] + 1, window[None, :])
    running = values
    for offset in range(1, RIM + 1):
        shifted = padded[RIM - offset : RIM - offset + tok_dev]
        running = running + jnp.where(offset < reach, shifted, 0.0)
    counts = reach.astype(jnp.float32)
    pooled = (running / counts - values).astype(jnp.bfloat16)
    tokens_pooled = lax.all_to_all(pooled, "tp", split_axis=0, concat_axis=1, tiled=True)
    lifted = jnp.dot(tokens_pooled, w_up, preferred_element_type=jnp.float32)
    gated_rows = (jax.nn.sigmoid(gate_pre.astype(jnp.float32)) * lifted).astype(jnp.bfloat16)
    mixed_rows = (
        resid.astype(jnp.float32) + jnp.dot(gated_rows, w_out, preferred_element_type=jnp.float32)
    ).astype(jnp.bfloat16)

    row_count, top_count = routes.shape
    count = lax.axis_size("sp")
    cap = capacity(row_count, top_count, count)
    order = partner(lax.axis_index("sp"), lax.iota(jnp.int32, count), count)
    chosen = routes[:, :, None] == order[None, None, :]
    named = jnp.any(chosen, axis=1)
    rank = jnp.where(named, jnp.cumsum(named.astype(jnp.int32), axis=0) - 1, -1)
    weight = jnp.sum(jnp.where(chosen, route_weight[:, :, None], 0.0), axis=1)
    return run_experts(mixed_rows, g_ffn, rank, weight, w_gate, w_lift, w_down, cap, count)


def solution(mesh):
    in_specs = (
        P("sp", "tp"),
        P(("sp", "tp"), None),
        P(("sp", "tp"), None),
        P("sp"),
        P(),
        P(),
        P(),
        P("sp", None, None),
        P("sp", None, None),
        P("sp", None, None),
        P(("sp", "tp"), None),
        P(("sp", "tp"), None),
    )
    out_specs = P(("sp", "tp"), None)
    count, tp_count = mesh.shape["sp"], mesh.shape["tp"]
    body = on_device
    if count == 4 and tp_count == 8:
        body = functools.partial(run_fused, count, tp_count)
    return jax.shard_map(
        body, mesh=mesh, in_specs=in_specs, out_specs=out_specs, check_vma=False
    )
```

```python
import functools

import jax
import jax.numpy as jnp
from jax import lax
from jax.experimental import pallas as pl
from jax.experimental.pallas import tpu as pltpu
from jax.sharding import PartitionSpec as P

POOL_W = 512
RIM = 15
TILE = 256
LANES = 128
UNIT = 16
END_SHARE = (11, 11, 12)
MESH = pl.DeviceIdType.MESH


def shifted_2(value, axis, steps):
    count = lax.axis_size(axis)
    leading, last = (max(0, -steps), min(count, count - steps))
    return lax.ppermute(value, axis, [(source, source + steps) for source in range(leading, last)])


def partner(me, step, count):
    other, bit = 0, 1
    while bit < count:
        other = other + ((me // bit + step // bit) % 2) * bit
        bit *= 2
    return other


def tile_of(t):
    return pl.ds(pl.multiple_of(t * TILE, TILE), TILE)


def experts_kernel(
    count,
    mixed_ref,
    gain_ref,
    rank_rows_ref,
    rank_cols_ref,
    weight_ref,
    w_gate_hbm,
    w_lift_hbm,
    w_down_hbm,
    out_ref,
    normed,
    onehot,
    send,
    recv,
    result,
    back,
    total,
    act,
    w_gate,
    w_lift,
    w_down,
    weight_sems,
    go_sems,
    come_sems,
    ret_go_sems,
    ret_come_sems,
):
    rows, model_dim = mixed_ref.shape
    cap = send.shape[1]
    hidden = w_gate.shape[1]
    me = lax.axis_index("sp")
    loads = [
        pltpu.make_async_copy(src.at[0], dst, weight_sems.at[i])
        for i, (src, dst) in enumerate(
            ((w_gate_hbm, w_gate), (w_lift_hbm, w_lift), (w_down_hbm, w_down))
        )
    ]

    barrier = pltpu.get_barrier_semaphore()

    def greet(j, carry):
        pl.semaphore_signal(
            barrier, inc=1, device_id={"sp": partner(me, j, count)}, device_id_type=MESH
        )
        return carry

    lax.fori_loop(1, count, greet, 0)
    for load in loads:
        load.start()

    def norm(t, carry):
        block = pl.ds(pl.multiple_of(t * 64, 64), 64)
        x = mixed_ref[block, :].astype(jnp.float32)
        scale = lax.rsqrt(jnp.mean(x * x, axis=-1, keepdims=True) + 1e-06)
        normed[block, :] = (x * scale * gain_ref[...]).astype(jnp.bfloat16)
        return carry

    lax.fori_loop(0, rows // 64, norm, 0)

    def out_copy(j):
        return pltpu.make_async_remote_copy(
            src_ref=send.at[j],
            dst_ref=recv.at[j],
            send_sem=go_sems.at[j],
            recv_sem=come_sems.at[j],
            device_id={"sp": partner(me, j, count)},
            device_id_type=MESH,
        )

    def back_copy(j):
        return pltpu.make_async_remote_copy(
            src_ref=result.at[j],
            dst_ref=back.at[j],
            send_sem=ret_go_sems.at[j],
            recv_sem=ret_come_sems.at[j],
            device_id={"sp": partner(me, j, count)},
            device_id_type=MESH,
        )

    def pack(j, target):
        slot = lax.broadcasted_iota(jnp.int32, (cap, rows), 0)
        onehot[...] = (slot == rank_rows_ref[j]).astype(jnp.float32).astype(jnp.bfloat16)

        def piece(t, carry):
            cols = tile_of(t)
            target[j, :, cols] = jnp.dot(
                onehot[...], normed[:, cols], preferred_element_type=jnp.float32
            ).astype(jnp.bfloat16)
            return carry

        lax.fori_loop(0, model_dim // TILE, piece, 0)

    def ffn(j, source):
        def up(t, carry):
            cols = tile_of(t)
            x = source[j]
            gate = jnp.minimum(jnp.dot(x, w_gate[:, cols], preferred_element_type=jnp.float32), 7.0)
            lift = jnp.clip(
                jnp.dot(x, w_lift[:, cols], preferred_element_type=jnp.float32), -7.0, 7.0
            )
            act[:, cols] = ((lift + 1.0) * gate * jax.nn.sigmoid(1.702 * gate)).astype(jnp.bfloat16)
            return carry

        lax.fori_loop(0, hidden // TILE, up, 0)

        def down(t, carry):
            cols = tile_of(t)
            result[j, :, cols] = jnp.dot(
                act[...], w_down[:, cols], preferred_element_type=jnp.float32
            ).astype(jnp.bfloat16)
            return carry

        lax.fori_loop(0, model_dim // TILE, down, 0)

    def column(ref, j):
        lane = lax.broadcasted_iota(jnp.int32, ref.shape, 1)
        return jnp.sum(jnp.where(lane == j, ref[...], 0.0), axis=1, keepdims=True)

    def combine(j, source, store):
        rank = column(rank_cols_ref, j).astype(jnp.int32)
        weight = column(weight_ref, j)
        slot = lax.broadcasted_iota(jnp.int32, (rows, cap), 1)
        pick = (slot == rank).astype(jnp.float32).astype(jnp.bfloat16)

        def piece(t, carry):
            cols = tile_of(t)
            found = jnp.dot(pick, source[j, :, cols], preferred_element_type=jnp.float32)
            store(cols, weight * found)
            return carry

        lax.fori_loop(0, model_dim // TILE, piece, 0)

    def store_first(cols, term):
        total[:, cols] = mixed_ref[:, cols].astype(jnp.float32) + term

    def store_more(cols, term):
        total[:, cols] = total[:, cols] + term

    def store_last(cols, term):
        out_ref[:, cols] = (total[:, cols] + term).astype(jnp.bfloat16)

    pl.semaphore_wait(barrier, count - 1)

    def dispatch(j, carry):
        pack(j, send)
        out_copy(j).start()
        return carry

    lax.fori_loop(1, count, dispatch, 0)
    pack(0, send)
    for load in loads:
        load.wait()
    ffn(0, send)
    combine(0, result, store_first)

    def serve(j, carry):
        out_copy(j).wait_recv()
        ffn(j, recv)
        back_copy(j).start()
        return carry

    lax.fori_loop(1, count, serve, 0)

    def gather(j, carry):
        back_copy(j).wait_recv()
        combine(j, back, store_more)
        return carry

    lax.fori_loop(1, count - 1, gather, 0)
    back_copy(count - 1).wait_recv()
    combine(count - 1, back, store_last)

    def finish(j, carry):
        out_copy(j).wait_send()
        back_copy(j).wait_send()
        return carry

    lax.fori_loop(1, count, finish, 0)


def run_experts(mixed, gain, rank, weight, w_gate, w_lift, w_down, cap, count):
    rows, model_dim = mixed.shape
    hidden = w_gate.shape[2]
    vmem = pl.BlockSpec(memory_space=pltpu.VMEM)
    anywhere = pl.BlockSpec(memory_space=pl.ANY)
    slots = pltpu.VMEM((count, cap, model_dim), jnp.bfloat16)
    return pl.pallas_call(
        functools.partial(experts_kernel, count),
        out_shape=jax.ShapeDtypeStruct((rows, model_dim), jnp.bfloat16),
        in_specs=[vmem] * 5 + [anywhere] * 3,
        out_specs=vmem,
        scratch_shapes=[
            pltpu.VMEM((rows, model_dim), jnp.bfloat16),
            pltpu.VMEM((cap, rows), jnp.bfloat16),
            slots,
            slots,
            slots,
            slots,
            pltpu.VMEM((rows, model_dim), jnp.float32),
            pltpu.VMEM((cap, hidden), jnp.bfloat16),
            pltpu.VMEM(w_gate.shape[1:], jnp.bfloat16),
            pltpu.VMEM(w_lift.shape[1:], jnp.bfloat16),
            pltpu.VMEM(w_down.shape[1:], jnp.bfloat16),
            pltpu.SemaphoreType.DMA((3,)),
            pltpu.SemaphoreType.DMA((count,)),
            pltpu.SemaphoreType.DMA((count,)),
            pltpu.SemaphoreType.DMA((count,)),
            pltpu.SemaphoreType.DMA((count,)),
        ],
        compiler_params=pltpu.CompilerParams(
            collective_id=0, has_side_effects=True, vmem_limit_bytes=60 * 2**20
        ),
        cost_estimate=pl.CostEstimate(
            flops=6 * count * cap * model_dim * hidden,
            bytes_accessed=3 * model_dim * hidden * 2,
            transcendentals=count * cap * hidden,
        ),
    )(
        mixed,
        gain[None, :],
        rank.T[:, None, :],
        rank.astype(jnp.float32),
        weight,
        w_gate,
        w_lift,
        w_down,
    )


def halves_dot(rows, weights):
    half = rows.shape[0] // 2
    parts = [
        jnp.dot(part, weights, preferred_element_type=jnp.float32)
        for part in (rows[:half], rows[half:])
    ]
    return jnp.concatenate(parts, axis=0)


def fused_kernel(
    count,
    tp_count,
    pool_hbm,
    docs_hbm,
    routes_hbm,
    route_weight_hbm,
    gain_hbm,
    gate_hbm,
    resid_hbm,
    w_up_hbm,
    w_out_hbm,
    w_gate_hbm,
    w_lift_hbm,
    w_down_hbm,
    out_ref,
    pool,
    docs,
    routes_ref,
    route_weight_ref,
    gain,
    gate_pre,
    resid,
    w_up,
    w_out,
    w_gate,
    w_lift,
    w_down,
    pooled,
    gathered,
    tokens,
    gated,
    mixed,
    normed,
    onehot,
    pick_own,
    pick_near,
    pick_rest,
    send,
    recv,
    result,
    back,
    own,
    corner,
    act,
    corner_act,
    corner_up,
    corner_down,
    corner_out,
    local_out,
    total,
    load_sems,
    edge_go,
    edge_come,
    pool_go,
    pool_come,
    part_go,
    direct_come,
    share_go,
    near_come,
    middle_come,
    out_go,
    out_come,
    ret_go,
    ret_come,
    late_go,
    late_come,
    mate_go,
    mate_come,
    core_go,
    core_come,
):
    channels = pool_hbm.shape[0]
    rows, model_dim = resid.shape
    hidden = w_gate.shape[1]
    half = hidden // 2
    cap = own.shape[0]
    part = cap // 2
    sp, tp = lax.axis_index("sp"), lax.axis_index("tp")
    plane, core = tp // 2, tp % 2
    planes = tp_count // 2
    at_end = (plane == 0) | (plane == planes - 1)
    inside = (plane > 0) & (plane < planes - 1)
    f32, bf16 = jnp.float32, jnp.bfloat16

    loads = [
        pltpu.make_async_copy(src, dst, load_sems.at[i])
        for i, (src, dst) in enumerate(
            (
                (pool_hbm, pool.at[:, LANES:]),
                (docs_hbm, docs.at[:, LANES:]),
                (w_gate_hbm.at[0], w_gate),
                (w_lift_hbm.at[0], w_lift),
                (w_down_hbm.at[0], w_down),
                (routes_hbm, routes_ref),
                (route_weight_hbm, route_weight_ref),
                (w_up_hbm, w_up),
                (gate_hbm, gate_pre),
                (w_out_hbm, w_out),
                (resid_hbm, resid),
                (gain_hbm, gain),
            )
        )
    ]
    for load in loads[:5]:
        load.start()
    barrier = pltpu.get_barrier_semaphore()

    def greet_sp(j, carry):
        pl.semaphore_signal(
            barrier, inc=1, device_id={"sp": partner(sp, j, count)}, device_id_type=MESH
        )
        return carry

    def greet_tp(j, carry):
        pl.semaphore_signal(
            barrier, inc=1, device_id={"tp": partner(tp, j, tp_count)}, device_id_type=MESH
        )
        return carry

    lax.fori_loop(1, count, greet_sp, 0)
    lax.fori_loop(1, tp_count, greet_tp, 0)
    def remote(src, dst, go, come, device):
        return pltpu.make_async_remote_copy(
            src_ref=src,
            dst_ref=dst,
            send_sem=go,
            recv_sem=come,
            device_id=device,
            device_id_type=MESH,
        )

    mate = {"tp": partner(tp, 1, tp_count)}
    following = {"sp": lax.rem(sp + 1, count)}
    tok_dev = pool_hbm.shape[1]
    edges = [
        remote(
            ref.at[:, pl.ds(tok_dev, LANES)],
            ref.at[:, pl.ds(0, LANES)],
            edge_go.at[i],
            edge_come.at[i],
            following,
        )
        for i, ref in enumerate((pool, docs))
    ]

    pieces = [(m, q) for q in range(4) for m in range(2)] + [(2, q) for q in range(4)]
    groups = [range(0, 1), range(1, 4)] + [range(i, i + 2) for i in range(4, 12, 2)]
    group_of = [g for g, some in enumerate(groups) for _ in some]
    sources = (w_gate, w_lift, w_down)
    far = partner(sp, 3, count)

    def span(m, q, zone):
        units = (model_dim if m < 2 else half) // UNIT
        ends = units * END_SHARE[m] // 32
        inner = (units - ends) // 2
        is_end = isinstance(zone, int) and zone == 0
        size = ends if is_end else inner
        low, high = (q % 2 * size // 2, (q % 2 + 1) * size // 2) if m < 2 else (0, size)
        if is_end:
            return low * UNIT, (high - low) * UNIT
        start = (ends + inner * (zone - 1) + low) * UNIT
        return pl.multiple_of(start, UNIT), (high - low) * UNIT

    def place(m, q, start, size):
        if m < 2:
            return corner_up.at[m, pl.ds(start, size), tile_of(q // 2)]
        return corner_down.at[pl.ds(start, size), pl.ds(q * TILE, TILE)]

    def fetch(i, zone):
        m, q = pieces[i]
        start, size = span(m, q, zone)
        if m < 2:
            cols = pl.ds(pl.multiple_of(core * half + q // 2 * TILE, TILE), TILE)
            src = sources[m].at[pl.ds(start, size), cols]
        else:
            first = pl.multiple_of(core * half + start, UNIT)
            src = sources[m].at[pl.ds(first, size), pl.ds(q * TILE, TILE)]
        return remote(
            src,
            place(m, q, start, size),
            part_go.at[m // 2],
            direct_come.at[group_of[i]],
            {"sp": far},
        )

    def share(i, zone, way):
        m, q = pieces[i]
        start, size = span(m, q, zone)
        return remote(
            place(m, q, start, size),
            place(m, q, start, size),
            share_go.at[way, m // 2],
            middle_come.at[i // 8] if way == 1 else near_come.at[i // 4 if i < 8 else i - 6],
            {"tp": partner(tp, 6 if way == 1 else 2, tp_count)},
        )

    def bytes_of(some, zones):
        size = sum(span(*pieces[i], zone)[1] for i in some for zone in zones)
        if size > model_dim:
            return corner_up.at[0, pl.ds(0, size // 2), :]
        return corner_up.at[0, pl.ds(0, size), tile_of(0)]

    def take(some, zones, sem):
        ref = bytes_of(some, zones)
        remote(ref, ref, share_go.at[0, 0], sem, mate).wait_recv()

    def pass_on(g):
        @pl.when(at_end)
        def _():
            take(groups[g], (0,), direct_come.at[g])
            for i in groups[g]:
                share(i, 0, 0).start()

        @pl.when(inside)
        def _():
            take(groups[g], (1,), direct_come.at[g])
            for i in groups[g]:
                share(i, plane, 1).start()
                share(i, plane, 0).start()

    def relay(some):
        @pl.when(inside)
        def _():
            take(some, (1,), middle_come.at[some[0] // 8])
            for i in some:
                share(i, 3 - plane, 2).start()

    def arrived(some, k):
        @pl.when(at_end)
        def _():
            take(some, (1, 2), near_come.at[k])

        @pl.when(inside)
        def _():
            take(some, (0,), near_come.at[k])

    def fetch_all(some):
        @pl.when(at_end)
        def _():
            for i in some:
                fetch(i, 0).start()

        @pl.when(inside)
        def _():
            for i in some:
                fetch(i, plane).start()

    for load in loads[:2]:
        load.wait()
    pl.semaphore_wait(barrier, count - 1 + tp_count - 1)
    for edge in edges:
        edge.start()

    for load in loads[2:4]:
        load.wait()
    fetch_all(range(8))
    for load in loads[5:]:
        load.start()

    level = (tp * channels) // (channels * tp_count // 4)

    def pool_copy(j):
        return remote(
            pooled.at[j],
            gathered.at[pl.ds(pl.multiple_of(tp * channels, channels), channels), :],
            pool_go.at[0],
            pool_come.at[0],
            {"tp": partner(tp, j, tp_count)},
        )

    def pool_block(j):
        owner = partner(tp, j, tp_count)
        cols = pl.ds(pl.multiple_of(owner * rows, LANES), rows + LANES)
        values = pool[:, cols].astype(f32)
        document = jnp.broadcast_to(docs[:, cols], (8, rows + LANES))
        lane = lax.broadcasted_iota(jnp.int32, document.shape, 1)
        document = jnp.where((lane < LANES) & (owner == 0) & (sp == 0), -1, document)
        running = values
        number = jnp.ones(document.shape, f32)
        for step in range(4):
            shift = 2**step
            same = (document == pltpu.roll(document, shift, 1)) & (level >= step)
            same = same.astype(f32)
            number = number + same * pltpu.roll(number, shift, 1)
            wide = jnp.concatenate([same] * (channels // 8), axis=0)
            running = running + wide * pltpu.roll(running, shift, 1)
        share_of = jnp.concatenate([1.0 / number] * (channels // 8), axis=0)
        return (running * share_of - values)[:, LANES:].astype(bf16)

    def pool_send(j):
        pooled[j] = pool_block(j)
        pool_copy(j).start()

    def pool_step(i, carry):
        j = lax.rem(i + 1, tp_count - 1) + 1

        @pl.when(j != tp)
        def _():
            pool_send(j)

        return carry

    lax.fori_loop(0, tp_count - 1, pool_step, 0)
    loads[4].wait()
    fetch_all(range(8, 12))
    for edge in edges:
        edge.wait_recv()

    @pl.when(tp != 0)
    def _():
        pool_send(tp)

    gathered[pl.ds(pl.multiple_of(tp * channels, channels), channels), :] = pool_block(0)
    pass_on(0)

    for load in loads[5:7]:
        load.wait()

    first, second = routes_ref[0:1, :], routes_ref[1:2, :]
    weight_first, weight_second = route_weight_ref[0:1, :], route_weight_ref[1:2, :]
    named, weights = [], []
    for j in range(count):
        expert = partner(sp, j, count)
        named.append(jnp.where((first == expert) | (second == expert), 1.0, 0.0))
        weights.append(
            jnp.where(first == expert, weight_first, 0.0)
            + jnp.where(second == expert, weight_second, 0.0)
        )
    named = jnp.concatenate(named + named, axis=0)
    weights = jnp.concatenate(weights + weights, axis=0)
    before = lax.broadcasted_iota(jnp.int32, (rows, rows), 0) <= lax.broadcasted_iota(
        jnp.int32, (rows, rows), 1
    )
    place_of = jnp.dot(
        named.astype(bf16), before.astype(f32).astype(bf16), preferred_element_type=f32
    )
    place_of = jnp.where(named > 0.0, place_of - 1.0, -4.0 * cap)
    split = jnp.where(place_of >= part, place_of + part, place_of)
    line = lax.broadcasted_iota(jnp.int32, place_of.shape, 0)
    goal = jnp.where(line == 1, split, place_of)
    goal = jnp.where(line == 2, split + part, goal)
    goal = jnp.where(line == 3, place_of + cap, goal)
    goal_rows = goal.astype(jnp.int32)
    goal_cols = goal.T.astype(jnp.int32)
    weight_cols = weights.T

    slot = lax.broadcasted_iota(jnp.int32, (2 * cap, rows), 0)
    for k, (a, b) in enumerate(((1, 2), (0, 3))):
        hit = (slot == goal_rows[a : a + 1, :]) | (slot == goal_rows[b : b + 1, :])
        onehot[k] = hit.astype(f32).astype(bf16)

    def weighed(slots, j, shift):
        return jnp.where(
            slots == goal_cols[:, j : j + 1] + shift, weight_cols[:, j : j + 1], 0.0
        )

    slots = lax.broadcasted_iota(jnp.int32, (rows, cap), 1)
    pick_own[...] = weighed(slots, 0, 0).astype(bf16)
    pick_near[...] = (weighed(slots, 1, 0) + weighed(slots, 2, 0)).astype(bf16)
    slots = lax.broadcasted_iota(jnp.int32, (rows, 3 * cap), 1)
    found = weighed(slots, 3, -cap) + weighed(slots, 3, 0)
    late = jnp.where(slots >= 2 * cap, slots - cap, -1)
    found = found + weighed(late, 1, 0) + weighed(late, 2, 0)
    pick_rest[...] = found.astype(bf16)

    pass_on(1)

    for load in loads[7:]:
        load.wait()

    others = gathered.at[pl.ds(0, (tp_count - 1) * channels), :]
    remote(others, others, pool_go.at[0], pool_come.at[0], mate).wait_recv()
    tokens[...] = gathered[...].T

    def lift_up(t, carry):
        cols = tile_of(t)
        lifted = halves_dot(tokens[...], w_up[:, cols])
        gated[:, cols] = (jax.nn.sigmoid(gate_pre[:, cols].astype(f32)) * lifted).astype(bf16)
        return carry

    lax.fori_loop(0, model_dim // TILE, lift_up, 0)

    def mix(t, carry):
        cols = tile_of(t)
        added = halves_dot(gated[...], w_out[:, cols])
        mixed[:, cols] = (resid[:, cols].astype(f32) + added).astype(bf16)
        return carry

    lax.fori_loop(0, model_dim // TILE, mix, 0)

    def norm(t, carry):
        block = pl.ds(pl.multiple_of(t * 64, 64), 64)
        x = mixed[block, :].astype(f32)
        scale = lax.rsqrt(jnp.mean(x * x, axis=-1, keepdims=True) + 1e-06)
        normed[block, :] = (x * scale * gain[...]).astype(bf16)
        return carry

    pass_on(2)
    lax.fori_loop(0, rows // 64, norm, 0)

    def pack_near(t, carry):
        cols = tile_of(t)
        send[:, cols] = halves_dot(onehot[0], normed[:, cols]).astype(bf16)
        return carry

    lax.fori_loop(0, model_dim // TILE, pack_near, 0)

    def out_copy(h, p):
        block = pl.ds((2 * h + p) * part, part)
        return remote(
            send.at[block],
            recv.at[block],
            out_go.at[0],
            out_come.at[h],
            {"sp": partner(sp, p + 1, count)},
        )

    def back_copy(p):
        block = pl.ds(p * part, part)
        return remote(
            result.at[block],
            back.at[block],
            ret_go.at[0],
            ret_come.at[0],
            {"sp": partner(sp, p + 1, count)},
        )

    def late_copy(p, t):
        return remote(
            result.at[pl.ds((2 + p) * part, part), tile_of(t)],
            back.at[pl.ds(3 * cap + p * part, part), tile_of(t)],
            late_go.at[0],
            late_come.at[t],
            {"sp": partner(sp, p + 1, count)},
        )

    chunks = [(h, p) for h in range(2) for p in range(2)]
    for h, p in chunks:
        out_copy(h, p).start()

    def pack_local(t, carry):
        cols = tile_of(t)
        packed = halves_dot(onehot[1], normed[:, cols]).astype(bf16)
        own[:, cols] = packed[:cap]
        corner[0:cap, cols] = packed[cap:]
        return carry

    lax.fori_loop(0, model_dim // TILE, pack_local, 0)
    corner_copy = remote(
        corner.at[pl.ds(0, cap)], corner.at[pl.ds(cap, cap)], core_go.at[0], core_come.at[0], mate
    )
    corner_copy.start()
    pass_on(3)

    def activate(gate, lift):
        gate = jnp.minimum(gate, 7.0)
        lift = jnp.clip(lift, -7.0, 7.0)
        return ((lift + 1.0) * gate * jax.nn.sigmoid(1.702 * gate)).astype(bf16)

    def ffn(source, target, base, then=lambda t: None):
        def up(t, carry):
            cols = tile_of(t)
            x = source[base : base + cap, :]
            act[:, cols] = activate(
                jnp.dot(x, w_gate[:, cols], preferred_element_type=f32),
                jnp.dot(x, w_lift[:, cols], preferred_element_type=f32),
            )
            return carry

        lax.fori_loop(0, hidden // TILE, up, 0)

        def down(t, carry):
            cols = tile_of(t)
            target[base : base + cap, cols] = halves_dot(act[...], w_down[:, cols]).astype(bf16)
            then(t)
            return carry

        lax.fori_loop(0, model_dim // TILE, down, 0)

    ffn(own, local_out, 0)
    pass_on(4)

    def combine_own(t, carry):
        cols = tile_of(t)
        found = halves_dot(pick_own[...], local_out[:, cols])
        total[:, cols] = mixed[:, cols].astype(f32) + found
        return carry

    lax.fori_loop(0, model_dim // TILE, combine_own, 0)
    pass_on(5)
    relay(range(8))

    def near_arrived(h):
        block = pl.ds(h * cap, cap)
        remote(send.at[block], recv.at[block], out_go.at[0], out_come.at[h], mate).wait_recv()

    near_arrived(0)
    ffn(recv, result, 0)
    for p in range(2):
        back_copy(p).start()
    relay(range(8, 12))
    near_arrived(1)

    def send_back(t):
        for p in range(2):
            late_copy(p, t).start()

    ffn(recv, result, cap, send_back)

    corner_copy.wait_recv()

    def corner_lift(t):
        cols = tile_of(t)
        x = corner[...]
        corner_act[:, cols] = activate(
            jnp.dot(x, corner_up[0, :, cols], preferred_element_type=f32),
            jnp.dot(x, corner_up[1, :, cols], preferred_element_type=f32),
        )

    def combine_near(t, carry):
        cols = tile_of(t)
        found = halves_dot(pick_near[...], back[0:cap, cols])
        total[:, cols] = total[:, cols] + found
        return carry

    tiles = model_dim // TILE
    arrived(range(4), 0)
    corner_lift(0)
    block = pl.ds(0, cap)
    remote(result.at[block], back.at[block], ret_go.at[0], ret_come.at[0], mate).wait_recv()
    lax.fori_loop(0, tiles, combine_near, 0)
    for u in range(1, half // TILE):
        arrived(range(4 * u, 4 * u + 4), u)
        corner_lift(u)

    def mate_copy(t):
        return remote(
            corner_out.at[:, tile_of(t)],
            back.at[pl.ds(2 * cap, cap), tile_of(t)],
            mate_go.at[0],
            mate_come.at[t],
            mate,
        )

    def corner_drop(t):
        cols = tile_of(t)
        found = halves_dot(corner_act[...], corner_down[:, cols]).astype(bf16)
        corner_out[:, cols] = found[cap:]
        mate_copy(t).start()
        back[cap : 2 * cap, cols] = found[:cap]

    def combine_rest(t):
        cols = tile_of(t)
        mate_copy(t).wait_recv()
        block = back.at[pl.ds(3 * cap, cap), cols]
        remote(block, block, late_go.at[0], late_come.at[t], mate).wait_recv()
        found = halves_dot(pick_rest[...], back[cap:, cols])
        out_ref[:, cols] = (total[:, cols] + found).astype(bf16)

    for t in range(tiles):
        arrived(range(8 + t, 9 + t), 2 + t)
        corner_drop(t)
        if t > 0:
            combine_rest(t - 1)
    combine_rest(tiles - 1)

    for edge in edges:
        edge.wait_send()

    others = pooled.at[pl.ds(1, tp_count - 1)]
    remote(others, others, pool_go.at[0], pool_come.at[0], mate).wait_send()
    remote(send, recv, out_go.at[0], out_come.at[0], mate).wait_send()
    corner_copy.wait_send()
    block = pl.ds(0, cap)
    remote(result.at[block], back.at[block], ret_go.at[0], ret_come.at[0], mate).wait_send()
    block = pl.ds(cap, cap)
    remote(result.at[block], back.at[block], late_go.at[0], late_come.at[0], mate).wait_send()
    remote(corner_out, corner_out, mate_go.at[0], mate_come.at[0], mate).wait_send()

    def gone(zone, sems):
        for k, some in enumerate((range(8), range(8, 12))):
            ref = bytes_of(some, (zone,))
            remote(ref, ref, sems.at[k], direct_come.at[0], mate).wait_send()

    @pl.when(at_end)
    def _():
        gone(0, part_go)
        gone(0, share_go.at[0])

    @pl.when(inside)
    def _():
        gone(1, part_go)
        for way in range(3):
            gone(1, share_go.at[way])


def run_fused(
    count,
    tp_count,
    pool_input,
    gate_pre,
    resid,
    docs,
    w_up,
    w_out,
    g_ffn,
    w_gate,
    w_lift,
    w_down,
    routes,
    route_weight,
):
    tok_dev, channels = pool_input.shape
    rows, model_dim = resid.shape
    hidden = w_gate.shape[2]
    half = hidden // 2
    pool_w = w_up.shape[0]
    top = routes.shape[1]
    cap = capacity(rows, top, count)
    vmem = pl.BlockSpec(memory_space=pltpu.VMEM)
    bf16, f32 = jnp.bfloat16, jnp.float32
    hbm = functools.partial(pltpu.with_memory_space_constraint, memory_space=pltpu.HBM)
    dma = pltpu.SemaphoreType.DMA
    return pl.pallas_call(
        functools.partial(fused_kernel, count, tp_count),
        out_shape=jax.ShapeDtypeStruct((rows, model_dim), bf16),
        in_specs=[pl.BlockSpec(memory_space=pltpu.HBM)] * 12,
        out_specs=vmem,
        scratch_shapes=[
            pltpu.VMEM((channels, tok_dev + LANES), bf16),
            pltpu.VMEM((1, tok_dev + LANES), jnp.int32),
            pltpu.VMEM((top, rows), jnp.int32),
            pltpu.VMEM((top, rows), f32),
            pltpu.VMEM((1, model_dim), f32),
            pltpu.VMEM((rows, model_dim), bf16),
            pltpu.VMEM((rows, model_dim), bf16),
            pltpu.VMEM(w_up.shape, bf16),
            pltpu.VMEM(w_out.shape, bf16),
            pltpu.VMEM(w_gate.shape[1:], bf16),
            pltpu.VMEM(w_lift.shape[1:], bf16),
            pltpu.VMEM(w_down.shape[1:], bf16),
            pltpu.VMEM((tp_count, channels, rows), bf16),
            pltpu.VMEM((pool_w, rows), bf16),
            pltpu.VMEM((rows, pool_w), bf16),
            pltpu.VMEM((rows, model_dim), bf16),
            pltpu.VMEM((rows, model_dim), bf16),
            pltpu.VMEM((rows, model_dim), bf16),
            pltpu.VMEM((2, 2 * cap, rows), bf16),
            pltpu.VMEM((rows, cap), bf16),
            pltpu.VMEM((rows, cap), bf16),
            pltpu.VMEM((rows, 3 * cap), bf16),
            pltpu.VMEM((2 * cap, model_dim), bf16),
            pltpu.VMEM((2 * cap, model_dim), bf16),
            pltpu.VMEM((2 * cap, model_dim), bf16),
            pltpu.VMEM((4 * cap, model_dim), bf16),
            pltpu.VMEM((cap, model_dim), bf16),
            pltpu.VMEM((2 * cap, model_dim), bf16),
            pltpu.VMEM((cap, hidden), bf16),
            pltpu.VMEM((2 * cap, half), bf16),
            pltpu.VMEM((2, model_dim, half), bf16),
            pltpu.VMEM((half, model_dim), bf16),
            pltpu.VMEM((cap, model_dim), bf16),
            pltpu.VMEM((cap, model_dim), bf16),
            pltpu.VMEM((rows, model_dim), f32),
            dma((12,)),
            dma((2,)),
            dma((2,)),
            dma((1,)),
            dma((1,)),
            dma((2,)),
            dma((6,)),
            dma((3, 2)),
            dma((6,)),
            dma((2,)),
            dma((1,)),
            dma((2,)),
            dma((1,)),
            dma((1,)),
            dma((1,)),
            dma((4,)),
            dma((1,)),
            dma((4,)),
            dma((1,)),
            dma((1,)),
        ],
        compiler_params=pltpu.CompilerParams(
            collective_id=1, has_side_effects=True, vmem_limit_bytes=52 * 2**20
        ),
        cost_estimate=pl.CostEstimate(
            flops=6 * count * cap * model_dim * hidden,
            bytes_accessed=3 * model_dim * hidden * 2,
            transcendentals=count * cap * hidden,
        ),
    )(
        hbm(pool_input.T),
        hbm(docs[None, :]),
        hbm(routes.T),
        hbm(route_weight.T),
        hbm(g_ffn[None, :]),
        gate_pre,
        resid,
        w_up,
        w_out,
        w_gate,
        w_lift,
        w_down,
    )


def capacity(row_count, top_count, count):
    cap = max(2, 5 * row_count * top_count // (4 * count))
    return (cap + 15) // 16 * 16


def on_device(
    pool_input,
    gate_pre,
    resid,
    docs,
    w_up,
    w_out,
    g_ffn,
    w_gate,
    w_lift,
    w_down,
    routes,
    route_weight,
):
    tok_dev = pool_input.shape[0]
    channels = pool_input.shape[1]
    group_size = POOL_W // 4
    channel_ids = lax.axis_index("tp") * channels + lax.iota(jnp.int32, channels)
    window = jnp.power(2, channel_ids // group_size + 1)
    edge = jnp.concatenate(
        [pool_input[tok_dev - RIM :], docs[tok_dev - RIM :, None].astype(jnp.bfloat16)], axis=1
    )
    before = shifted_2(edge, "sp", 1)
    before_rows = before[:, :channels]
    before_docs = before[:, channels].astype(jnp.int32)
    first_dev = lax.axis_index("sp") == 0
    before_docs = jnp.where(first_dev, -1, before_docs)
    values = pool_input.astype(jnp.float32)
    padded = jnp.concatenate([before_rows.astype(jnp.float32), values], axis=0)
    doc_padded = jnp.concatenate([before_docs.astype(jnp.int32), docs], axis=0)
    earlier = sum(
        (doc_padded[RIM - offset : RIM - offset + tok_dev] == docs).astype(jnp.int32)
        for offset in range(1, RIM + 1)
    )
    reach = jnp.minimum(earlier[:, None] + 1, window[None, :])
    running = values
    for offset in range(1, RIM + 1):
        shifted = padded[RIM - offset : RIM - offset + tok_dev]
        running = running + jnp.where(offset < reach, shifted, 0.0)
    counts = reach.astype(jnp.float32)
    pooled = (running / counts - values).astype(jnp.bfloat16)
    tokens_pooled = lax.all_to_all(pooled, "tp", split_axis=0, concat_axis=1, tiled=True)
    lifted = jnp.dot(tokens_pooled, w_up, preferred_element_type=jnp.float32)
    gated_rows = (jax.nn.sigmoid(gate_pre.astype(jnp.float32)) * lifted).astype(jnp.bfloat16)
    mixed_rows = (
        resid.astype(jnp.float32) + jnp.dot(gated_rows, w_out, preferred_element_type=jnp.float32)
    ).astype(jnp.bfloat16)

    row_count, top_count = routes.shape
    count = lax.axis_size("sp")
    cap = capacity(row_count, top_count, count)
    order = partner(lax.axis_index("sp"), lax.iota(jnp.int32, count), count)
    chosen = routes[:, :, None] == order[None, None, :]
    named = jnp.any(chosen, axis=1)
    rank = jnp.where(named, jnp.cumsum(named.astype(jnp.int32), axis=0) - 1, -1)
    weight = jnp.sum(jnp.where(chosen, route_weight[:, :, None], 0.0), axis=1)
    return run_experts(mixed_rows, g_ffn, rank, weight, w_gate, w_lift, w_down, cap, count)


def solution(mesh):
    in_specs = (
        P("sp", "tp"),
        P(("sp", "tp"), None),
        P(("sp", "tp"), None),
        P("sp"),
        P(),
        P(),
        P(),
        P("sp", None, None),
        P("sp", None, None),
        P("sp", None, None),
        P(("sp", "tp"), None),
        P(("sp", "tp"), None),
    )
    out_specs = P(("sp", "tp"), None)
    count, tp_count = mesh.shape["sp"], mesh.shape["tp"]
    body = on_device
    if count == 4 and tp_count == 8:
        body = functools.partial(run_fused, count, tp_count)
    return jax.shard_map(
        body, mesh=mesh, in_specs=in_specs, out_specs=out_specs, check_vma=False
    )
```

```python
import functools

import jax
import jax.numpy as jnp
from jax import lax
from jax.experimental import pallas as pl
from jax.experimental.pallas import tpu as pltpu
from jax.sharding import PartitionSpec as P

POOL_W = 512
RIM = 15
TILE = 256
LANES = 128
UNIT = 16
END_SHARE = (11, 11, 12)
MESH = pl.DeviceIdType.MESH


def shifted_2(value, axis, steps):
    count = lax.axis_size(axis)
    leading, last = (max(0, -steps), min(count, count - steps))
    return lax.ppermute(value, axis, [(source, source + steps) for source in range(leading, last)])


def partner(me, step, count):
    other, bit = 0, 1
    while bit < count:
        other = other + ((me // bit + step // bit) % 2) * bit
        bit *= 2
    return other


def tile_of(t):
    return pl.ds(pl.multiple_of(t * TILE, TILE), TILE)


def experts_kernel(
    count,
    mixed_ref,
    gain_ref,
    rank_rows_ref,
    rank_cols_ref,
    weight_ref,
    w_gate_hbm,
    w_lift_hbm,
    w_down_hbm,
    out_ref,
    normed,
    onehot,
    send,
    recv,
    result,
    back,
    total,
    act,
    w_gate,
    w_lift,
    w_down,
    weight_sems,
    go_sems,
    come_sems,
    ret_go_sems,
    ret_come_sems,
):
    rows, model_dim = mixed_ref.shape
    cap = send.shape[1]
    hidden = w_gate.shape[1]
    me = lax.axis_index("sp")
    loads = [
        pltpu.make_async_copy(src.at[0], dst, weight_sems.at[i])
        for i, (src, dst) in enumerate(
            ((w_gate_hbm, w_gate), (w_lift_hbm, w_lift), (w_down_hbm, w_down))
        )
    ]

    barrier = pltpu.get_barrier_semaphore()

    def greet(j, carry):
        pl.semaphore_signal(
            barrier, inc=1, device_id={"sp": partner(me, j, count)}, device_id_type=MESH
        )
        return carry

    lax.fori_loop(1, count, greet, 0)
    for load in loads:
        load.start()

    def norm(t, carry):
        block = pl.ds(pl.multiple_of(t * 64, 64), 64)
        x = mixed_ref[block, :].astype(jnp.float32)
        scale = lax.rsqrt(jnp.mean(x * x, axis=-1, keepdims=True) + 1e-06)
        normed[block, :] = (x * scale * gain_ref[...]).astype(jnp.bfloat16)
        return carry

    lax.fori_loop(0, rows // 64, norm, 0)

    def out_copy(j):
        return pltpu.make_async_remote_copy(
            src_ref=send.at[j],
            dst_ref=recv.at[j],
            send_sem=go_sems.at[j],
            recv_sem=come_sems.at[j],
            device_id={"sp": partner(me, j, count)},
            device_id_type=MESH,
        )

    def back_copy(j):
        return pltpu.make_async_remote_copy(
            src_ref=result.at[j],
            dst_ref=back.at[j],
            send_sem=ret_go_sems.at[j],
            recv_sem=ret_come_sems.at[j],
            device_id={"sp": partner(me, j, count)},
            device_id_type=MESH,
        )

    def pack(j, target):
        slot = lax.broadcasted_iota(jnp.int32, (cap, rows), 0)
        onehot[...] = (slot == rank_rows_ref[j]).astype(jnp.float32).astype(jnp.bfloat16)

        def piece(t, carry):
            cols = tile_of(t)
            target[j, :, cols] = jnp.dot(
                onehot[...], normed[:, cols], preferred_element_type=jnp.float32
            ).astype(jnp.bfloat16)
            return carry

        lax.fori_loop(0, model_dim // TILE, piece, 0)

    def ffn(j, source):
        def up(t, carry):
            cols = tile_of(t)
            x = source[j]
            gate = jnp.minimum(jnp.dot(x, w_gate[:, cols], preferred_element_type=jnp.float32), 7.0)
            lift = jnp.clip(
                jnp.dot(x, w_lift[:, cols], preferred_element_type=jnp.float32), -7.0, 7.0
            )
            act[:, cols] = ((lift + 1.0) * gate * jax.nn.sigmoid(1.702 * gate)).astype(jnp.bfloat16)
            return carry

        lax.fori_loop(0, hidden // TILE, up, 0)

        def down(t, carry):
            cols = tile_of(t)
            result[j, :, cols] = jnp.dot(
                act[...], w_down[:, cols], preferred_element_type=jnp.float32
            ).astype(jnp.bfloat16)
            return carry

        lax.fori_loop(0, model_dim // TILE, down, 0)

    def column(ref, j):
        lane = lax.broadcasted_iota(jnp.int32, ref.shape, 1)
        return jnp.sum(jnp.where(lane == j, ref[...], 0.0), axis=1, keepdims=True)

    def combine(j, source, store):
        rank = column(rank_cols_ref, j).astype(jnp.int32)
        weight = column(weight_ref, j)
        slot = lax.broadcasted_iota(jnp.int32, (rows, cap), 1)
        pick = (slot == rank).astype(jnp.float32).astype(jnp.bfloat16)

        def piece(t, carry):
            cols = tile_of(t)
            found = jnp.dot(pick, source[j, :, cols], preferred_element_type=jnp.float32)
            store(cols, weight * found)
            return carry

        lax.fori_loop(0, model_dim // TILE, piece, 0)

    def store_first(cols, term):
        total[:, cols] = mixed_ref[:, cols].astype(jnp.float32) + term

    def store_more(cols, term):
        total[:, cols] = total[:, cols] + term

    def store_last(cols, term):
        out_ref[:, cols] = (total[:, cols] + term).astype(jnp.bfloat16)

    pl.semaphore_wait(barrier, count - 1)

    def dispatch(j, carry):
        pack(j, send)
        out_copy(j).start()
        return carry

    lax.fori_loop(1, count, dispatch, 0)
    pack(0, send)
    for load in loads:
        load.wait()
    ffn(0, send)
    combine(0, result, store_first)

    def serve(j, carry):
        out_copy(j).wait_recv()
        ffn(j, recv)
        back_copy(j).start()
        return carry

    lax.fori_loop(1, count, serve, 0)

    def gather(j, carry):
        back_copy(j).wait_recv()
        combine(j, back, store_more)
        return carry

    lax.fori_loop(1, count - 1, gather, 0)
    back_copy(count - 1).wait_recv()
    combine(count - 1, back, store_last)

    def finish(j, carry):
        out_copy(j).wait_send()
        back_copy(j).wait_send()
        return carry

    lax.fori_loop(1, count, finish, 0)


def run_experts(mixed, gain, rank, weight, w_gate, w_lift, w_down, cap, count):
    rows, model_dim = mixed.shape
    hidden = w_gate.shape[2]
    vmem = pl.BlockSpec(memory_space=pltpu.VMEM)
    anywhere = pl.BlockSpec(memory_space=pl.ANY)
    slots = pltpu.VMEM((count, cap, model_dim), jnp.bfloat16)
    return pl.pallas_call(
        functools.partial(experts_kernel, count),
        out_shape=jax.ShapeDtypeStruct((rows, model_dim), jnp.bfloat16),
        in_specs=[vmem] * 5 + [anywhere] * 3,
        out_specs=vmem,
        scratch_shapes=[
            pltpu.VMEM((rows, model_dim), jnp.bfloat16),
            pltpu.VMEM((cap, rows), jnp.bfloat16),
            slots,
            slots,
            slots,
            slots,
            pltpu.VMEM((rows, model_dim), jnp.float32),
            pltpu.VMEM((cap, hidden), jnp.bfloat16),
            pltpu.VMEM(w_gate.shape[1:], jnp.bfloat16),
            pltpu.VMEM(w_lift.shape[1:], jnp.bfloat16),
            pltpu.VMEM(w_down.shape[1:], jnp.bfloat16),
            pltpu.SemaphoreType.DMA((3,)),
            pltpu.SemaphoreType.DMA((count,)),
            pltpu.SemaphoreType.DMA((count,)),
            pltpu.SemaphoreType.DMA((count,)),
            pltpu.SemaphoreType.DMA((count,)),
        ],
        compiler_params=pltpu.CompilerParams(
            collective_id=0, has_side_effects=True, vmem_limit_bytes=60 * 2**20
        ),
        cost_estimate=pl.CostEstimate(
            flops=6 * count * cap * model_dim * hidden,
            bytes_accessed=3 * model_dim * hidden * 2,
            transcendentals=count * cap * hidden,
        ),
    )(
        mixed,
        gain[None, :],
        rank.T[:, None, :],
        rank.astype(jnp.float32),
        weight,
        w_gate,
        w_lift,
        w_down,
    )


def halves_dot(rows, weights):
    half = rows.shape[0] // 2
    parts = [
        jnp.dot(part, weights, preferred_element_type=jnp.float32)
        for part in (rows[:half], rows[half:])
    ]
    return jnp.concatenate(parts, axis=0)


def fused_kernel(
    count,
    tp_count,
    pool_hbm,
    docs_hbm,
    routes_hbm,
    route_weight_hbm,
    gain_hbm,
    gate_hbm,
    resid_hbm,
    w_up_hbm,
    w_out_hbm,
    w_gate_hbm,
    w_lift_hbm,
    w_down_hbm,
    out_ref,
    pool,
    docs,
    routes_ref,
    route_weight_ref,
    gain,
    gate_pre,
    resid,
    w_up,
    w_out,
    w_gate,
    w_lift,
    w_down,
    pooled,
    gathered,
    tokens,
    gated,
    mixed,
    normed,
    onehot,
    pick_own,
    pick_near,
    pick_rest,
    send,
    recv,
    result,
    back,
    own,
    corner,
    act,
    corner_act,
    corner_up,
    corner_down,
    corner_out,
    local_out,
    total,
    load_sems,
    edge_go,
    edge_come,
    pool_go,
    pool_come,
    part_go,
    direct_come,
    share_go,
    near_come,
    middle_come,
    out_go,
    out_come,
    ret_go,
    ret_come,
    late_go,
    late_come,
    mate_go,
    mate_come,
    core_go,
    core_come,
):
    channels = pool_hbm.shape[0]
    rows, model_dim = resid.shape
    hidden = w_gate.shape[1]
    half = hidden // 2
    cap = own.shape[0]
    part = cap // 2
    sp, tp = lax.axis_index("sp"), lax.axis_index("tp")
    plane, core = tp // 2, tp % 2
    planes = tp_count // 2
    at_end = (plane == 0) | (plane == planes - 1)
    inside = (plane > 0) & (plane < planes - 1)
    f32, bf16 = jnp.float32, jnp.bfloat16

    loads = [
        pltpu.make_async_copy(src, dst, load_sems.at[i])
        for i, (src, dst) in enumerate(
            (
                (pool_hbm, pool.at[:, LANES:]),
                (docs_hbm, docs.at[:, LANES:]),
                (w_gate_hbm.at[0], w_gate),
                (w_lift_hbm.at[0], w_lift),
                (w_down_hbm.at[0], w_down),
                (routes_hbm, routes_ref),
                (route_weight_hbm, route_weight_ref),
                (w_up_hbm, w_up),
                (gate_hbm, gate_pre),
                (w_out_hbm, w_out),
                (resid_hbm, resid),
                (gain_hbm, gain),
            )
        )
    ]
    barrier = pltpu.get_barrier_semaphore()

    for axis, me, size in (("tp", tp, tp_count), ("sp", sp, count)):
        for j in range(size - 1, 0, -1):
            pl.semaphore_signal(
                barrier, inc=1, device_id={axis: partner(me, j, size)}, device_id_type=MESH
            )
    for load in loads[:5]:
        load.start()
    def remote(src, dst, go, come, device):
        return pltpu.make_async_remote_copy(
            src_ref=src,
            dst_ref=dst,
            send_sem=go,
            recv_sem=come,
            device_id=device,
            device_id_type=MESH,
        )

    mate = {"tp": partner(tp, 1, tp_count)}
    following = {"sp": lax.rem(sp + 1, count)}
    tok_dev = pool_hbm.shape[1]
    edges = [
        remote(
            ref.at[:, pl.ds(tok_dev, LANES)],
            ref.at[:, pl.ds(0, LANES)],
            edge_go.at[i],
            edge_come.at[i],
            following,
        )
        for i, ref in enumerate((pool, docs))
    ]

    pieces = [(m, q) for q in range(4) for m in range(2)] + [(2, q) for q in range(4)]
    groups = [range(0, 1), range(1, 4)] + [range(i, i + 2) for i in range(4, 12, 2)]
    group_of = [g for g, some in enumerate(groups) for _ in some]
    sources = (w_gate, w_lift, w_down)
    far = partner(sp, 3, count)

    def span(m, q, zone):
        units = (model_dim if m < 2 else half) // UNIT
        ends = units * END_SHARE[m] // 32
        inner = (units - ends) // 2
        is_end = isinstance(zone, int) and zone == 0
        size = ends if is_end else inner
        low, high = (q % 2 * size // 2, (q % 2 + 1) * size // 2) if m < 2 else (0, size)
        if is_end:
            return low * UNIT, (high - low) * UNIT
        start = (ends + inner * (zone - 1) + low) * UNIT
        return pl.multiple_of(start, UNIT), (high - low) * UNIT

    def place(m, q, start, size):
        if m < 2:
            return corner_up.at[m, pl.ds(start, size), tile_of(q // 2)]
        return corner_down.at[pl.ds(start, size), pl.ds(q * TILE, TILE)]

    def fetch(i, zone):
        m, q = pieces[i]
        start, size = span(m, q, zone)
        if m < 2:
            cols = pl.ds(pl.multiple_of(core * half + q // 2 * TILE, TILE), TILE)
            src = sources[m].at[pl.ds(start, size), cols]
        else:
            first = pl.multiple_of(core * half + start, UNIT)
            src = sources[m].at[pl.ds(first, size), pl.ds(q * TILE, TILE)]
        return remote(
            src,
            place(m, q, start, size),
            part_go.at[m // 2],
            direct_come.at[group_of[i]],
            {"sp": far},
        )

    def share(i, zone, way):
        m, q = pieces[i]
        start, size = span(m, q, zone)
        return remote(
            place(m, q, start, size),
            place(m, q, start, size),
            share_go.at[way, m // 2],
            middle_come.at[i // 8] if way == 1 else near_come.at[i // 4 if i < 8 else i - 6],
            {"tp": partner(tp, 6 if way == 1 else 2, tp_count)},
        )

    def bytes_of(some, zones):
        size = sum(span(*pieces[i], zone)[1] for i in some for zone in zones)
        if size > model_dim:
            return corner_up.at[0, pl.ds(0, size // 2), :]
        return corner_up.at[0, pl.ds(0, size), tile_of(0)]

    def take(some, zones, sem):
        ref = bytes_of(some, zones)
        remote(ref, ref, share_go.at[0, 0], sem, mate).wait_recv()

    def pass_on(g):
        @pl.when(at_end)
        def _():
            take(groups[g], (0,), direct_come.at[g])
            for i in groups[g]:
                share(i, 0, 0).start()

        @pl.when(inside)
        def _():
            take(groups[g], (1,), direct_come.at[g])
            for i in groups[g]:
                share(i, plane, 1).start()
                share(i, plane, 0).start()

    def relay(some):
        @pl.when(inside)
        def _():
            take(some, (1,), middle_come.at[some[0] // 8])
            for i in some:
                share(i, 3 - plane, 2).start()

    def arrived(some, k):
        @pl.when(at_end)
        def _():
            take(some, (1, 2), near_come.at[k])

        @pl.when(inside)
        def _():
            take(some, (0,), near_come.at[k])

    def fetch_all(some):
        @pl.when(at_end)
        def _():
            for i in some:
                fetch(i, 0).start()

        @pl.when(inside)
        def _():
            for i in some:
                fetch(i, plane).start()

    for load in loads[:2]:
        load.wait()
    pl.semaphore_wait(barrier, count - 1 + tp_count - 1)
    for edge in edges:
        edge.start()

    for load in loads[2:4]:
        load.wait()
    fetch_all(range(8))
    for load in loads[5:]:
        load.start()

    level = (tp * channels) // (channels * tp_count // 4)

    def pool_copy(j):
        return remote(
            pooled.at[j],
            gathered.at[pl.ds(pl.multiple_of(tp * channels, channels), channels), :],
            pool_go.at[0],
            pool_come.at[0],
            {"tp": partner(tp, j, tp_count)},
        )

    def pool_block(j):
        owner = partner(tp, j, tp_count)
        cols = pl.ds(pl.multiple_of(owner * rows, LANES), rows + LANES)
        values = pool[:, cols].astype(f32)
        document = jnp.broadcast_to(docs[:, cols], (8, rows + LANES))
        lane = lax.broadcasted_iota(jnp.int32, document.shape, 1)
        document = jnp.where((lane < LANES) & (owner == 0) & (sp == 0), -1, document)
        running = values
        number = jnp.ones(document.shape, f32)
        for step in range(4):
            shift = 2**step
            same = (document == pltpu.roll(document, shift, 1)) & (level >= step)
            same = same.astype(f32)
            number = number + same * pltpu.roll(number, shift, 1)
            wide = jnp.concatenate([same] * (channels // 8), axis=0)
            running = running + wide * pltpu.roll(running, shift, 1)
        share_of = jnp.concatenate([1.0 / number] * (channels // 8), axis=0)
        return (running * share_of - values)[:, LANES:].astype(bf16)

    def pool_send(j):
        pooled[j] = pool_block(j)
        pool_copy(j).start()

    def pool_step(i, carry):
        j = lax.rem(i + 1, tp_count - 1) + 1

        @pl.when(j != tp)
        def _():
            pool_send(j)

        return carry

    lax.fori_loop(0, tp_count - 1, pool_step, 0)
    loads[4].wait()
    fetch_all(range(8, 12))
    for edge in edges:
        edge.wait_recv()

    @pl.when(tp != 0)
    def _():
        pool_send(tp)

    gathered[pl.ds(pl.multiple_of(tp * channels, channels), channels), :] = pool_block(0)
    pass_on(0)

    for load in loads[5:7]:
        load.wait()

    first, second = routes_ref[0:1, :], routes_ref[1:2, :]
    weight_first, weight_second = route_weight_ref[0:1, :], route_weight_ref[1:2, :]
    named, weights = [], []
    for j in range(count):
        expert = partner(sp, j, count)
        named.append(jnp.where((first == expert) | (second == expert), 1.0, 0.0))
        weights.append(
            jnp.where(first == expert, weight_first, 0.0)
            + jnp.where(second == expert, weight_second, 0.0)
        )
    named = jnp.concatenate(named + named, axis=0)
    weights = jnp.concatenate(weights + weights, axis=0)
    before = lax.broadcasted_iota(jnp.int32, (rows, rows), 0) <= lax.broadcasted_iota(
        jnp.int32, (rows, rows), 1
    )
    place_of = jnp.dot(
        named.astype(bf16), before.astype(f32).astype(bf16), preferred_element_type=f32
    )
    place_of = jnp.where(named > 0.0, place_of - 1.0, -4.0 * cap)
    split = jnp.where(place_of >= part, place_of + part, place_of)
    line = lax.broadcasted_iota(jnp.int32, place_of.shape, 0)
    goal = jnp.where(line == 1, split, place_of)
    goal = jnp.where(line == 2, split + part, goal)
    goal = jnp.where(line == 3, place_of + cap, goal)
    goal_rows = goal.astype(jnp.int32)
    goal_cols = goal.T.astype(jnp.int32)
    weight_cols = weights.T

    slot = lax.broadcasted_iota(jnp.int32, (2 * cap, rows), 0)
    for k, (a, b) in enumerate(((1, 2), (0, 3))):
        hit = (slot == goal_rows[a : a + 1, :]) | (slot == goal_rows[b : b + 1, :])
        onehot[k] = hit.astype(f32).astype(bf16)

    def weighed(slots, j, shift):
        return jnp.where(
            slots == goal_cols[:, j : j + 1] + shift, weight_cols[:, j : j + 1], 0.0
        )

    slots = lax.broadcasted_iota(jnp.int32, (rows, cap), 1)
    pick_own[...] = weighed(slots, 0, 0).astype(bf16)
    pick_near[...] = (weighed(slots, 1, 0) + weighed(slots, 2, 0)).astype(bf16)
    slots = lax.broadcasted_iota(jnp.int32, (rows, 3 * cap), 1)
    found = weighed(slots, 3, -cap) + weighed(slots, 3, 0)
    late = jnp.where(slots >= 2 * cap, slots - cap, -1)
    found = found + weighed(late, 1, 0) + weighed(late, 2, 0)
    pick_rest[...] = found.astype(bf16)

    pass_on(1)

    for load in loads[7:]:
        load.wait()

    others = gathered.at[pl.ds(0, (tp_count - 1) * channels), :]
    remote(others, others, pool_go.at[0], pool_come.at[0], mate).wait_recv()
    tokens[...] = gathered[...].T

    def lift_up(t, carry):
        cols = tile_of(t)
        lifted = halves_dot(tokens[...], w_up[:, cols])
        gated[:, cols] = (jax.nn.sigmoid(gate_pre[:, cols].astype(f32)) * lifted).astype(bf16)
        return carry

    lax.fori_loop(0, model_dim // TILE, lift_up, 0)

    def mix(t, carry):
        cols = tile_of(t)
        added = halves_dot(gated[...], w_out[:, cols])
        mixed[:, cols] = (resid[:, cols].astype(f32) + added).astype(bf16)
        return carry

    lax.fori_loop(0, model_dim // TILE, mix, 0)

    def norm(t, carry):
        block = pl.ds(pl.multiple_of(t * 64, 64), 64)
        x = mixed[block, :].astype(f32)
        scale = lax.rsqrt(jnp.mean(x * x, axis=-1, keepdims=True) + 1e-06)
        normed[block, :] = (x * scale * gain[...]).astype(bf16)
        return carry

    pass_on(2)
    lax.fori_loop(0, rows // 64, norm, 0)

    def pack_near(t, carry):
        cols = tile_of(t)
        send[:, cols] = halves_dot(onehot[0], normed[:, cols]).astype(bf16)
        return carry

    lax.fori_loop(0, model_dim // TILE, pack_near, 0)

    def out_copy(h, p):
        block = pl.ds((2 * h + p) * part, part)
        return remote(
            send.at[block],
            recv.at[block],
            out_go.at[0],
            out_come.at[h],
            {"sp": partner(sp, p + 1, count)},
        )

    def back_copy(p):
        block = pl.ds(p * part, part)
        return remote(
            result.at[block],
            back.at[block],
            ret_go.at[0],
            ret_come.at[0],
            {"sp": partner(sp, p + 1, count)},
        )

    def late_copy(p, t):
        return remote(
            result.at[pl.ds((2 + p) * part, part), tile_of(t)],
            back.at[pl.ds(3 * cap + p * part, part), tile_of(t)],
            late_go.at[0],
            late_come.at[t],
            {"sp": partner(sp, p + 1, count)},
        )

    chunks = [(h, p) for h in range(2) for p in range(2)]
    for h, p in chunks:
        out_copy(h, p).start()

    def pack_local(t, carry):
        cols = tile_of(t)
        packed = halves_dot(onehot[1], normed[:, cols]).astype(bf16)
        own[:, cols] = packed[:cap]
        corner[0:cap, cols] = packed[cap:]
        return carry

    lax.fori_loop(0, model_dim // TILE, pack_local, 0)
    corner_copy = remote(
        corner.at[pl.ds(0, cap)], corner.at[pl.ds(cap, cap)], core_go.at[0], core_come.at[0], mate
    )
    corner_copy.start()
    pass_on(3)

    def activate(gate, lift):
        gate = jnp.minimum(gate, 7.0)
        lift = jnp.clip(lift, -7.0, 7.0)
        return ((lift + 1.0) * gate * jax.nn.sigmoid(1.702 * gate)).astype(bf16)

    def ffn(source, target, base, then=lambda t: None):
        def up(t, carry):
            cols = tile_of(t)
            x = source[base : base + cap, :]
            act[:, cols] = activate(
                jnp.dot(x, w_gate[:, cols], preferred_element_type=f32),
                jnp.dot(x, w_lift[:, cols], preferred_element_type=f32),
            )
            return carry

        lax.fori_loop(0, hidden // TILE, up, 0)

        def down(t, carry):
            cols = tile_of(t)
            target[base : base + cap, cols] = halves_dot(act[...], w_down[:, cols]).astype(bf16)
            then(t)
            return carry

        lax.fori_loop(0, model_dim // TILE, down, 0)

    ffn(own, local_out, 0)
    pass_on(4)

    def combine_own(t, carry):
        cols = tile_of(t)
        found = halves_dot(pick_own[...], local_out[:, cols])
        total[:, cols] = mixed[:, cols].astype(f32) + found
        return carry

    lax.fori_loop(0, model_dim // TILE, combine_own, 0)
    pass_on(5)
    relay(range(8))

    def near_arrived(h):
        block = pl.ds(h * cap, cap)
        remote(send.at[block], recv.at[block], out_go.at[0], out_come.at[h], mate).wait_recv()

    near_arrived(0)
    ffn(recv, result, 0)
    for p in range(2):
        back_copy(p).start()
    relay(range(8, 12))
    near_arrived(1)

    def send_back(t):
        for p in range(2):
            late_copy(p, t).start()

    ffn(recv, result, cap, send_back)

    corner_copy.wait_recv()

    def corner_lift(t):
        cols = tile_of(t)
        x = corner[...]
        corner_act[:, cols] = activate(
            jnp.dot(x, corner_up[0, :, cols], preferred_element_type=f32),
            jnp.dot(x, corner_up[1, :, cols], preferred_element_type=f32),
        )

    def combine_near(t, carry):
        cols = tile_of(t)
        found = halves_dot(pick_near[...], back[0:cap, cols])
        total[:, cols] = total[:, cols] + found
        return carry

    tiles = model_dim // TILE
    arrived(range(4), 0)
    corner_lift(0)
    block = pl.ds(0, cap)
    remote(result.at[block], back.at[block], ret_go.at[0], ret_come.at[0], mate).wait_recv()
    lax.fori_loop(0, tiles, combine_near, 0)
    for u in range(1, half // TILE):
        arrived(range(4 * u, 4 * u + 4), u)
        corner_lift(u)

    def mate_copy(t):
        return remote(
            corner_out.at[:, tile_of(t)],
            back.at[pl.ds(2 * cap, cap), tile_of(t)],
            mate_go.at[0],
            mate_come.at[t],
            mate,
        )

    def corner_drop(t):
        cols = tile_of(t)
        found = halves_dot(corner_act[...], corner_down[:, cols]).astype(bf16)
        corner_out[:, cols] = found[cap:]
        mate_copy(t).start()
        back[cap : 2 * cap, cols] = found[:cap]

    def combine_rest(t):
        cols = tile_of(t)
        mate_copy(t).wait_recv()
        block = back.at[pl.ds(3 * cap, cap), cols]
        remote(block, block, late_go.at[0], late_come.at[t], mate).wait_recv()
        found = halves_dot(pick_rest[...], back[cap:, cols])
        out_ref[:, cols] = (total[:, cols] + found).astype(bf16)

    for t in range(tiles):
        arrived(range(8 + t, 9 + t), 2 + t)
        corner_drop(t)
        if t > 0:
            combine_rest(t - 1)
    combine_rest(tiles - 1)

    for edge in edges:
        edge.wait_send()

    others = pooled.at[pl.ds(1, tp_count - 1)]
    remote(others, others, pool_go.at[0], pool_come.at[0], mate).wait_send()
    remote(send, recv, out_go.at[0], out_come.at[0], mate).wait_send()
    corner_copy.wait_send()
    block = pl.ds(0, cap)
    remote(result.at[block], back.at[block], ret_go.at[0], ret_come.at[0], mate).wait_send()
    block = pl.ds(cap, cap)
    remote(result.at[block], back.at[block], late_go.at[0], late_come.at[0], mate).wait_send()
    remote(corner_out, corner_out, mate_go.at[0], mate_come.at[0], mate).wait_send()

    def gone(zone, sems):
        for k, some in enumerate((range(8), range(8, 12))):
            ref = bytes_of(some, (zone,))
            remote(ref, ref, sems.at[k], direct_come.at[0], mate).wait_send()

    @pl.when(at_end)
    def _():
        gone(0, part_go)
        gone(0, share_go.at[0])

    @pl.when(inside)
    def _():
        gone(1, part_go)
        for way in range(3):
            gone(1, share_go.at[way])


def run_fused(
    count,
    tp_count,
    pool_input,
    gate_pre,
    resid,
    docs,
    w_up,
    w_out,
    g_ffn,
    w_gate,
    w_lift,
    w_down,
    routes,
    route_weight,
):
    tok_dev, channels = pool_input.shape
    rows, model_dim = resid.shape
    hidden = w_gate.shape[2]
    half = hidden // 2
    pool_w = w_up.shape[0]
    top = routes.shape[1]
    cap = capacity(rows, top, count)
    vmem = pl.BlockSpec(memory_space=pltpu.VMEM)
    bf16, f32 = jnp.bfloat16, jnp.float32
    hbm = functools.partial(pltpu.with_memory_space_constraint, memory_space=pltpu.HBM)
    dma = pltpu.SemaphoreType.DMA
    return pl.pallas_call(
        functools.partial(fused_kernel, count, tp_count),
        out_shape=jax.ShapeDtypeStruct((rows, model_dim), bf16),
        in_specs=[pl.BlockSpec(memory_space=pltpu.HBM)] * 12,
        out_specs=vmem,
        scratch_shapes=[
            pltpu.VMEM((channels, tok_dev + LANES), bf16),
            pltpu.VMEM((1, tok_dev + LANES), jnp.int32),
            pltpu.VMEM((top, rows), jnp.int32),
            pltpu.VMEM((top, rows), f32),
            pltpu.VMEM((1, model_dim), f32),
            pltpu.VMEM((rows, model_dim), bf16),
            pltpu.VMEM((rows, model_dim), bf16),
            pltpu.VMEM(w_up.shape, bf16),
            pltpu.VMEM(w_out.shape, bf16),
            pltpu.VMEM(w_gate.shape[1:], bf16),
            pltpu.VMEM(w_lift.shape[1:], bf16),
            pltpu.VMEM(w_down.shape[1:], bf16),
            pltpu.VMEM((tp_count, channels, rows), bf16),
            pltpu.VMEM((pool_w, rows), bf16),
            pltpu.VMEM((rows, pool_w), bf16),
            pltpu.VMEM((rows, model_dim), bf16),
            pltpu.VMEM((rows, model_dim), bf16),
            pltpu.VMEM((rows, model_dim), bf16),
            pltpu.VMEM((2, 2 * cap, rows), bf16),
            pltpu.VMEM((rows, cap), bf16),
            pltpu.VMEM((rows, cap), bf16),
            pltpu.VMEM((rows, 3 * cap), bf16),
            pltpu.VMEM((2 * cap, model_dim), bf16),
            pltpu.VMEM((2 * cap, model_dim), bf16),
            pltpu.VMEM((2 * cap, model_dim), bf16),
            pltpu.VMEM((4 * cap, model_dim), bf16),
            pltpu.VMEM((cap, model_dim), bf16),
            pltpu.VMEM((2 * cap, model_dim), bf16),
            pltpu.VMEM((cap, hidden), bf16),
            pltpu.VMEM((2 * cap, half), bf16),
            pltpu.VMEM((2, model_dim, half), bf16),
            pltpu.VMEM((half, model_dim), bf16),
            pltpu.VMEM((cap, model_dim), bf16),
            pltpu.VMEM((cap, model_dim), bf16),
            pltpu.VMEM((rows, model_dim), f32),
            dma((12,)),
            dma((2,)),
            dma((2,)),
            dma((1,)),
            dma((1,)),
            dma((2,)),
            dma((6,)),
            dma((3, 2)),
            dma((6,)),
            dma((2,)),
            dma((1,)),
            dma((2,)),
            dma((1,)),
            dma((1,)),
            dma((1,)),
            dma((4,)),
            dma((1,)),
            dma((4,)),
            dma((1,)),
            dma((1,)),
        ],
        compiler_params=pltpu.CompilerParams(
            collective_id=1, has_side_effects=True, vmem_limit_bytes=52 * 2**20
        ),
        cost_estimate=pl.CostEstimate(
            flops=6 * count * cap * model_dim * hidden,
            bytes_accessed=3 * model_dim * hidden * 2,
            transcendentals=count * cap * hidden,
        ),
    )(
        hbm(pool_input.T),
        hbm(docs[None, :]),
        hbm(routes.T),
        hbm(route_weight.T),
        hbm(g_ffn[None, :]),
        gate_pre,
        resid,
        w_up,
        w_out,
        w_gate,
        w_lift,
        w_down,
    )


def capacity(row_count, top_count, count):
    cap = max(2, 5 * row_count * top_count // (4 * count))
    return (cap + 15) // 16 * 16


def on_device(
    pool_input,
    gate_pre,
    resid,
    docs,
    w_up,
    w_out,
    g_ffn,
    w_gate,
    w_lift,
    w_down,
    routes,
    route_weight,
):
    tok_dev = pool_input.shape[0]
    channels = pool_input.shape[1]
    group_size = POOL_W // 4
    channel_ids = lax.axis_index("tp") * channels + lax.iota(jnp.int32, channels)
    window = jnp.power(2, channel_ids // group_size + 1)
    edge = jnp.concatenate(
        [pool_input[tok_dev - RIM :], docs[tok_dev - RIM :, None].astype(jnp.bfloat16)], axis=1
    )
    before = shifted_2(edge, "sp", 1)
    before_rows = before[:, :channels]
    before_docs = before[:, channels].astype(jnp.int32)
    first_dev = lax.axis_index("sp") == 0
    before_docs = jnp.where(first_dev, -1, before_docs)
    values = pool_input.astype(jnp.float32)
    padded = jnp.concatenate([before_rows.astype(jnp.float32), values], axis=0)
    doc_padded = jnp.concatenate([before_docs.astype(jnp.int32), docs], axis=0)
    earlier = sum(
        (doc_padded[RIM - offset : RIM - offset + tok_dev] == docs).astype(jnp.int32)
        for offset in range(1, RIM + 1)
    )
    reach = jnp.minimum(earlier[:, None] + 1, window[None, :])
    running = values
    for offset in range(1, RIM + 1):
        shifted = padded[RIM - offset : RIM - offset + tok_dev]
        running = running + jnp.where(offset < reach, shifted, 0.0)
    counts = reach.astype(jnp.float32)
    pooled = (running / counts - values).astype(jnp.bfloat16)
    tokens_pooled = lax.all_to_all(pooled, "tp", split_axis=0, concat_axis=1, tiled=True)
    lifted = jnp.dot(tokens_pooled, w_up, preferred_element_type=jnp.float32)
    gated_rows = (jax.nn.sigmoid(gate_pre.astype(jnp.float32)) * lifted).astype(jnp.bfloat16)
    mixed_rows = (
        resid.astype(jnp.float32) + jnp.dot(gated_rows, w_out, preferred_element_type=jnp.float32)
    ).astype(jnp.bfloat16)

    row_count, top_count = routes.shape
    count = lax.axis_size("sp")
    cap = capacity(row_count, top_count, count)
    order = partner(lax.axis_index("sp"), lax.iota(jnp.int32, count), count)
    chosen = routes[:, :, None] == order[None, None, :]
    named = jnp.any(chosen, axis=1)
    rank = jnp.where(named, jnp.cumsum(named.astype(jnp.int32), axis=0) - 1, -1)
    weight = jnp.sum(jnp.where(chosen, route_weight[:, :, None], 0.0), axis=1)
    return run_experts(mixed_rows, g_ffn, rank, weight, w_gate, w_lift, w_down, cap, count)


def solution(mesh):
    in_specs = (
        P("sp", "tp"),
        P(("sp", "tp"), None),
        P(("sp", "tp"), None),
        P("sp"),
        P(),
        P(),
        P(),
        P("sp", None, None),
        P("sp", None, None),
        P("sp", None, None),
        P(("sp", "tp"), None),
        P(("sp", "tp"), None),
    )
    out_specs = P(("sp", "tp"), None)
    count, tp_count = mesh.shape["sp"], mesh.shape["tp"]
    body = on_device
    if count == 4 and tp_count == 8:
        body = functools.partial(run_fused, count, tp_count)
    return jax.shard_map(
        body, mesh=mesh, in_specs=in_specs, out_specs=out_specs, check_vma=False
    )
```
